512 devices in a mesh: ep: 128 (over z, y, core), tp: 4 (over x).
Axes of the slice: x: 4, y: 8, z: 8, core: 2. Of those that a mesh axis runs over, the one named last changes fastest.
Arguments:
- residual_in: bfloat16 [256, 2048], P('ep'), may hold values from -6 to 6
- gla_state: float32 [256, 4, 256, 512], P('ep', 'tp'), may hold values from -6 to 6
- norm_gain: bfloat16 [2048], replicated, may hold values from 0.099609375 to 1.8984375
- w_query: bfloat16 [2048, 1024], P('ep', 'tp'), may hold values from -0.125 to 0.125
- w_key: bfloat16 [2048, 1024], P('ep', 'tp'), may hold values from -0.125 to 0.125
- w_value: bfloat16 [2048, 2048], P('ep', 'tp'), may hold values from -0.125 to 0.125
- w_decay: bfloat16 [2048, 1024], P('ep', 'tp'), may hold values from -0.5 to 0.5
- decay_bias: float32 [1024], P('tp'), may hold values from -40 to 8
- head_gain: bfloat16 [512], replicated, may hold values from 0.099609375 to 1.8984375
- w_output: bfloat16 [2048, 2048], P('tp', 'ep'), may hold values from -0.125 to 0.125
- ffn_gain: bfloat16 [2048], replicated, may hold values from 0.099609375 to 1.8984375
- router_group: bfloat16 [2048, 4], replicated, may hold values from -0.125 to 0.125
- router_expert: bfloat16 [128, 2048], replicated, may hold values from -0.125 to 0.125
- expert_ids: int32 [256, 2], replicated, may hold values from 0 to 127, all different within a row; in each aligned block of 256 rows (0 to 255, 256 to 511, ...) at most 16 rows name the same one
- w_gate: bfloat16 [128, 2048, 512], P('ep', None, 'tp'), may hold values from -0.125 to 0.125
- w_up: bfloat16 [128, 2048, 512], P('ep', None, 'tp'), may hold values from -0.125 to 0.125
- w_down: bfloat16 [128, 512, 2048], P('ep', 'tp'), may hold values from -0.75 to 0.75
Outputs:
- layer_out: bfloat16 [256, 2048], P('ep')
- new_state: float32 [256, 4, 256, 512], P('ep', 'tp')
The draws below stay inside these ranges and needn't reach their ends.
Inputs may be any that keep to these rules, and one draw needn't show every extreme that they name: `expert_ids`: each row names 2 different experts; no expert is named by more than 16 rows of the whole batch, a bound that some block reaches.
All inputs are finite; a program needn't handle non-finite values.
Results may differ from the reference program's by a relative error of at most 0.023.
Values may be sent and summed in bfloat16 or wider, within the bound.
No kernel may reach another device: no remote copies, remote signals or barrier semaphores. Data moves between devices by JAX's collectives and lax.ppermute only.
A program may use at most 64 MiB of HBM per device.

```python
import math
import jax
import jax.numpy as jnp
import numpy as np
from jax import lax

D = 2048
HEADS = 4
DKH = 256
DVH = 512
FF = 512
GROUPS = 4
TOP = 2
TOKENS = 256
EXPERTS = 128
CAP = 16
DK = 1024
DV = 2048


def draw_decay_bias(key, part):
    return jax.random.uniform(key, (HEADS * DKH,), jnp.float32, -40.0, 8.0)


def levels(own_key, shape, cuts, least, high):
    loudness = 1.0
    for axis_at, shards_of in cuts:
        heights = jax.random.uniform(jax.random.fold_in(jax.random.fold_in(own_key, 6), axis_at), (shards_of,), jnp.float32, least / len(cuts), high / len(cuts))
        loudness = loudness * jnp.repeat(jnp.exp(heights), shape[axis_at] // shards_of).reshape((-1,) + (1,) * (len(shape) - 1 - axis_at))
    return loudness


def deal_out(own_key, own, number, rows, count, top, reach, slope):
    sequence = jax.random.permutation(own_key, count)
    crowded, usual = portions_of(count, rows * top, reach, slope, True), portions_of(count, rows * top, reach, slope, False)
    places = jnp.arange(count)

    def named(lengths, rotation):
        used = int((lengths > 0).sum())
        fixed = max(1, used // 4)
        shifted = fixed + (places - fixed + rotation * (used - fixed)) % max(1, count - fixed)
        return jnp.zeros((count,), jnp.int32).at[sequence[jnp.where(places < fixed, places, shifted)]].set(jnp.asarray(lengths, jnp.int32))

    lengths = jnp.where(number % 4 == 0, named(crowded, number // 4), named(usual, number - number // 4 - 1))
    mixed = jax.random.permutation(jax.random.fold_in(own, 3), count)
    source_of, receiver = mixed[0:count // 2 * 2:2], mixed[1:count // 2 * 2:2]
    margin = jnp.minimum(lengths[source_of] - 1, reach - lengths[receiver]) // 2
    margin = jnp.where((source_of == sequence[0]) | (receiver == sequence[0]) | (lengths[receiver] == 0), 0, jnp.maximum(margin, 0))
    shifted = jax.random.randint(jax.random.fold_in(own, 4), (count // 2,), 0, 1 << 20) % (margin + 1)
    lengths = lengths.at[source_of].add(-shifted).at[receiver].add(shifted)
    labels = jnp.searchsorted(jnp.cumsum(lengths), jnp.arange(rows * top), side="right").astype(jnp.int32)
    listing = labels.reshape(top, rows).T
    listing = listing[jax.random.permutation(jax.random.fold_in(own, 1), rows)]
    rotation = jax.random.randint(jax.random.fold_in(own, 2), (rows, 1), 0, top)
    return jnp.take_along_axis(listing, (jnp.arange(top)[None, :] + rotation) % top, axis=1)


def portions_of(amount, total, limit, lean, full):
    portions = [(1 << 20) // math.isqrt(rank ** lean) + 1 for rank in range(1, amount + 1)]
    largest = limit if full else min(limit, max(-(-total // amount), total * portions[0] // sum(portions)))
    least = 1 if total - largest >= amount - 1 else 0
    holding, surplus = [largest] + [least] * (amount - 1), total - largest - least * (amount - 1)
    while surplus > 0:
        candidates = [i for i in range(1, amount) if holding[i] < largest] or [i for i in range(1, amount) if holding[i] < limit]
        pool, remaining = sum([portions[i] for i in candidates]), surplus
        for i in candidates:
            addition = min(limit - holding[i], max(1, remaining * portions[i] // pool), surplus)
            holding[i] = holding[i] + addition
            surplus = surplus - addition
    return np.array(holding)


def normal_values(rng, extent, scale, bound, shards=(), kind=jnp.bfloat16):
    array = scale * jax.random.normal(rng, extent, jnp.float32)
    if shards:
        array = array * levels(rng, extent, shards, -0.22, 0.18)
    return jnp.clip(array, -bound, bound).astype(kind)


def setup_inputs(seed: int = 0) -> dict:
    arg_keys = jax.random.split(jax.random.key(seed), 18)
    residual_in = normal_values(arg_keys[0], (TOKENS, D), 1.0, 6.0, ((0, 128),))
    gla_state = normal_values(arg_keys[1], (TOKENS, HEADS, DKH, DVH), 1.0, 6.0, ((0, 128), (1, 4)), jnp.float32)
    norm_gain = jnp.clip(1.0 + 0.18 * jax.random.normal(arg_keys[2], (D,), jnp.float32), 0.099609375, 1.8984375).astype(jnp.bfloat16)
    w_query = normal_values(arg_keys[3], (D, DK), D ** -0.5, 0.125, ((0, 128), (1, 4)))
    w_key = normal_values(arg_keys[4], (D, DK), D ** -0.5, 0.125, ((0, 128), (1, 4)))
    w_value = normal_values(arg_keys[5], (D, DV), D ** -0.5, 0.125, ((0, 128), (1, 4)))
    w_decay = normal_values(arg_keys[6], (D, DK), (4 * D ** -0.5), 0.5, ((0, 128), (1, 4)))
    decay_bias = draw_decay_bias(jax.random.fold_in(arg_keys[17], 71), 0)
    head_gain = jnp.clip(1.0 + 0.18 * jax.random.normal(arg_keys[8], (DVH,), jnp.float32), 0.099609375, 1.8984375).astype(jnp.bfloat16)
    w_output = normal_values(arg_keys[9], (DV, D), DV ** -0.5, 0.125, ((0, 4), (1, 128)))
    ffn_gain = jnp.clip(1.0 + 0.18 * jax.random.normal(arg_keys[10], (D,), jnp.float32), 0.099609375, 1.8984375).astype(jnp.bfloat16)
    router_group = normal_values(arg_keys[11], (D, GROUPS), D ** -0.5, 0.125)
    router_expert = normal_values(arg_keys[12], (EXPERTS, D), D ** -0.5, 0.125)
    expert_ids_keys = jax.random.split(jax.random.fold_in(arg_keys[13], 1), TOKENS // TOKENS)
    expert_ids_turns = jax.random.permutation(jax.random.fold_in(arg_keys[13], 3), TOKENS // TOKENS)
    expert_ids = jax.vmap(lambda own, number: deal_out(jax.random.fold_in(arg_keys[13], 2), own, number, TOKENS, EXPERTS, TOP, CAP, 2))(expert_ids_keys, expert_ids_turns).reshape((TOKENS, TOP))
    w_gate = normal_values(arg_keys[14], (EXPERTS, D, FF), D ** -0.5, 0.125, ((0, 128), (2, 4)))
    w_up = normal_values(arg_keys[15], (EXPERTS, D, FF), D ** -0.5, 0.125, ((0, 128), (2, 4)))
    w_down = normal_values(arg_keys[16], (EXPERTS, FF, D), (3 * FF ** -0.5), 0.75, ((0, 128), (1, 4)))
    return {"residual_in": residual_in, "gla_state": gla_state, "norm_gain": norm_gain, "w_query": w_query, "w_key": w_key, "w_value": w_value, "w_decay": w_decay, "decay_bias": decay_bias, "head_gain": head_gain, "w_output": w_output, "ffn_gain": ffn_gain, "router_group": router_group, "router_expert": router_expert, "expert_ids": expert_ids, "w_gate": w_gate, "w_up": w_up, "w_down": w_down}


EPSILON = 1e-06
GATE_SCALE = 16.0

def rms_scale(values, gain_vec):
    floats = values.astype(jnp.float32)
    return floats * lax.rsqrt(lax.optimization_barrier(jnp.mean(floats * floats, axis=-1, keepdims=True)) + EPSILON) * gain_vec.astype(jnp.float32)

def reference(residual_in, gla_state, norm_gain, w_query, w_key, w_value, w_decay, decay_bias, head_gain, w_output, ffn_gain, router_group, router_expert, expert_ids, w_gate, w_up, w_down):
    tokens = residual_in.shape[0]
    normed = rms_scale(residual_in, norm_gain).astype(jnp.bfloat16)
    query_rows = jnp.dot(normed, w_query, preferred_element_type=jnp.float32).astype(jnp.bfloat16)
    key_rows = jnp.dot(normed, w_key, preferred_element_type=jnp.float32).astype(jnp.bfloat16)
    value_rows = jnp.dot(normed, w_value, preferred_element_type=jnp.float32).astype(jnp.bfloat16)
    decay_pre = jnp.dot(normed, w_decay, preferred_element_type=jnp.float32)
    log_decay = jax.nn.log_sigmoid(decay_pre + decay_bias) / GATE_SCALE
    query_float = lax.optimization_barrier(query_rows).astype(jnp.float32).reshape(tokens, HEADS, DKH) * DKH ** (-0.5)
    key_float = lax.optimization_barrier(key_rows).astype(jnp.float32).reshape(tokens, HEADS, DKH)
    value_float = lax.optimization_barrier(value_rows).astype(jnp.float32).reshape(tokens, HEADS, DVH)
    alpha = jnp.exp(log_decay).reshape(tokens, HEADS, DKH)
    new_state = alpha[..., None] * gla_state + key_float[..., None] * value_float[:, :, None, :]
    read_out = jnp.einsum('thk,thkv->thv', query_float, new_state, precision=lax.Precision.HIGHEST)
    gated_heads = rms_scale(read_out, head_gain).astype(jnp.bfloat16)
    attention = jnp.zeros((tokens, D), jnp.float32)
    for head_index in range(HEADS):
        partial_out = jnp.dot(gated_heads[:, head_index], w_output[head_index * DVH:(head_index + 1) * DVH], preferred_element_type=jnp.float32).astype(jnp.bfloat16)
        attention = attention + lax.optimization_barrier(partial_out).astype(jnp.float32)
    hidden_res = (residual_in.astype(jnp.float32) + attention).astype(jnp.bfloat16)
    moe_in = rms_scale(hidden_res, ffn_gain).astype(jnp.bfloat16)
    group_logits = jnp.dot(moe_in, router_group, preferred_element_type=jnp.float32)
    expert_logits = jnp.dot(moe_in, router_expert.T, preferred_element_type=jnp.float32)
    per_group = EXPERTS // GROUPS

    def route_weight(mine_col, other_col):
        chosen = jnp.take_along_axis(expert_logits, expert_ids[:, mine_col:mine_col + 1], axis=1)[:, 0]
        rival_logit = jnp.take_along_axis(expert_logits, expert_ids[:, other_col:other_col + 1], axis=1)[:, 0]
        group_of = (expert_ids[:, mine_col] // per_group).astype(jnp.int32)
        group_logit = jnp.take_along_axis(group_logits, group_of[:, None], axis=1)[:, 0]
        group_share = 1.0 / lax.optimization_barrier(jnp.sum(jnp.exp(group_logits - group_logit[:, None]), axis=1))
        return group_share * jax.nn.sigmoid(chosen - rival_logit)
    weights = jnp.stack([route_weight(0, 1), route_weight(1, 0)], axis=1)
    slot_index = jnp.arange(CAP, dtype=jnp.int32)

    def expert_step(summed, expert):
        is_named = jnp.any(expert_ids == expert, axis=1)
        slot_of = jnp.cumsum(is_named.astype(jnp.int32)) - 1
        select = (is_named[None, :] & (slot_of[None, :] == slot_index[:, None])).astype(jnp.float32)
        slot_rows = jnp.dot(select.astype(jnp.bfloat16), moe_in, preferred_element_type=jnp.float32).astype(jnp.bfloat16)
        gate_out = jnp.dot(slot_rows, w_gate[expert], preferred_element_type=jnp.float32)
        up_out = jnp.dot(slot_rows, w_up[expert], preferred_element_type=jnp.float32)
        hidden = (jax.nn.silu(gate_out) * up_out).astype(jnp.bfloat16)
        output = jnp.dot(hidden, w_down[expert], preferred_element_type=jnp.float32)
        token_weight = lax.optimization_barrier(jnp.sum(jnp.where(expert_ids == expert, weights, jnp.zeros_like(weights)), axis=1))
        slot_weight = jnp.dot(select, token_weight, precision=lax.Precision.HIGHEST)
        summed = summed + jnp.dot(select.T, output * slot_weight[:, None], precision=lax.Precision.HIGHEST)
        return (summed, None)
    moe_sum, _ = lax.scan(expert_step, jnp.zeros((tokens, D), jnp.float32), jnp.arange(EXPERTS, dtype=jnp.int32))
    layer_out = (hidden_res.astype(jnp.float32) + moe_sum).astype(jnp.bfloat16)
    return (layer_out, new_state)
```

```python
import jax
import jax.numpy as jnp
from jax import lax
from jax.sharding import Mesh
from jax.sharding import PartitionSpec as P

CAP = 16
EP = ("ep_0", "ep_1", "ep_2")
FAR = ("ep_0", "ep_1")
SLAB = ("ep_1", "ep_2")
SLAB_TP = ("ep_1", "ep_2", "tp")
CHIPS = ("ep_2", "tp")

EPSILON = 1e-06
GATE_SCALE = 16.0
F32 = jnp.float32
BF16 = jnp.bfloat16


def exchange(blocks, axes, *later):
    came = lax.all_to_all(blocks, axes, split_axis=0, concat_axis=0, tiled=True)
    return lax.optimization_barrier((came, *later)) if later else came


def to_all(shard, count):
    return jnp.broadcast_to(shard[None], (count, *shard.shape))


def rms_scale(values, gain_vec):
    floats = values.astype(F32)
    return (
        floats
        * lax.rsqrt(jnp.mean(floats * floats, axis=-1, keepdims=True) + EPSILON)
        * gain_vec.astype(F32)
    )


def on_device(
    residual_in,
    gla_state,
    norm_gain,
    w_query,
    w_key,
    w_value,
    w_decay,
    decay_bias,
    head_gain,
    w_output,
    ffn_gain,
    router_group,
    router_expert,
    expert_ids,
    w_gate,
    w_up,
    w_down,
):
    depths, rows, cores = (lax.axis_size(a) for a in EP)
    heads = lax.axis_size("tp")
    slab = rows * cores
    parts = cores * heads
    far = depths * rows
    tokens = expert_ids.shape[0]
    seqs, width = residual_in.shape
    strip = w_query.shape[0]
    key_width, value_width = w_query.shape[1], w_value.shape[1]
    in_width = 3 * key_width + value_width
    held = depths * strip
    piece = width // parts
    place = lax.axis_index(SLAB)
    chip = lax.axis_index(FAR)
    core = lax.axis_index("ep_2")

    experts = chip * cores + jnp.arange(cores, dtype=jnp.int32)
    named = jnp.any(expert_ids[None] == experts[:, None, None], axis=2)
    slot_of = jnp.cumsum(named.astype(jnp.int32), axis=1) - 1
    slots = jnp.arange(CAP, dtype=jnp.int32)
    chosen_rows = named[:, None, :] & (slot_of[:, None, :] == slots[None, :, None])
    select = chosen_rows.astype(BF16).reshape(cores * CAP, tokens)
    expert = lax.axis_index(EP)
    own_int = lax.dynamic_index_in_dim(chosen_rows, core, 0, False).astype(jnp.int32)
    slot_ids = jnp.sum(own_int[:, :, None] * expert_ids[None], axis=1)
    rival_ids = jnp.where(slot_ids[:, 0] == expert, slot_ids[:, 1], slot_ids[:, 0])
    groups = router_group.shape[1]
    lanes = jnp.arange(router_expert.shape[0], dtype=jnp.int32)
    own_group = jnp.arange(groups, dtype=jnp.int32) == expert // (router_expert.shape[0] // groups)
    own_lane = (lanes == expert).astype(F32)
    rival_lane = (lanes[None] == rival_ids[:, None]).astype(F32)
    own_group = own_group.astype(F32)
    own_gain = norm_gain.reshape(depths, slab, strip)[:, place].reshape(held).astype(F32)
    res_float = residual_in.astype(F32)
    scale = lax.rsqrt(jnp.mean(res_float * res_float, axis=-1, keepdims=True) + EPSILON)
    strips = residual_in.reshape(seqs, depths, slab, strip).transpose(2, 0, 1, 3)
    strips = strips.reshape(slab, seqs, held)

    own_w = jnp.concatenate([w_query, w_key, w_value, w_decay, w_output.T], axis=1)
    tied = lax.optimization_barrier(
        (to_all(own_w, depths), strips, select, rival_lane, own_lane, own_group, own_gain, scale)
    )
    spread, strips, select, rival_lane, own_lane, own_group, own_gain, scale = tied
    gathered = exchange(spread, "ep_0").reshape(held, in_width + value_width)
    gathered, strips = lax.optimization_barrier((gathered, strips))
    slab_res = exchange(strips, SLAB).reshape(slab * seqs, held)
    lhs = (slab_res.astype(F32) * own_gain).astype(BF16)
    sums = jnp.dot(lhs, gathered[:, :in_width], preferred_element_type=F32).astype(BF16)
    arrived, head_gain, decay_bias = exchange(
        sums.reshape(slab, seqs, in_width), SLAB, head_gain, decay_bias
    )
    projected = arrived.astype(F32).sum(axis=0) * scale

    query = projected[:, :key_width].astype(BF16).astype(F32) * key_width ** (-0.5)
    key = projected[:, key_width : 2 * key_width].astype(BF16).astype(F32)
    value = projected[:, 2 * key_width : 2 * key_width + value_width].astype(BF16).astype(F32)
    decay_pre = projected[:, 2 * key_width + value_width :]
    alpha = jnp.exp(jax.nn.log_sigmoid(decay_pre + decay_bias) / GATE_SCALE)
    new_state = alpha[:, :, None] * gla_state[:, 0] + key[:, :, None] * value[:, None, :]
    read_out = jnp.sum(query[:, :, None] * new_state, axis=1)
    gated = rms_scale(read_out, head_gain).astype(BF16)
    gated, new_state = lax.optimization_barrier((gated, new_state))

    slab_heads, slab_res = exchange(to_all(gated, slab), SLAB, slab_res)
    slab_heads = slab_heads.reshape(slab * seqs, value_width)
    head_part = lax.dot_general(
        slab_heads,
        gathered[:, in_width:],
        (((1,), (1,)), ((), ())),
        preferred_element_type=F32,
    ).astype(BF16)

    def by_owner(columns):
        return columns.reshape(rows, cores * seqs, parts, strip)

    both = jnp.concatenate([by_owner(head_part), by_owner(slab_res)], axis=3)
    both = both.transpose(0, 2, 1, 3).reshape(rows * parts, cores * seqs, 2 * strip)
    came = exchange(both, SLAB_TP).reshape(slab, heads, cores * seqs, 2 * strip)
    attention = came[..., :strip].astype(F32).sum(axis=1)
    came_res = came[:, 0, :, strip:].astype(F32)
    hidden = (came_res + attention).astype(BF16)
    hidden = hidden.transpose(1, 0, 2).reshape(cores * seqs, piece)

    all_hidden = exchange(to_all(hidden, far), FAR).reshape(tokens, piece)
    slot_part = jnp.dot(select, all_hidden, preferred_element_type=F32).astype(BF16)
    outward = jnp.broadcast_to(
        slot_part.reshape(cores, 1, CAP, piece), (cores, heads, CAP, piece)
    ).reshape(parts, CAP, piece)
    slot_hidden, ffn_gain, router_group, router_expert = exchange(
        outward, CHIPS, ffn_gain, router_group, router_expert
    )
    slot_hidden = slot_hidden.transpose(1, 0, 2).reshape(CAP, width)
    slot_rows = rms_scale(slot_hidden, ffn_gain).astype(BF16)

    group_logits = jnp.dot(slot_rows, router_group, preferred_element_type=F32)
    group_logit = jnp.sum(group_logits * own_group[None], axis=1)
    group_share = 1.0 / jnp.sum(jnp.exp(group_logits - group_logit[:, None]), axis=1)
    expert_logits = lax.dot_general(
        slot_rows, router_expert, (((1,), (1,)), ((), ())), preferred_element_type=F32
    )
    chosen = jnp.sum(expert_logits * own_lane[None], axis=1)
    rival = jnp.sum(expert_logits * rival_lane, axis=1)
    slot_weight = group_share * jax.nn.sigmoid(chosen - rival)

    gate_out = jnp.dot(slot_rows, w_gate[0], preferred_element_type=F32)
    up_out = jnp.dot(slot_rows, w_up[0], preferred_element_type=F32)
    units = (jax.nn.silu(gate_out) * up_out).astype(BF16)
    output = jnp.dot(units, w_down[0], preferred_element_type=F32) * slot_weight[:, None]
    back = output.astype(BF16).reshape(CAP, parts, piece).transpose(1, 0, 2)
    summed = exchange(back, CHIPS).reshape(cores, heads, CAP, piece).astype(F32).sum(axis=1)
    dense = lax.dot_general(
        select,
        summed.astype(BF16).reshape(cores * CAP, piece),
        (((0,), (0,)), ((), ())),
        preferred_element_type=F32,
    ).astype(BF16)
    moe, hidden = exchange(dense.reshape(far, cores * seqs, piece), FAR, hidden)
    moe = moe.astype(F32).sum(axis=0)
    layer = (hidden.astype(F32) + moe).astype(BF16)
    last = jnp.broadcast_to(
        layer.reshape(cores, 1, seqs, piece), (cores, heads, seqs, piece)
    ).reshape(parts, seqs, piece)
    layer_out = exchange(last, CHIPS).transpose(1, 0, 2).reshape(seqs, width)
    return (layer_out, new_state[:, None])


def solution(mesh):
    torus = Mesh(mesh.devices.reshape(8, 8, 2, mesh.shape["tp"]), (*EP, "tp"))
    in_specs = (
        P(EP, None),
        P(EP, "tp", None, None),
        P(),
        P(EP, "tp"),
        P(EP, "tp"),
        P(EP, "tp"),
        P(EP, "tp"),
        P("tp"),
        P(),
        P("tp", EP),
        P(),
        P(),
        P(),
        P(),
        P(EP, None, "tp"),
        P(EP, None, "tp"),
        P(EP, "tp", None),
    )
    out_specs = (P(EP, None), P(EP, "tp", None, None))
    return jax.shard_map(
        on_device, mesh=torus, in_specs=in_specs, out_specs=out_specs, check_vma=False
    )
```

```python
import functools

import jax
import jax.numpy as jnp
from jax import lax
from jax.experimental import pallas as pl
from jax.experimental.pallas import tpu as pltpu
from jax.sharding import Mesh
from jax.sharding import PartitionSpec as P

CAP = 16
EP = ("ep_0", "ep_1", "ep_2")
FAR = ("ep_0", "ep_1")
SLAB = ("ep_1", "ep_2")
SLAB_TP = ("ep_1", "ep_2", "tp")
CHIPS = ("ep_2", "tp")

EPSILON = 1e-06
GATE_SCALE = 16.0
F32 = jnp.float32
BF16 = jnp.bfloat16


def exchange(blocks, axes, *later):
    came = lax.all_to_all(blocks, axes, split_axis=0, concat_axis=0, tiled=True)
    return lax.optimization_barrier((came, *later)) if later else came


def to_all(shard, count):
    return jnp.broadcast_to(shard[None], (count, *shard.shape))


def rms_scale(values, gain_vec):
    floats = values.astype(F32)
    return (
        floats
        * lax.rsqrt(jnp.mean(floats * floats, axis=-1, keepdims=True) + EPSILON)
        * gain_vec.astype(F32)
    )


def prepare(experts_of, *refs):
    sources, (spread, select, rival, *kept), (ids, sems) = refs[:12], refs[12:-2], refs[-2:]
    *weights, ids_in = sources[:6]
    width = 0
    copies = []
    for source in weights:
        place = spread.at[0, :, pl.ds(width, source.shape[1])]
        width += source.shape[1]
        copies.append(pltpu.make_async_copy(source, place, sems.at[len(copies)]))
    copies.append(pltpu.make_async_copy(ids_in, ids, sems.at[len(copies)]))
    for source, target in zip(sources[6:], kept, strict=True):
        copies.append(pltpu.make_async_copy(source, target, sems.at[len(copies)]))
    for copy in copies:
        copy.start()
    first, core = experts_of()
    count = ids.shape[1]
    row = lax.broadcasted_iota(jnp.int32, (count, count), 0)
    col = lax.broadcasted_iota(jnp.int32, (count, count), 1)
    upper = jnp.where(row <= col, 1.0, 0.0).astype(BF16)
    copies[5].wait()
    one, two = ids[0:1, :], ids[1:2, :]
    experts = first + lax.broadcasted_iota(jnp.int32, (8, count), 0)
    named = (one == experts) | (two == experts)
    marks = jnp.where(named, 1.0, 0.0)
    ends = jnp.dot(marks.astype(BF16), upper, preferred_element_type=F32)
    slots = lax.broadcasted_iota(jnp.int32, (CAP, count), 0).astype(F32) + 1.0
    both = (one + two).astype(F32)
    own = first + core
    others = jnp.zeros((CAP, 1), F32)
    for c in range(select.shape[0] // CAP):
        mine = jnp.where(ends[c : c + 1] == slots, marks[c : c + 1], 0.0)
        select[CAP * c : CAP * (c + 1)] = mine.astype(BF16)
        total = jnp.sum(mine * both, axis=1, keepdims=True)
        others = jnp.where(core == c, total, others)
    lanes = lax.broadcasted_iota(jnp.int32, rival.shape, 1)
    rival[...] = jnp.where(lanes == others.astype(jnp.int32) - own, 1.0, 0.0)
    for copy in copies[:5]:
        copy.wait()
    own_w = spread[0]
    for depth in range(1, spread.shape[0]):
        spread[depth] = own_w
    for copy in copies[6:]:
        copy.wait()


def on_device(
    residual_in,
    gla_state,
    norm_gain,
    w_query,
    w_key,
    w_value,
    w_decay,
    decay_bias,
    head_gain,
    w_output,
    ffn_gain,
    router_group,
    router_expert,
    expert_ids,
    w_gate,
    w_up,
    w_down,
):
    depths, rows, cores = (lax.axis_size(a) for a in EP)
    heads = lax.axis_size("tp")
    slab = rows * cores
    parts = cores * heads
    far = depths * rows
    tokens = expert_ids.shape[0]
    seqs, width = residual_in.shape
    strip = w_query.shape[0]
    key_width, value_width = w_query.shape[1], w_value.shape[1]
    in_width = 3 * key_width + value_width
    held = depths * strip
    piece = width // parts
    place = lax.axis_index(SLAB)
    chip = lax.axis_index(FAR)
    core = lax.axis_index("ep_2")

    n_experts = router_expert.shape[0]

    def experts_of():
        return lax.axis_index(FAR) * cores, lax.axis_index("ep_2")

    vmem = pl.BlockSpec(memory_space=pltpu.VMEM)
    later = (residual_in, norm_gain, head_gain, ffn_gain, decay_bias, router_group.T)
    shapes = [
        pltpu.VMEM((depths, strip, in_width + value_width), BF16),
        pltpu.VMEM((cores * CAP, tokens), BF16),
        pltpu.VMEM((CAP, n_experts), F32),
        *(pltpu.VMEM(a.shape, a.dtype) for a in later),
    ]
    spread, select, rival_lane, *later = pl.pallas_call(
        functools.partial(prepare, experts_of),
        out_shape=shapes,
        in_specs=[pl.BlockSpec(memory_space=pl.ANY)] * 12,
        out_specs=[vmem] * len(shapes),
        scratch_shapes=[
            pltpu.VMEM((expert_ids.shape[1], tokens), jnp.int32),
            pltpu.SemaphoreType.DMA((12,)),
        ],
    )(w_query, w_key, w_value, w_decay, w_output.T, expert_ids.T, *later)
    residual_in, norm_gain, head_gain, ffn_gain, decay_bias, group_rows = later
    expert = lax.axis_index(EP)
    groups = router_group.shape[1]
    lanes = jnp.arange(n_experts, dtype=jnp.int32)
    own_group = jnp.arange(groups, dtype=jnp.int32) == expert // (n_experts // groups)
    own_lane = (lanes == expert).astype(F32)
    own_group = own_group.astype(F32)
    own_gain = norm_gain.reshape(depths, slab, strip)[:, place].reshape(held).astype(F32)
    res_float = residual_in.astype(F32)
    scale = lax.rsqrt(jnp.mean(res_float * res_float, axis=-1, keepdims=True) + EPSILON)
    strips = residual_in.reshape(seqs, depths, slab, strip).transpose(2, 0, 1, 3)
    strips = strips.reshape(slab, seqs, held)

    tied = lax.optimization_barrier(
        (spread, strips, select, rival_lane, own_lane, own_group, own_gain, scale)
    )
    spread, strips, select, rival_lane, own_lane, own_group, own_gain, scale = tied
    gathered = exchange(spread, "ep_0").reshape(held, in_width + value_width)
    gathered, strips = lax.optimization_barrier((gathered, strips))
    slab_res = exchange(strips, SLAB).reshape(slab * seqs, held)
    lhs = (slab_res.astype(F32) * own_gain).astype(BF16)
    sums = jnp.dot(lhs, gathered[:, :in_width], preferred_element_type=F32).astype(BF16)
    arrived, head_gain, decay_bias = exchange(
        sums.reshape(slab, seqs, in_width), SLAB, head_gain, decay_bias
    )
    projected = arrived.astype(F32).sum(axis=0) * scale

    query = projected[:, :key_width].astype(BF16).astype(F32) * key_width ** (-0.5)
    key = projected[:, key_width : 2 * key_width].astype(BF16).astype(F32)
    value = projected[:, 2 * key_width : 2 * key_width + value_width].astype(BF16).astype(F32)
    decay_pre = projected[:, 2 * key_width + value_width :]
    alpha = jnp.exp(jax.nn.log_sigmoid(decay_pre + decay_bias) / GATE_SCALE)
    new_state = alpha[:, :, None] * gla_state[:, 0] + key[:, :, None] * value[:, None, :]
    read_out = jnp.sum(query[:, :, None] * new_state, axis=1)
    gated = rms_scale(read_out, head_gain).astype(BF16)
    gated, new_state = lax.optimization_barrier((gated, new_state))

    slab_heads, slab_res = exchange(to_all(gated, slab), SLAB, slab_res)
    slab_heads = slab_heads.reshape(slab * seqs, value_width)
    head_part = lax.dot_general(
        slab_heads,
        gathered[:, in_width:],
        (((1,), (1,)), ((), ())),
        preferred_element_type=F32,
    ).astype(BF16)

    def by_owner(columns):
        return columns.reshape(rows, cores * seqs, parts, strip)

    both = jnp.concatenate([by_owner(head_part), by_owner(slab_res)], axis=3)
    both = both.transpose(0, 2, 1, 3).reshape(rows * parts, cores * seqs, 2 * strip)
    came = exchange(both, SLAB_TP).reshape(slab, heads, cores * seqs, 2 * strip)
    attention = came[..., :strip].astype(F32).sum(axis=1)
    came_res = came[:, 0, :, strip:].astype(F32)
    hidden = (came_res + attention).astype(BF16)
    hidden = hidden.transpose(1, 0, 2).reshape(cores * seqs, piece)

    all_hidden = exchange(to_all(hidden, far), FAR).reshape(tokens, piece)
    slot_part = jnp.dot(select, all_hidden, preferred_element_type=F32).astype(BF16)
    outward = jnp.broadcast_to(
        slot_part.reshape(cores, 1, CAP, piece), (cores, heads, CAP, piece)
    ).reshape(parts, CAP, piece)
    slot_hidden, ffn_gain = exchange(outward, CHIPS, ffn_gain)
    slot_hidden = slot_hidden.transpose(1, 0, 2).reshape(CAP, width)
    slot_rows = rms_scale(slot_hidden, ffn_gain).astype(BF16)

    group_logits = lax.dot_general(
        slot_rows, group_rows, (((1,), (1,)), ((), ())), preferred_element_type=F32
    )
    group_logit = jnp.sum(group_logits * own_group[None], axis=1)
    group_share = 1.0 / jnp.sum(jnp.exp(group_logits - group_logit[:, None]), axis=1)
    expert_logits = lax.dot_general(
        slot_rows, router_expert, (((1,), (1,)), ((), ())), preferred_element_type=F32
    )
    chosen = jnp.sum(expert_logits * own_lane[None], axis=1)
    rival = jnp.sum(expert_logits * rival_lane, axis=1)
    slot_weight = group_share * jax.nn.sigmoid(chosen - rival)

    gate_out = jnp.dot(slot_rows, w_gate[0], preferred_element_type=F32)
    up_out = jnp.dot(slot_rows, w_up[0], preferred_element_type=F32)
    units = (jax.nn.silu(gate_out) * up_out).astype(BF16)
    output = jnp.dot(units, w_down[0], preferred_element_type=F32) * slot_weight[:, None]
    back = output.astype(BF16).reshape(CAP, parts, piece).transpose(1, 0, 2)
    summed = exchange(back, CHIPS).reshape(cores, heads, CAP, piece).astype(F32).sum(axis=1)
    dense = lax.dot_general(
        select,
        summed.astype(BF16).reshape(cores * CAP, piece),
        (((0,), (0,)), ((), ())),
        preferred_element_type=F32,
    ).astype(BF16)
    moe, hidden = exchange(dense.reshape(far, cores * seqs, piece), FAR, hidden)
    moe = moe.astype(F32).sum(axis=0)
    layer = (hidden.astype(F32) + moe).astype(BF16)
    last = jnp.broadcast_to(
        layer.reshape(cores, 1, seqs, piece), (cores, heads, seqs, piece)
    ).reshape(parts, seqs, piece)
    layer_out = exchange(last, CHIPS).transpose(1, 0, 2).reshape(seqs, width)
    return (layer_out, new_state[:, None])


def solution(mesh):
    torus = Mesh(mesh.devices.reshape(8, 8, 2, mesh.shape["tp"]), (*EP, "tp"))
    in_specs = (
        P(EP, None),
        P(EP, "tp", None, None),
        P(),
        P(EP, "tp"),
        P(EP, "tp"),
        P(EP, "tp"),
        P(EP, "tp"),
        P("tp"),
        P(),
        P("tp", EP),
        P(),
        P(),
        P(),
        P(),
        P(EP, None, "tp"),
        P(EP, None, "tp"),
        P(EP, "tp", None),
    )
    out_specs = (P(EP, None), P(EP, "tp", None, None))
    return jax.shard_map(
        on_device, mesh=torus, in_specs=in_specs, out_specs=out_specs, check_vma=False
    )
```

```python
import functools

import jax
import jax.numpy as jnp
from jax import lax
from jax.experimental import pallas as pl
from jax.experimental.pallas import tpu as pltpu
from jax.sharding import Mesh
from jax.sharding import PartitionSpec as P

CAP = 16
EP = ("ep_0", "ep_1", "ep_2")
FAR = ("ep_0", "ep_1")
SLAB = ("ep_1", "ep_2")
SLAB_TP = ("ep_1", "ep_2", "tp")
CHIPS = ("ep_2", "tp")

EPSILON = 1e-06
GATE_SCALE = 16.0
F32 = jnp.float32
BF16 = jnp.bfloat16


def exchange(blocks, axes, *later):
    came = lax.all_to_all(blocks, axes, split_axis=0, concat_axis=0, tiled=True)
    return lax.optimization_barrier((came, *later)) if later else came


def on_chip(array):
    return pltpu.with_memory_space_constraint(array, pltpu.VMEM)


def to_all(shard, count):
    return jnp.broadcast_to(shard[None], (count, *shard.shape))


def rms_scale(values, gain_vec):
    floats = values.astype(F32)
    return (
        floats
        * lax.rsqrt(jnp.mean(floats * floats, axis=-1, keepdims=True) + EPSILON)
        * gain_vec.astype(F32)
    )


def prepare(experts_of, *refs):
    sources, (spread, along, select, rival, *kept), (ids, sems) = refs[:13], refs[13:-2], refs[-2:]
    *weights, ids_in = sources[:6]
    width = 0
    copies = []
    for source in weights:
        place = spread.at[0, :, pl.ds(width, source.shape[1])]
        width += source.shape[1]
        copies.append(pltpu.make_async_copy(source, place, sems.at[len(copies)]))
    copies.append(pltpu.make_async_copy(ids_in, ids, sems.at[len(copies)]))
    for source, target in zip(sources[6:], kept, strict=True):
        copies.append(pltpu.make_async_copy(source, target, sems.at[len(copies)]))
    for copy in copies:
        copy.start()
    first, core, place, slab = experts_of()
    count = ids.shape[1]
    row = lax.broadcasted_iota(jnp.int32, (count, count), 0)
    col = lax.broadcasted_iota(jnp.int32, (count, count), 1)
    upper = jnp.where(row <= col, 1.0, 0.0).astype(BF16)
    copies[5].wait()
    one, two = ids[0:1, :], ids[1:2, :]
    depths = spread.shape[0]
    index = lax.broadcasted_iota(jnp.int32, (2 * depths, count), 0)
    experts = jnp.where(index < depths, index * slab + place, index - depths + first)
    named = (one == experts) | (two == experts)
    marks = jnp.where(named, 1.0, 0.0)
    ends = jnp.dot(marks.astype(BF16), upper, preferred_element_type=F32)
    slots = lax.broadcasted_iota(jnp.int32, (CAP, count), 0).astype(F32) + 1.0
    both = (one + two).astype(F32)
    own = first + core
    others = jnp.zeros((CAP, 1), F32)


    def slots_of(at):
        return jnp.where(ends[at : at + 1] == slots, marks[at : at + 1], 0.0)

    for depth in range(depths):
        along[CAP * depth : CAP * (depth + 1)] = slots_of(depth).astype(BF16)
    for c in range(select.shape[0] // CAP):
        mine = slots_of(depths + c)
        select[CAP * c : CAP * (c + 1)] = mine.astype(BF16)
        total = jnp.sum(mine * both, axis=1, keepdims=True)
        others = jnp.where(core == c, total, others)
    lanes = lax.broadcasted_iota(jnp.int32, rival.shape, 1)
    rival[...] = jnp.where(lanes == others.astype(jnp.int32) - own, 1.0, 0.0)
    for copy in copies[:5]:
        copy.wait()
    own_w = spread[0]
    for depth in range(1, spread.shape[0]):
        spread[depth] = own_w
    for copy in copies[6:]:
        copy.wait()


def pack(heads_ref, held_ref, res_ref, out_ref):
    value_width = heads_ref.shape[1]
    part = lax.dot_general(
        heads_ref[...],
        held_ref[:, held_ref.shape[1] - value_width :],
        (((1,), (1,)), ((), ())),
        preferred_element_type=F32,
    )
    with_res = (lax.axis_index("tp") == 0).astype(F32)
    part = part + res_ref[...].astype(F32) * with_res
    lines, lanes = out_ref.shape[1:]
    count = part.shape[0] // lines
    size = lanes // count
    group = lax.broadcasted_iota(jnp.int32, (lines, lanes), 1) // size
    for quarter in range(count):
        block = jnp.zeros((lines, lanes), F32)
        for k in range(count):
            rows = part[lines * k : lines * (k + 1)]
            moved = pltpu.roll(rows, (size * (k - quarter)) % lanes, 1)
            block = jnp.where(group == k, moved, block)
        block = block.astype(BF16)
        for at in range(out_ref.shape[0] // count):
            out_ref[count * at + quarter] = block


def dispatch(at_place, came_ref, along_ref, out_ref, hidden_ref, rows_ref, all_ref):
    depth, row, core = at_place()
    count, lines, lanes = came_ref.shape
    heads = lanes // (2 * 16)
    all_ref[...] = jnp.zeros_like(all_ref)
    hidden = []
    for at in range(count // heads):
        total = came_ref[heads * at].astype(F32)
        for head in range(1, heads):
            total = total + came_ref[heads * at + head].astype(F32)
        hidden.append(total.astype(BF16).astype(F32))
    group = lax.broadcasted_iota(jnp.int32, (lines, lanes), 1) // 16
    for k in range(heads):
        for strip in range(2):
            for half in range(2):
                block = jnp.zeros((lines, lanes), F32)
                for m in range(8):
                    shift = (16 * m - 32 * k - 16 * strip) % lanes
                    moved = pltpu.roll(hidden[8 * half + m], shift, 1)
                    block = jnp.where(group == m, moved, block)
                at = 256 * strip + 128 * half
                rows_ref[lines * k : lines * (k + 1), at : at + lanes] = block
    rows = rows_ref[...].astype(BF16)
    size = rows.shape[0]
    all_ref[pl.ds(pl.multiple_of(depth * size, size), size)] = rows
    slots = jnp.dot(along_ref[...], all_ref[...], preferred_element_type=F32).astype(BF16)
    for at in range(out_ref.shape[0]):
        out_ref[at] = slots[CAP * at : CAP * (at + 1)]
    own, piece = hidden_ref.shape
    here = lax.broadcasted_iota(jnp.int32, (8, size), 0)
    there = lax.broadcasted_iota(jnp.int32, (8, size), 1)
    pick = jnp.where(there == here + own * row, 1.0, 0.0).astype(BF16)
    mine = jnp.dot(pick, rows, preferred_element_type=F32)
    mine = jnp.where(core == 0, mine[:, :piece], mine[:, piece:])
    hidden_ref[...] = mine[:own].astype(BF16)


def on_device(
    residual_in,
    gla_state,
    norm_gain,
    w_query,
    w_key,
    w_value,
    w_decay,
    decay_bias,
    head_gain,
    w_output,
    ffn_gain,
    router_group,
    router_expert,
    expert_ids,
    w_gate,
    w_up,
    w_down,
):
    depths, rows, cores = (lax.axis_size(a) for a in EP)
    heads = lax.axis_size("tp")
    slab = rows * cores
    parts = cores * heads
    far = depths * rows
    tokens = expert_ids.shape[0]
    seqs, width = residual_in.shape
    strip = w_query.shape[0]
    key_width, value_width = w_query.shape[1], w_value.shape[1]
    in_width = 3 * key_width + value_width
    held = depths * strip
    piece = width // parts
    place = lax.axis_index(SLAB)
    chip = lax.axis_index(FAR)
    core = lax.axis_index("ep_2")

    n_experts = router_expert.shape[0]

    def experts_of():
        core = lax.axis_index("ep_2")
        return lax.axis_index(FAR) * cores, core, lax.axis_index(SLAB), slab

    vmem = pl.BlockSpec(memory_space=pltpu.VMEM)
    later = (residual_in, norm_gain, head_gain, ffn_gain, decay_bias, router_group.T)
    later += (router_expert,)
    shapes = [
        pltpu.VMEM((depths, strip, in_width + value_width), BF16),
        pltpu.VMEM((depths * CAP, tokens), BF16),
        pltpu.VMEM((cores * CAP, tokens), BF16),
        pltpu.VMEM((CAP, n_experts), F32),
        *(pltpu.VMEM(a.shape, a.dtype) for a in later),
    ]
    spread, along, select, rival_lane, *later = pl.pallas_call(
        functools.partial(prepare, experts_of),
        out_shape=shapes,
        in_specs=[pl.BlockSpec(memory_space=pl.ANY)] * 13,
        out_specs=[vmem] * len(shapes),
        scratch_shapes=[
            pltpu.VMEM((expert_ids.shape[1], tokens), jnp.int32),
            pltpu.SemaphoreType.DMA((13,)),
        ],
    )(w_query, w_key, w_value, w_decay, w_output.T, expert_ids.T, *later)
    residual_in, norm_gain, head_gain, ffn_gain, decay_bias, group_rows, router_expert = later
    expert = lax.axis_index(EP)
    groups = router_group.shape[1]
    lanes = jnp.arange(n_experts, dtype=jnp.int32)
    own_group = jnp.arange(groups, dtype=jnp.int32) == expert // (n_experts // groups)
    own_lane = (lanes == expert).astype(F32)
    own_group = own_group.astype(F32)
    own_gain = norm_gain.reshape(depths, slab, strip)[:, place].reshape(held).astype(F32)
    res_float = residual_in.astype(F32)
    scale = lax.rsqrt(jnp.mean(res_float * res_float, axis=-1, keepdims=True) + EPSILON)
    strips = residual_in.reshape(seqs, depths, slab, strip).transpose(2, 0, 1, 3)
    strips = strips.reshape(slab, seqs, held)

    tied = lax.optimization_barrier(
        (spread, strips, along, select, rival_lane, own_lane, own_group, own_gain, scale)
    )
    spread, strips, along, select, rival_lane, own_lane, own_group, own_gain, scale = tied
    gathered = exchange(spread, "ep_0").reshape(held, in_width + value_width)
    gathered, strips = lax.optimization_barrier((gathered, strips))
    slab_res = exchange(strips, SLAB).reshape(slab * seqs, held)
    lhs = (slab_res.astype(F32) * own_gain).astype(BF16)
    sums = jnp.dot(lhs, gathered[:, :in_width], preferred_element_type=F32).astype(BF16)
    arrived, head_gain, decay_bias = exchange(
        sums.reshape(slab, seqs, in_width), SLAB, head_gain, decay_bias
    )
    projected = arrived.astype(F32).sum(axis=0) * scale

    query = projected[:, :key_width].astype(BF16).astype(F32) * key_width ** (-0.5)
    key = projected[:, key_width : 2 * key_width].astype(BF16).astype(F32)
    value = projected[:, 2 * key_width : 2 * key_width + value_width].astype(BF16).astype(F32)
    decay_pre = projected[:, 2 * key_width + value_width :]
    alpha = jnp.exp(jax.nn.log_sigmoid(decay_pre + decay_bias) / GATE_SCALE)
    new_state = alpha[:, :, None] * gla_state[:, 0] + key[:, :, None] * value[:, None, :]
    read_out = jnp.sum(query[:, :, None] * new_state, axis=1)
    gated = rms_scale(read_out, head_gain).astype(BF16)
    gated, new_state = lax.optimization_barrier((gated, new_state))

    slab_heads, slab_res = exchange(to_all(gated, slab), SLAB, slab_res)
    slab_heads = slab_heads.reshape(slab * seqs, value_width)
    lines = slab * seqs // (128 // (held // heads))
    came = pl.pallas_call(
        pack,
        out_shape=pltpu.VMEM((slab * heads, lines, held), BF16),
        in_specs=[vmem] * 3,
        out_specs=vmem,
    )(*map(on_chip, (slab_heads, gathered, slab_res)))
    came = exchange(came, SLAB_TP)

    def at_place():
        return lax.axis_index("ep_0"), lax.axis_index("ep_1"), lax.axis_index("ep_2")

    outward, hidden = pl.pallas_call(
        functools.partial(dispatch, at_place),
        out_shape=[
            pltpu.VMEM((depths, CAP, width // heads), BF16),
            pltpu.VMEM((cores * seqs, piece), BF16),
        ],
        in_specs=[vmem] * 2,
        out_specs=[vmem] * 2,
        scratch_shapes=[
            pltpu.VMEM((slab * seqs, width // heads), F32),
            pltpu.VMEM((tokens, width // heads), BF16),
        ],
    )(on_chip(came), on_chip(along))
    slot_part = exchange(outward, "ep_0").astype(F32).sum(axis=0).astype(BF16)
    slot_hidden, ffn_gain = exchange(to_all(slot_part, heads), "tp", ffn_gain)
    slot_hidden = slot_hidden.transpose(1, 0, 2).reshape(CAP, width)
    slot_rows = rms_scale(slot_hidden, ffn_gain).astype(BF16)

    group_logits = lax.dot_general(
        slot_rows, group_rows, (((1,), (1,)), ((), ())), preferred_element_type=F32
    )
    group_logit = jnp.sum(group_logits * own_group[None], axis=1)
    group_share = 1.0 / jnp.sum(jnp.exp(group_logits - group_logit[:, None]), axis=1)
    expert_logits = lax.dot_general(
        slot_rows, router_expert, (((1,), (1,)), ((), ())), preferred_element_type=F32
    )
    chosen = jnp.sum(expert_logits * own_lane[None], axis=1)
    rival = jnp.sum(expert_logits * rival_lane, axis=1)
    slot_weight = group_share * jax.nn.sigmoid(chosen - rival)

    gate_out = jnp.dot(slot_rows, w_gate[0], preferred_element_type=F32)
    up_out = jnp.dot(slot_rows, w_up[0], preferred_element_type=F32)
    units = (jax.nn.silu(gate_out) * up_out).astype(BF16)
    output = jnp.dot(units, w_down[0], preferred_element_type=F32) * slot_weight[:, None]
    back = output.astype(BF16).reshape(CAP, heads, cores, piece).transpose(2, 1, 0, 3)
    back = back.reshape(parts, CAP, piece)
    summed = exchange(back, CHIPS).reshape(cores, heads, CAP, piece).astype(F32).sum(axis=1)
    dense = lax.dot_general(
        select,
        summed.astype(BF16).reshape(cores * CAP, piece),
        (((0,), (0,)), ((), ())),
        preferred_element_type=F32,
    ).astype(BF16)
    moe, hidden = exchange(dense.reshape(far, cores * seqs, piece), FAR, hidden)
    moe = moe.astype(F32).sum(axis=0)
    layer = (hidden.astype(F32) + moe).astype(BF16)
    last = jnp.broadcast_to(
        layer.reshape(cores, 1, seqs, piece), (cores, heads, seqs, piece)
    ).reshape(parts, seqs, piece)
    layer_out = exchange(last, CHIPS).reshape(cores, heads, seqs, piece)
    layer_out = layer_out.transpose(2, 1, 0, 3).reshape(seqs, width)
    return (layer_out, new_state[:, None])


def solution(mesh):
    torus = Mesh(mesh.devices.reshape(8, 8, 2, mesh.shape["tp"]), (*EP, "tp"))
    in_specs = (
        P(EP, None),
        P(EP, "tp", None, None),
        P(),
        P(EP, "tp"),
        P(EP, "tp"),
        P(EP, "tp"),
        P(EP, "tp"),
        P("tp"),
        P(),
        P("tp", EP),
        P(),
        P(),
        P(),
        P(),
        P(EP, None, "tp"),
        P(EP, None, "tp"),
        P(EP, "tp", None),
    )
    out_specs = (P(EP, None), P(EP, "tp", None, None))
    return jax.shard_map(
        on_device, mesh=torus, in_specs=in_specs, out_specs=out_specs, check_vma=False
    )
```

```python
import functools

import jax
import jax.numpy as jnp
from jax import lax
from jax.experimental import pallas as pl
from jax.experimental.pallas import tpu as pltpu
from jax.sharding import Mesh
from jax.sharding import PartitionSpec as P

CAP = 16
EP = ("ep_0", "ep_1", "ep_2")
FAR = ("ep_0", "ep_1")
SLAB = ("ep_1", "ep_2")
SLAB_TP = ("ep_1", "ep_2", "tp")
CHIPS = ("tp", "ep_2")
DEPTH_TP = ("ep_0", "tp")

EPSILON = 1e-06
GATE_SCALE = 16.0
F32 = jnp.float32
BF16 = jnp.bfloat16


def exchange(blocks, axes, *later):
    came = lax.all_to_all(blocks, axes, split_axis=0, concat_axis=0, tiled=True)
    return lax.optimization_barrier((came, *later)) if later else came


def on_chip(array):
    return pltpu.with_memory_space_constraint(array, pltpu.VMEM)


def to_all(shard, count):
    return jnp.broadcast_to(shard[None], (count, *shard.shape))


def prepare(experts_of, *refs):
    sources, (spread, along, select, rival, *kept), (ids, sems) = refs[:12], refs[12:-2], refs[-2:]
    *weights, ids_in = sources[:6]
    width = 0
    copies = []
    for source in weights:
        place = spread.at[0, :, pl.ds(width, source.shape[1])]
        width += source.shape[1]
        copies.append(pltpu.make_async_copy(source, place, sems.at[len(copies)]))
    copies.append(pltpu.make_async_copy(ids_in, ids, sems.at[len(copies)]))
    for source, target in zip(sources[6:], kept, strict=True):
        copies.append(pltpu.make_async_copy(source, target, sems.at[len(copies)]))
    for copy in copies:
        copy.start()
    first, core, place, slab = experts_of()
    count = ids.shape[1]
    row = lax.broadcasted_iota(jnp.int32, (count, count), 0)
    col = lax.broadcasted_iota(jnp.int32, (count, count), 1)
    upper = jnp.where(row <= col, 1.0, 0.0).astype(BF16)
    copies[5].wait()
    one, two = ids[0:1, :], ids[1:2, :]
    depths = spread.shape[0]
    index = lax.broadcasted_iota(jnp.int32, (2 * depths, count), 0)
    experts = jnp.where(index < depths, index * slab + place, index - depths + first)
    named = (one == experts) | (two == experts)
    marks = jnp.where(named, 1.0, 0.0)
    ends = jnp.dot(marks.astype(BF16), upper, preferred_element_type=F32)
    slots = lax.broadcasted_iota(jnp.int32, (CAP, count), 0).astype(F32) + 1.0
    both = (one + two).astype(F32)
    own = first + core
    others = jnp.zeros((CAP, 1), F32)


    def slots_of(at):
        return jnp.where(ends[at : at + 1] == slots, marks[at : at + 1], 0.0)

    for depth in range(depths):
        along[CAP * depth : CAP * (depth + 1)] = slots_of(depth).astype(BF16)
    for c in range(select.shape[0] // CAP):
        mine = slots_of(depths + c)
        select[CAP * c : CAP * (c + 1)] = mine.astype(BF16)
        total = jnp.sum(mine * both, axis=1, keepdims=True)
        others = jnp.where(core == c, total, others)
    lanes = lax.broadcasted_iota(jnp.int32, rival.shape, 1)
    rival[...] = jnp.where(lanes == others.astype(jnp.int32) - own, 1.0, 0.0)
    for copy in copies[:5]:
        copy.wait()
    own_w = spread[0]
    for depth in range(1, spread.shape[0]):
        spread[depth] = own_w
    for copy in copies[6:]:
        copy.wait()


def advance(came_ref, res_ref, bias_ref, gain_ref, old_ref, out_ref, new_ref, held_ref, sems):
    seqs, key_width, value_width = old_ref.shape
    total = came_ref[0].astype(F32)
    for at in range(1, came_ref.shape[0]):
        total = total + came_ref[at].astype(F32)
    res = res_ref[...].astype(F32)
    total = total * lax.rsqrt(jnp.mean(res * res, axis=1, keepdims=True) + EPSILON)
    query = total[:, :key_width].astype(BF16).astype(F32) * key_width ** (-0.5)
    key = total[:, key_width : 2 * key_width].astype(BF16).astype(F32)
    value = total[:, 2 * key_width : 2 * key_width + value_width].astype(BF16).astype(F32)
    pre = total[:, 2 * key_width + value_width :] + bias_ref[...]
    log_decay = (jnp.minimum(pre, 0.0) - jnp.log1p(jnp.exp(-jnp.abs(pre)))) / GATE_SCALE
    down = jnp.concatenate([query, key, jnp.exp(log_decay), jnp.zeros_like(query)], axis=0).T
    copies = []
    gated = []
    for seq in range(seqs):
        read = jnp.zeros((1, value_width), F32)
        for at in range(0, key_width, 32):
            block = down[at : at + 32]
            query_col = block[:, seq : seq + 1]
            key_col = block[:, seqs + seq : seqs + seq + 1]
            alpha_col = block[:, 2 * seqs + seq : 2 * seqs + seq + 1]
            new = alpha_col * old_ref[seq, at : at + 32] + key_col * value[seq : seq + 1]
            held_ref[seq, at : at + 32] = new
            read = read + jnp.sum(query_col * new, axis=0, keepdims=True)
        copies.append(pltpu.make_async_copy(held_ref.at[seq], new_ref.at[seq], sems.at[seq]))
        copies[-1].start()
        mean = jnp.mean(read * read, axis=1, keepdims=True)
        gated.append(read * lax.rsqrt(mean + EPSILON) * gain_ref[...])
    gated = jnp.concatenate(gated, axis=0).astype(BF16)
    for at in range(out_ref.shape[0]):
        out_ref[at] = gated
    for copy in copies:
        copy.wait()


def mix(
    which,
    expert_ref,
    came_ref,
    gain_ref,
    group_ref,
    rival_ref,
    gate_ref,
    up_ref,
    down_ref,
    out_ref,
    rows_ref,
):
    expert = which()
    count, slots, size = came_ref.shape
    quarters = rows_ref.shape[1] // size
    for quarter in range(quarters):
        total = came_ref[quarter].astype(F32)
        for at in range(quarters + quarter, count, quarters):
            total = total + came_ref[at].astype(F32)
        rows_ref[:, size * quarter : size * (quarter + 1)] = total
    rows = rows_ref[...]
    mean = jnp.mean(rows * rows, axis=1, keepdims=True)
    rows = (rows * lax.rsqrt(mean + EPSILON) * gain_ref[...]).astype(BF16)
    gate = jnp.dot(rows, gate_ref[...], preferred_element_type=F32)
    up = jnp.dot(rows, up_ref[...], preferred_element_type=F32)
    over = (((1,), (1,)), ((), ()))
    groups = lax.dot_general(rows, group_ref[...], over, preferred_element_type=F32)
    logits = lax.dot_general(rows, expert_ref[...], over, preferred_element_type=F32)
    units = (gate * jax.nn.sigmoid(gate) * up).astype(BF16)
    output = jnp.dot(units, down_ref[...], preferred_element_type=F32)
    of_group = lax.broadcasted_iota(jnp.int32, groups.shape, 1)
    own = of_group == expert // (logits.shape[1] // groups.shape[1])
    group_logit = jnp.sum(jnp.where(own, groups, 0.0), axis=1, keepdims=True)
    share = 1.0 / jnp.sum(jnp.exp(groups - group_logit), axis=1, keepdims=True)
    lanes = lax.broadcasted_iota(jnp.int32, logits.shape, 1)
    chosen = jnp.sum(jnp.where(lanes == expert, logits, 0.0), axis=1, keepdims=True)
    rival = jnp.sum(logits * rival_ref[...], axis=1, keepdims=True)
    output = (output * (share * jax.nn.sigmoid(chosen - rival))).astype(BF16)
    piece = out_ref.shape[2]
    for at in range(out_ref.shape[0]):
        out_ref[at] = output[:, piece * at : piece * (at + 1)]


def pack(heads_ref, held_ref, res_ref, out_ref):
    value_width = heads_ref.shape[1]
    part = lax.dot_general(
        heads_ref[...],
        held_ref[:, held_ref.shape[1] - value_width :],
        (((1,), (1,)), ((), ())),
        preferred_element_type=F32,
    )
    with_res = (lax.axis_index("tp") == 0).astype(F32)
    part = part + res_ref[...].astype(F32) * with_res
    lines, lanes = out_ref.shape[1:]
    count = part.shape[0] // lines
    size = lanes // count
    group = lax.broadcasted_iota(jnp.int32, (lines, lanes), 1) // size
    for quarter in range(count):
        block = jnp.zeros((lines, lanes), F32)
        for k in range(count):
            rows = part[lines * k : lines * (k + 1)]
            moved = pltpu.roll(rows, (size * (k - quarter)) % lanes, 1)
            block = jnp.where(group == k, moved, block)
        block = block.astype(BF16)
        for at in range(out_ref.shape[0] // count):
            out_ref[count * at + quarter] = block


def dispatch(at_place, came_ref, along_ref, _, out_ref, hidden_ref, rows_ref, all_ref):
    depth, row, core = at_place()
    count, lines, lanes = came_ref.shape
    heads = lanes // (2 * 16)
    all_ref[...] = jnp.zeros_like(all_ref)
    hidden = []
    for at in range(count // heads):
        total = came_ref[heads * at].astype(F32)
        for head in range(1, heads):
            total = total + came_ref[heads * at + head].astype(F32)
        hidden.append(total.astype(BF16).astype(F32))
    group = lax.broadcasted_iota(jnp.int32, (lines, lanes), 1) // 16
    for k in range(heads):
        for strip in range(2):
            for half in range(2):
                block = jnp.zeros((lines, lanes), F32)
                for m in range(8):
                    shift = (16 * m - 32 * k - 16 * strip) % lanes
                    moved = pltpu.roll(hidden[8 * half + m], shift, 1)
                    block = jnp.where(group == m, moved, block)
                at = 256 * strip + 128 * half
                rows_ref[lines * k : lines * (k + 1), at : at + lanes] = block
    rows = rows_ref[...].astype(BF16)
    size = rows.shape[0]
    all_ref[pl.ds(pl.multiple_of(depth * size, size), size)] = rows
    slots = jnp.dot(along_ref[...], all_ref[...], preferred_element_type=F32).astype(BF16)
    for at in range(out_ref.shape[0]):
        first = CAP * (at // heads)
        out_ref[at] = slots[first : first + CAP]
    own, piece = hidden_ref.shape
    here = lax.broadcasted_iota(jnp.int32, (8, size), 0)
    there = lax.broadcasted_iota(jnp.int32, (8, size), 1)
    pick = jnp.where(there == here + own * row, 1.0, 0.0).astype(BF16)
    mine = jnp.dot(pick, rows, preferred_element_type=F32)
    mine = jnp.where(core == 0, mine[:, :piece], mine[:, piece:])
    hidden_ref[...] = mine[:own].astype(BF16)


def on_device(
    residual_in,
    gla_state,
    norm_gain,
    w_query,
    w_key,
    w_value,
    w_decay,
    decay_bias,
    head_gain,
    w_output,
    ffn_gain,
    router_group,
    router_expert,
    expert_ids,
    w_gate,
    w_up,
    w_down,
):
    depths, rows, cores = (lax.axis_size(a) for a in EP)
    heads = lax.axis_size("tp")
    slab = rows * cores
    parts = cores * heads
    far = depths * rows
    tokens = expert_ids.shape[0]
    seqs, width = residual_in.shape
    strip = w_query.shape[0]
    key_width, value_width = w_query.shape[1], w_value.shape[1]
    in_width = 3 * key_width + value_width
    held = depths * strip
    piece = width // parts
    place = lax.axis_index(SLAB)
    chip = lax.axis_index(FAR)
    core = lax.axis_index("ep_2")

    n_experts = router_expert.shape[0]

    def experts_of():
        core = lax.axis_index("ep_2")
        return lax.axis_index(FAR) * cores, core, lax.axis_index(SLAB), slab

    vmem = pl.BlockSpec(memory_space=pltpu.VMEM)
    later = (residual_in, norm_gain, head_gain, ffn_gain, decay_bias, router_group.T)
    shapes = [
        pltpu.VMEM((depths, strip, in_width + value_width), BF16),
        pltpu.VMEM((depths * CAP, tokens), BF16),
        pltpu.VMEM((cores * CAP, tokens), BF16),
        pltpu.VMEM((CAP, n_experts), F32),
        *(pltpu.VMEM(a.shape, a.dtype) for a in later),
    ]
    spread, along, select, rival_lane, *later = pl.pallas_call(
        functools.partial(prepare, experts_of),
        out_shape=shapes,
        in_specs=[pl.BlockSpec(memory_space=pl.ANY)] * 12,
        out_specs=[vmem] * len(shapes),
        scratch_shapes=[
            pltpu.VMEM((expert_ids.shape[1], tokens), jnp.int32),
            pltpu.SemaphoreType.DMA((12,)),
        ],
    )(w_query, w_key, w_value, w_decay, w_output.T, expert_ids.T, *later)
    residual_in, norm_gain, head_gain, ffn_gain, decay_bias, group_rows = later
    head_gain = head_gain.astype(F32)[None]
    ffn_gain = ffn_gain.astype(F32)[None]
    decay_bias = decay_bias[None]
    own_gain = norm_gain.reshape(depths, slab, strip)[:, place].reshape(held).astype(F32)
    strips = residual_in.reshape(seqs, depths, slab, strip).transpose(2, 0, 1, 3)
    strips = strips.reshape(slab, seqs, held)

    tied = lax.optimization_barrier(
        (spread, strips, along, select, rival_lane, own_gain)
        + (head_gain, ffn_gain, decay_bias)
    )
    spread, strips, along, select, rival_lane, own_gain, *tied = tied
    head_gain, ffn_gain, decay_bias = tied
    gathered = exchange(spread, "ep_0").reshape(held, in_width + value_width)
    gathered, strips = lax.optimization_barrier((gathered, strips))
    slab_res = exchange(strips, SLAB).reshape(slab * seqs, held)
    lhs = (slab_res.astype(F32) * own_gain).astype(BF16)
    sums = jnp.dot(lhs, gathered[:, :in_width], preferred_element_type=F32).astype(BF16)
    arrived = exchange(sums.reshape(slab, seqs, in_width), SLAB)
    gated, new_state = pl.pallas_call(
        advance,
        out_shape=[
            pltpu.VMEM((slab, seqs, value_width), BF16),
            jax.ShapeDtypeStruct((seqs, key_width, value_width), F32),
        ],
        in_specs=[vmem] * 5,
        out_specs=[vmem, pl.BlockSpec(memory_space=pl.ANY)],
        scratch_shapes=[
            pltpu.VMEM((seqs, key_width, value_width), F32),
            pltpu.SemaphoreType.DMA((seqs,)),
        ],
    )(*map(on_chip, (arrived, residual_in, decay_bias, head_gain, gla_state[:, 0])))

    slab_heads, slab_res = exchange(gated, SLAB, slab_res)
    slab_heads = slab_heads.reshape(slab * seqs, value_width)
    lines = slab * seqs // (128 // (held // heads))
    came = pl.pallas_call(
        pack,
        out_shape=pltpu.VMEM((slab * heads, lines, held), BF16),
        in_specs=[vmem] * 3,
        out_specs=vmem,
    )(*map(on_chip, (slab_heads, gathered, slab_res)))
    came = exchange(came, SLAB_TP)
    router = on_chip(router_expert)

    def at_place():
        return lax.axis_index("ep_0"), lax.axis_index("ep_1"), lax.axis_index("ep_2")

    outward, hidden = pl.pallas_call(
        functools.partial(dispatch, at_place),
        out_shape=[
            pltpu.VMEM((depths * heads, CAP, width // heads), BF16),
            pltpu.VMEM((cores * seqs, piece), BF16),
        ],
        in_specs=[vmem] * 3,
        out_specs=[vmem] * 2,
        scratch_shapes=[
            pltpu.VMEM((slab * seqs, width // heads), F32),
            pltpu.VMEM((tokens, width // heads), BF16),
        ],
    )(on_chip(came), on_chip(along), router)
    came = exchange(outward, DEPTH_TP)
    operands = (came, ffn_gain, group_rows, rival_lane)
    operands += (w_gate[0], w_up[0], w_down[0])
    back = pl.pallas_call(
        functools.partial(mix, lambda: lax.axis_index(EP)),
        out_shape=pltpu.VMEM((parts, CAP, piece), BF16),
        in_specs=[vmem] * (1 + len(operands)),
        out_specs=vmem,
        scratch_shapes=[pltpu.VMEM((CAP, width), F32)],
    )(router, *map(on_chip, operands))
    summed = exchange(back, CHIPS).reshape(heads, cores, CAP, piece).astype(F32).sum(axis=0)
    dense = lax.dot_general(
        select,
        summed.astype(BF16).reshape(cores * CAP, piece),
        (((0,), (0,)), ((), ())),
        preferred_element_type=F32,
    ).astype(BF16)
    moe, hidden = exchange(dense.reshape(far, cores * seqs, piece), FAR, hidden)
    moe = moe.astype(F32).sum(axis=0)
    layer = (hidden.astype(F32) + moe).astype(BF16)
    last = to_all(layer.reshape(cores, seqs, piece), heads).reshape(parts, seqs, piece)
    layer_out = exchange(last, CHIPS).transpose(1, 0, 2).reshape(seqs, width)
    return (layer_out, new_state[:, None])


def solution(mesh):
    torus = Mesh(mesh.devices.reshape(8, 8, 2, mesh.shape["tp"]), (*EP, "tp"))
    in_specs = (
        P(EP, None),
        P(EP, "tp", None, None),
        P(),
        P(EP, "tp"),
        P(EP, "tp"),
        P(EP, "tp"),
        P(EP, "tp"),
        P("tp"),
        P(),
        P("tp", EP),
        P(),
        P(),
        P(),
        P(),
        P(EP, None, "tp"),
        P(EP, None, "tp"),
        P(EP, "tp", None),
    )
    out_specs = (P(EP, None), P(EP, "tp", None, None))
    return jax.shard_map(
        on_device, mesh=torus, in_specs=in_specs, out_specs=out_specs, check_vma=False
    )
```

```python
import functools

import jax
import jax.numpy as jnp
from jax import lax
from jax.experimental import pallas as pl
from jax.experimental.pallas import tpu as pltpu
from jax.sharding import Mesh
from jax.sharding import PartitionSpec as P

CAP = 16
EP = ("ep_0", "ep_1", "ep_2")
FAR = ("ep_0", "ep_1")
SLAB = ("ep_1", "ep_2")
SLAB_TP = ("ep_1", "ep_2", "tp")
CHIPS = ("tp", "ep_2")

EPSILON = 1e-06
GATE_SCALE = 16.0
F32 = jnp.float32
BF16 = jnp.bfloat16


def exchange(blocks, axes, *later):
    came = lax.all_to_all(blocks, axes, split_axis=0, concat_axis=0, tiled=True)
    return lax.optimization_barrier((came, *later)) if later else came


def on_chip(array):
    return pltpu.with_memory_space_constraint(array, pltpu.VMEM)


def to_all(shard, count):
    return jnp.broadcast_to(shard[None], (count, *shard.shape))


def prepare(experts_of, *refs):
    sources, (spread, along, select, rival, *kept), (ids, sems) = refs[:12], refs[12:-2], refs[-2:]
    *weights, ids_in = sources[:6]
    width = 0
    copies = []
    for source in weights:
        place = spread.at[0, :, pl.ds(width, source.shape[1])]
        width += source.shape[1]
        copies.append(pltpu.make_async_copy(source, place, sems.at[len(copies)]))
    copies.append(pltpu.make_async_copy(ids_in, ids, sems.at[len(copies)]))
    for source, target in zip(sources[6:], kept, strict=True):
        copies.append(pltpu.make_async_copy(source, target, sems.at[len(copies)]))
    for copy in copies:
        copy.start()
    first, core, place, slab = experts_of()
    count = ids.shape[1]
    row = lax.broadcasted_iota(jnp.int32, (count, count), 0)
    col = lax.broadcasted_iota(jnp.int32, (count, count), 1)
    upper = jnp.where(row <= col, 1.0, 0.0).astype(BF16)
    copies[5].wait()
    one, two = ids[0:1, :], ids[1:2, :]
    spans = along.shape[0] // CAP
    cores = select.shape[0] // CAP
    index = lax.broadcasted_iota(jnp.int32, (spans + 8, count), 0)
    experts = index // cores * slab + place - core + index % cores
    experts = jnp.where(index < spans, experts, index - spans + first)
    named = (one == experts) | (two == experts)
    marks = jnp.where(named, 1.0, 0.0)
    ends = jnp.dot(marks.astype(BF16), upper, preferred_element_type=F32)
    slots = lax.broadcasted_iota(jnp.int32, (CAP, count), 0).astype(F32) + 1.0
    both = (one + two).astype(F32)
    own = first + core
    others = jnp.zeros((CAP, 1), F32)


    def slots_of(at):
        return jnp.where(ends[at : at + 1] == slots, marks[at : at + 1], 0.0)

    for span in range(spans):
        along[CAP * span : CAP * (span + 1)] = slots_of(span).astype(BF16)
    for c in range(cores):
        mine = slots_of(spans + c)
        select[CAP * c : CAP * (c + 1)] = mine.astype(BF16)
        total = jnp.sum(mine * both, axis=1, keepdims=True)
        others = jnp.where(core == c, total, others)
    lanes = lax.broadcasted_iota(jnp.int32, rival.shape, 1)
    rival[...] = jnp.where(lanes == others.astype(jnp.int32) - own, 1.0, 0.0)
    for copy in copies[:5]:
        copy.wait()
    own_w = spread[0]
    for depth in range(1, spread.shape[0]):
        spread[depth] = own_w
    for copy in copies[6:]:
        copy.wait()


def advance(came_ref, res_ref, bias_ref, gain_ref, old_ref, out_ref, new_ref, held_ref, sems):
    seqs, key_width, value_width = old_ref.shape
    total = came_ref[0].astype(F32)
    for at in range(1, came_ref.shape[0]):
        total = total + came_ref[at].astype(F32)
    res = res_ref[...].astype(F32)
    total = total * lax.rsqrt(jnp.mean(res * res, axis=1, keepdims=True) + EPSILON)
    query = total[:, :key_width].astype(BF16).astype(F32) * key_width ** (-0.5)
    key = total[:, key_width : 2 * key_width].astype(BF16).astype(F32)
    value = total[:, 2 * key_width : 2 * key_width + value_width].astype(BF16).astype(F32)
    pre = total[:, 2 * key_width + value_width :] + bias_ref[...]
    log_decay = (jnp.minimum(pre, 0.0) - jnp.log1p(jnp.exp(-jnp.abs(pre)))) / GATE_SCALE
    down = jnp.concatenate([query, key, jnp.exp(log_decay), jnp.zeros_like(query)], axis=0).T
    copies = []
    gated = []
    for seq in range(seqs):
        read = jnp.zeros((1, value_width), F32)
        for at in range(0, key_width, 32):
            block = down[at : at + 32]
            query_col = block[:, seq : seq + 1]
            key_col = block[:, seqs + seq : seqs + seq + 1]
            alpha_col = block[:, 2 * seqs + seq : 2 * seqs + seq + 1]
            new = alpha_col * old_ref[seq, at : at + 32] + key_col * value[seq : seq + 1]
            held_ref[seq, at : at + 32] = new
            if at % 64:
                rows = pl.ds(at - 32, 64)
                copies.append(
                    pltpu.make_async_copy(
                        held_ref.at[seq, rows], new_ref.at[seq, rows], sems.at[len(copies)]
                    )
                )
                copies[-1].start()
            read = read + jnp.sum(query_col * new, axis=0, keepdims=True)
        mean = jnp.mean(read * read, axis=1, keepdims=True)
        gated.append(read * lax.rsqrt(mean + EPSILON) * gain_ref[...])
    gated = jnp.concatenate(gated, axis=0).astype(BF16)
    for at in range(out_ref.shape[0]):
        out_ref[at] = gated
    for copy in copies:
        copy.wait()


def mix(
    which,
    expert_ref,
    came_ref,
    gain_ref,
    group_ref,
    rival_ref,
    gate_ref,
    up_ref,
    down_ref,
    out_ref,
    rows_ref,
):
    expert = which()
    size = came_ref.shape[2]
    for at in range(came_ref.shape[0]):
        rows_ref[:, size * at : size * (at + 1)] = came_ref[at].astype(F32)
    rows = rows_ref[...]
    mean = jnp.mean(rows * rows, axis=1, keepdims=True)
    rows = (rows * lax.rsqrt(mean + EPSILON) * gain_ref[...]).astype(BF16)
    gate = jnp.dot(rows, gate_ref[...], preferred_element_type=F32)
    up = jnp.dot(rows, up_ref[...], preferred_element_type=F32)
    over = (((1,), (1,)), ((), ()))
    groups = lax.dot_general(rows, group_ref[...], over, preferred_element_type=F32)
    logits = lax.dot_general(rows, expert_ref[...], over, preferred_element_type=F32)
    units = (gate * jax.nn.sigmoid(gate) * up).astype(BF16)
    output = jnp.dot(units, down_ref[...], preferred_element_type=F32)
    of_group = lax.broadcasted_iota(jnp.int32, groups.shape, 1)
    own = of_group == expert // (logits.shape[1] // groups.shape[1])
    group_logit = jnp.sum(jnp.where(own, groups, 0.0), axis=1, keepdims=True)
    share = 1.0 / jnp.sum(jnp.exp(groups - group_logit), axis=1, keepdims=True)
    lanes = lax.broadcasted_iota(jnp.int32, logits.shape, 1)
    chosen = jnp.sum(jnp.where(lanes == expert, logits, 0.0), axis=1, keepdims=True)
    rival = jnp.sum(logits * rival_ref[...], axis=1, keepdims=True)
    output = (output * (share * jax.nn.sigmoid(chosen - rival))).astype(BF16)
    piece = out_ref.shape[2]
    for at in range(out_ref.shape[0]):
        out_ref[at] = output[:, piece * at : piece * (at + 1)]


def pack(heads_ref, held_ref, res_ref, out_ref):
    value_width = heads_ref.shape[1]
    part = lax.dot_general(
        heads_ref[...],
        held_ref[:, held_ref.shape[1] - value_width :],
        (((1,), (1,)), ((), ())),
        preferred_element_type=F32,
    )
    with_res = (lax.axis_index("tp") == 0).astype(F32)
    part = part + res_ref[...].astype(F32) * with_res
    lines, lanes = out_ref.shape[1:]
    eighths = part.shape[0] // lines
    size = lanes // eighths
    group = lax.broadcasted_iota(jnp.int32, (2 * lines, lanes), 1) // size
    lower = lax.broadcasted_iota(jnp.int32, (2 * lines, lanes), 0) // lines
    for eighth in range(eighths):
        block = jnp.zeros((2 * lines, lanes), F32)
        for k in range(0, eighths, 2):
            rows = part[lines * k : lines * (k + 2)]
            for low in range(2):
                moved = pltpu.roll(rows, (size * (k + low - eighth)) % lanes, 1)
                block = jnp.where((group == k + low) & (lower == low), moved, block)
        block = (block[:lines] + block[lines:]).astype(BF16)
        quarter, core = eighth // 2, eighth % 2
        for row in range(out_ref.shape[0] // eighths):
            out_ref[eighths * row + eighths // 2 * core + quarter] = block


def dispatch(at_place, came_ref, along_ref, _, out_ref, hidden_ref, rows_ref, all_ref):
    depth, row = at_place()
    count, lines, lanes = came_ref.shape
    eighths = rows_ref.shape[0] // lines
    size = lanes // eighths
    heads = eighths // 2
    all_ref[...] = jnp.zeros_like(all_ref)
    hidden = []
    for at in range(count // heads):
        total = came_ref[heads * at].astype(F32)
        for head in range(1, heads):
            total = total + came_ref[heads * at + head].astype(F32)
        total = total.astype(BF16).astype(F32)
        both = jnp.concatenate([total, total], axis=0)
        back = pltpu.roll(both, lanes - size, 1)
        lower = lax.broadcasted_iota(jnp.int32, both.shape, 0) // lines
        hidden.append(jnp.where(lower == 0, both, back))
    group = lax.broadcasted_iota(jnp.int32, (2 * lines, lanes), 1) // size
    for k in range(0, eighths, 2):
        for half in range(2):
            block = jnp.zeros((2 * lines, lanes), F32)
            for m in range(eighths):
                moved = pltpu.roll(hidden[eighths * half + m], (size * (m - k)) % lanes, 1)
                block = jnp.where(group == m, moved, block)
            rows_ref[lines * k : lines * (k + 2), lanes * half : lanes * (half + 1)] = block
    rows = rows_ref[...].astype(BF16)
    own = hidden_ref.shape[0]
    slab = rows.shape[0]
    all_ref[pl.ds(pl.multiple_of(depth * slab, slab), slab)] = rows
    slots = jnp.dot(along_ref[...], all_ref[...], preferred_element_type=F32).astype(BF16)
    span = out_ref.shape[1]
    for at in range(out_ref.shape[0]):
        out_ref[at] = slots[span * at : span * (at + 1)]
    here = lax.broadcasted_iota(jnp.int32, (8, slab), 0)
    there = lax.broadcasted_iota(jnp.int32, (8, slab), 1)
    pick = jnp.where(there == here + own * row, 1.0, 0.0).astype(BF16)
    hidden_ref[...] = jnp.dot(pick, rows, preferred_element_type=F32)[:own].astype(BF16)


def on_device(
    residual_in,
    gla_state,
    norm_gain,
    w_query,
    w_key,
    w_value,
    w_decay,
    decay_bias,
    head_gain,
    w_output,
    ffn_gain,
    router_group,
    router_expert,
    expert_ids,
    w_gate,
    w_up,
    w_down,
):
    depths, rows, cores = (lax.axis_size(a) for a in EP)
    heads = lax.axis_size("tp")
    slab = rows * cores
    parts = cores * heads
    far = depths * rows
    tokens = expert_ids.shape[0]
    seqs, width = residual_in.shape
    strip = w_query.shape[0]
    key_width, value_width = w_query.shape[1], w_value.shape[1]
    in_width = 3 * key_width + value_width
    held = depths * strip
    piece = width // parts
    place = lax.axis_index(SLAB)
    chip = lax.axis_index(FAR)
    core = lax.axis_index("ep_2")

    n_experts = router_expert.shape[0]

    def experts_of():
        core = lax.axis_index("ep_2")
        return lax.axis_index(FAR) * cores, core, lax.axis_index(SLAB), slab

    vmem = pl.BlockSpec(memory_space=pltpu.VMEM)
    later = (residual_in, norm_gain, head_gain, ffn_gain, decay_bias, router_group.T)
    shapes = [
        pltpu.VMEM((depths, strip, in_width + value_width), BF16),
        pltpu.VMEM((depths * cores * CAP, tokens), BF16),
        pltpu.VMEM((cores * CAP, tokens), BF16),
        pltpu.VMEM((CAP, n_experts), F32),
        *(pltpu.VMEM(a.shape, a.dtype) for a in later),
    ]
    spread, along, select, rival_lane, *later = pl.pallas_call(
        functools.partial(prepare, experts_of),
        out_shape=shapes,
        in_specs=[pl.BlockSpec(memory_space=pl.ANY)] * 12,
        out_specs=[vmem] * len(shapes),
        scratch_shapes=[
            pltpu.VMEM((expert_ids.shape[1], tokens), jnp.int32),
            pltpu.SemaphoreType.DMA((12,)),
        ],
    )(w_query, w_key, w_value, w_decay, w_output.T, expert_ids.T, *later)
    residual_in, norm_gain, head_gain, ffn_gain, decay_bias, group_rows = later
    head_gain = head_gain.astype(F32)[None]
    ffn_gain = ffn_gain.astype(F32)[None]
    decay_bias = decay_bias[None]
    own_gain = norm_gain.reshape(depths, slab, strip)[:, place].reshape(held).astype(F32)
    strips = residual_in.reshape(seqs, depths, slab, strip).transpose(2, 0, 1, 3)
    strips = strips.reshape(slab, seqs, held)

    tied = lax.optimization_barrier(
        (spread, strips, along, select, rival_lane, own_gain)
        + (head_gain, ffn_gain, decay_bias)
    )
    spread, strips, along, select, rival_lane, own_gain, *tied = tied
    head_gain, ffn_gain, decay_bias = tied
    gathered = exchange(spread, "ep_0").reshape(held, in_width + value_width)
    gathered, strips = lax.optimization_barrier((gathered, strips))
    slab_res = exchange(strips, SLAB).reshape(slab * seqs, held)
    lhs = (slab_res.astype(F32) * own_gain).astype(BF16)
    sums = jnp.dot(lhs, gathered[:, :in_width], preferred_element_type=F32).astype(BF16)
    arrived = exchange(sums.reshape(slab, seqs, in_width), SLAB)
    gated, new_state = pl.pallas_call(
        advance,
        out_shape=[
            pltpu.VMEM((slab, seqs, value_width), BF16),
            jax.ShapeDtypeStruct((seqs, key_width, value_width), F32),
        ],
        in_specs=[vmem] * 5,
        out_specs=[vmem, pl.BlockSpec(memory_space=pl.ANY)],
        scratch_shapes=[
            pltpu.VMEM((seqs, key_width, value_width), F32),
            pltpu.SemaphoreType.DMA((seqs * key_width // 64,)),
        ],
    )(*map(on_chip, (arrived, residual_in, decay_bias, head_gain, gla_state[:, 0])))

    slab_heads, slab_res = exchange(gated, SLAB, slab_res)
    slab_heads = slab_heads.reshape(slab * seqs, value_width)
    lines = slab * seqs // parts
    came = pl.pallas_call(
        pack,
        out_shape=pltpu.VMEM((slab * heads, lines, held), BF16),
        in_specs=[vmem] * 3,
        out_specs=vmem,
    )(*map(on_chip, (slab_heads, gathered, slab_res)))
    came = exchange(came, SLAB_TP)
    router = on_chip(router_expert)

    def at_place():
        return lax.axis_index("ep_0"), lax.axis_index("ep_1")

    outward, hidden = pl.pallas_call(
        functools.partial(dispatch, at_place),
        out_shape=[
            pltpu.VMEM((depths, cores * CAP, piece), BF16),
            pltpu.VMEM((cores * seqs, piece), BF16),
        ],
        in_specs=[vmem] * 3,
        out_specs=[vmem] * 2,
        scratch_shapes=[
            pltpu.VMEM((slab * seqs, piece), F32),
            pltpu.VMEM((tokens, piece), BF16),
        ],
    )(on_chip(came), on_chip(along), router)
    slot_part = exchange(outward, "ep_0").astype(F32).sum(axis=0).astype(BF16)
    slot_part = to_all(slot_part.reshape(cores, CAP, piece), heads)
    came = exchange(slot_part.reshape(parts, CAP, piece), CHIPS)
    operands = (came, ffn_gain, group_rows, rival_lane)
    operands += (w_gate[0], w_up[0], w_down[0])
    back = pl.pallas_call(
        functools.partial(mix, lambda: lax.axis_index(EP)),
        out_shape=pltpu.VMEM((parts, CAP, piece), BF16),
        in_specs=[vmem] * (1 + len(operands)),
        out_specs=vmem,
        scratch_shapes=[pltpu.VMEM((CAP, width), F32)],
    )(router, *map(on_chip, operands))
    summed = exchange(back, CHIPS).reshape(heads, cores, CAP, piece).astype(F32).sum(axis=0)
    dense = lax.dot_general(
        select,
        summed.astype(BF16).reshape(cores * CAP, piece),
        (((0,), (0,)), ((), ())),
        preferred_element_type=F32,
    ).astype(BF16)
    moe, hidden = exchange(dense.reshape(far, cores * seqs, piece), FAR, hidden)
    moe = moe.astype(F32).sum(axis=0)
    layer = (hidden.astype(F32) + moe).astype(BF16)
    last = to_all(layer.reshape(cores, seqs, piece), heads).reshape(parts, seqs, piece)
    layer_out = exchange(last, CHIPS).transpose(1, 0, 2).reshape(seqs, width)
    return (layer_out, new_state[:, None])


def solution(mesh):
    torus = Mesh(mesh.devices.reshape(8, 8, 2, mesh.shape["tp"]), (*EP, "tp"))
    in_specs = (
        P(EP, None),
        P(EP, "tp", None, None),
        P(),
        P(EP, "tp"),
        P(EP, "tp"),
        P(EP, "tp"),
        P(EP, "tp"),
        P("tp"),
        P(),
        P("tp", EP),
        P(),
        P(),
        P(),
        P(),
        P(EP, None, "tp"),
        P(EP, None, "tp"),
        P(EP, "tp", None),
    )
    out_specs = (P(EP, None), P(EP, "tp", None, None))
    return jax.shard_map(
        on_device, mesh=torus, in_specs=in_specs, out_specs=out_specs, check_vma=False
    )
```

```python
import functools

import jax
import jax.numpy as jnp
from jax import lax
from jax.experimental import pallas as pl
from jax.experimental.pallas import tpu as pltpu
from jax.sharding import Mesh
from jax.sharding import PartitionSpec as P


CAP = 16
EP = ("ep_0", "ep_1", "ep_2")
FAR = ("ep_0", "ep_1")
SLAB = ("ep_1", "ep_2")
SLAB_TP = ("ep_1", "ep_2", "tp")
CHIPS = ("tp", "ep_2")

EPSILON = 1e-06
GATE_SCALE = 16.0
F32 = jnp.float32
BF16 = jnp.bfloat16


def exchange(blocks, axes, *later):
    came = lax.all_to_all(blocks, axes, split_axis=0, concat_axis=0, tiled=True)
    return lax.optimization_barrier((came, *later)) if later else came


def on_chip(array):
    return pltpu.with_memory_space_constraint(array, pltpu.VMEM)


def to_all(shard, count):
    return jnp.broadcast_to(shard[None], (count, *shard.shape))


def prepare(experts_of, *refs):
    sources, (spread, along, select, rival, *kept), (ids, sems) = refs[:12], refs[12:-2], refs[-2:]
    *weights, ids_in = sources[:6]
    width = 0
    copies = []
    for source in weights:
        for depth in range(spread.shape[0]):
            place = spread.at[depth, :, pl.ds(width, source.shape[1])]
            copies.append(pltpu.make_async_copy(source, place, sems.at[len(copies)]))
        width += source.shape[1]
    spreads = len(copies)
    copies.append(pltpu.make_async_copy(ids_in, ids, sems.at[len(copies)]))
    for source, target in zip(sources[6:], kept, strict=True):
        copies.append(pltpu.make_async_copy(source, target, sems.at[len(copies)]))
    for copy in copies:
        copy.start()
    first, core, place, slab = experts_of()
    count = ids.shape[1]
    row = lax.broadcasted_iota(jnp.int32, (count, count), 0)
    col = lax.broadcasted_iota(jnp.int32, (count, count), 1)
    upper = jnp.where(row <= col, 1.0, 0.0).astype(BF16)
    copies[spreads].wait()
    one, two = ids[0:1, :], ids[1:2, :]
    spans = along.shape[0] // CAP
    cores = select.shape[0] // CAP
    index = lax.broadcasted_iota(jnp.int32, (spans + 8, count), 0)
    experts = index // cores * slab + place - core + index % cores
    experts = jnp.where(index < spans, experts, index - spans + first)
    named = (one == experts) | (two == experts)
    marks = jnp.where(named, 1.0, 0.0)
    ends = jnp.dot(marks.astype(BF16), upper, preferred_element_type=F32)
    slots = lax.broadcasted_iota(jnp.int32, (CAP, count), 0).astype(F32) + 1.0
    both = (one + two).astype(F32)
    own = first + core
    others = jnp.zeros((CAP, 1), F32)


    def slots_of(at):
        return jnp.where(ends[at : at + 1] == slots, marks[at : at + 1], 0.0)

    for span in range(spans):
        along[CAP * span : CAP * (span + 1)] = slots_of(span).astype(BF16)
    for c in range(cores):
        mine = slots_of(spans + c)
        select[CAP * c : CAP * (c + 1)] = mine.astype(BF16)
        total = jnp.sum(mine * both, axis=1, keepdims=True)
        others = jnp.where(core == c, total, others)
    lanes = lax.broadcasted_iota(jnp.int32, rival.shape, 1)
    rival[...] = jnp.where(lanes == others.astype(jnp.int32) - own, 1.0, 0.0)
    for copy in copies[:spreads] + copies[spreads + 1 :]:
        copy.wait()


def strips_of(place_of, slab, strip, rows_ref, gain_ref, lhs_ref, res_ref):
    place = place_of()
    width, held = rows_ref.shape[1], res_ref.shape[1]
    feature = lax.broadcasted_iota(jnp.int32, (width, held), 0)
    lane = lax.broadcasted_iota(jnp.int32, (width, held), 1)
    taken = feature == lane // strip * (slab * strip) + place * strip + lane % strip
    pick = jnp.where(taken, 1.0, 0.0).astype(BF16)
    rows = rows_ref[...]
    scaled = (rows.astype(F32) * gain_ref[...]).astype(BF16)
    res_ref[...] = jnp.dot(rows, pick, preferred_element_type=F32).astype(BF16)
    lhs_ref[...] = jnp.dot(scaled, pick, preferred_element_type=F32).astype(BF16)


def advance(came_ref, res_ref, bias_ref, gain_ref, old_ref, out_ref, new_ref, held_ref, sems):
    seqs, key_width, value_width = old_ref.shape
    total = came_ref[0].astype(F32)
    for at in range(1, came_ref.shape[0]):
        total = total + came_ref[at].astype(F32)
    res = res_ref[...].astype(F32)
    total = total * lax.rsqrt(jnp.mean(res * res, axis=1, keepdims=True) + EPSILON)
    query = total[:, :key_width].astype(BF16).astype(F32) * key_width ** (-0.5)
    key = total[:, key_width : 2 * key_width].astype(BF16).astype(F32)
    value = total[:, 2 * key_width : 2 * key_width + value_width].astype(BF16).astype(F32)
    pre = total[:, 2 * key_width + value_width :] + bias_ref[...]
    log_decay = (jnp.minimum(pre, 0.0) - jnp.log1p(jnp.exp(-jnp.abs(pre)))) / GATE_SCALE
    down = jnp.concatenate([query, key, jnp.exp(log_decay), jnp.zeros_like(query)], axis=0).T
    copies = []
    gated = []
    for seq in range(seqs):
        read = jnp.zeros((1, value_width), F32)
        for at in range(0, key_width, 32):
            block = down[at : at + 32]
            query_col = block[:, seq : seq + 1]
            key_col = block[:, seqs + seq : seqs + seq + 1]
            alpha_col = block[:, 2 * seqs + seq : 2 * seqs + seq + 1]
            new = alpha_col * old_ref[seq, at : at + 32] + key_col * value[seq : seq + 1]
            held_ref[seq, at : at + 32] = new
            if at % 64:
                rows = pl.ds(at - 32, 64)
                copies.append(
                    pltpu.make_async_copy(
                        held_ref.at[seq, rows], new_ref.at[seq, rows], sems.at[len(copies)]
                    )
                )
                copies[-1].start()
            read = read + jnp.sum(query_col * new, axis=0, keepdims=True)
        mean = jnp.mean(read * read, axis=1, keepdims=True)
        gated.append(read * lax.rsqrt(mean + EPSILON) * gain_ref[...])
    gated = jnp.concatenate(gated, axis=0).astype(BF16)
    for at in range(out_ref.shape[0]):
        out_ref[at] = gated
    for copy in copies:
        copy.wait()


def mix(
    which,
    expert_ref,
    came_ref,
    gain_ref,
    group_ref,
    rival_ref,
    gate_ref,
    up_ref,
    down_ref,
    out_ref,
    rows_ref,
):
    expert = which()
    size = came_ref.shape[2]
    for at in range(came_ref.shape[0]):
        rows_ref[:, size * at : size * (at + 1)] = came_ref[at].astype(F32)
    rows = rows_ref[...]
    mean = jnp.mean(rows * rows, axis=1, keepdims=True)
    rows = (rows * lax.rsqrt(mean + EPSILON) * gain_ref[...]).astype(BF16)
    gate = jnp.dot(rows, gate_ref[...], preferred_element_type=F32)
    up = jnp.dot(rows, up_ref[...], preferred_element_type=F32)
    over = (((1,), (1,)), ((), ()))
    groups = lax.dot_general(rows, group_ref[...], over, preferred_element_type=F32)
    logits = lax.dot_general(rows, expert_ref[...], over, preferred_element_type=F32)
    units = (gate * jax.nn.sigmoid(gate) * up).astype(BF16)
    output = jnp.dot(units, down_ref[...], preferred_element_type=F32)
    of_group = lax.broadcasted_iota(jnp.int32, groups.shape, 1)
    own = of_group == expert // (logits.shape[1] // groups.shape[1])
    group_logit = jnp.sum(jnp.where(own, groups, 0.0), axis=1, keepdims=True)
    share = 1.0 / jnp.sum(jnp.exp(groups - group_logit), axis=1, keepdims=True)
    lanes = lax.broadcasted_iota(jnp.int32, logits.shape, 1)
    chosen = jnp.sum(jnp.where(lanes == expert, logits, 0.0), axis=1, keepdims=True)
    rival = jnp.sum(logits * rival_ref[...], axis=1, keepdims=True)
    output = (output * (share * jax.nn.sigmoid(chosen - rival))).astype(BF16)
    piece = out_ref.shape[2]
    for at in range(out_ref.shape[0]):
        out_ref[at] = output[:, piece * at : piece * (at + 1)]


def pack(heads_ref, held_ref, res_ref, out_ref):
    value_width = heads_ref.shape[1]
    part = lax.dot_general(
        heads_ref[...],
        held_ref[:, held_ref.shape[1] - value_width :],
        (((1,), (1,)), ((), ())),
        preferred_element_type=F32,
    )
    with_res = (lax.axis_index("tp") == 0).astype(F32)
    part = part + res_ref[...].astype(F32) * with_res
    lines, lanes = out_ref.shape[1:]
    eighths = part.shape[0] // lines
    size = lanes // eighths
    group = lax.broadcasted_iota(jnp.int32, (2 * lines, lanes), 1) // size
    lower = lax.broadcasted_iota(jnp.int32, (2 * lines, lanes), 0) // lines
    for eighth in range(eighths):
        block = jnp.zeros((2 * lines, lanes), F32)
        for k in range(0, eighths, 2):
            rows = part[lines * k : lines * (k + 2)]
            for low in range(2):
                moved = pltpu.roll(rows, (size * (k + low - eighth)) % lanes, 1)
                block = jnp.where((group == k + low) & (lower == low), moved, block)
        block = (block[:lines] + block[lines:]).astype(BF16)
        quarter, core = eighth // 2, eighth % 2
        for row in range(out_ref.shape[0] // eighths):
            out_ref[eighths * row + eighths // 2 * core + quarter] = block


def dispatch(at_place, came_ref, along_ref, _, out_ref, hidden_ref, rows_ref, all_ref):
    depth, row = at_place()
    count, lines, lanes = came_ref.shape
    eighths = rows_ref.shape[0] // lines
    size = lanes // eighths
    heads = eighths // 2
    all_ref[...] = jnp.zeros_like(all_ref)
    hidden = []
    for at in range(count // heads):
        total = came_ref[heads * at].astype(F32)
        for head in range(1, heads):
            total = total + came_ref[heads * at + head].astype(F32)
        total = total.astype(BF16).astype(F32)
        both = jnp.concatenate([total, total], axis=0)
        back = pltpu.roll(both, lanes - size, 1)
        lower = lax.broadcasted_iota(jnp.int32, both.shape, 0) // lines
        hidden.append(jnp.where(lower == 0, both, back))
    group = lax.broadcasted_iota(jnp.int32, (2 * lines, lanes), 1) // size
    for k in range(0, eighths, 2):
        for half in range(2):
            block = jnp.zeros((2 * lines, lanes), F32)
            for m in range(eighths):
                moved = pltpu.roll(hidden[eighths * half + m], (size * (m - k)) % lanes, 1)
                block = jnp.where(group == m, moved, block)
            rows_ref[lines * k : lines * (k + 2), lanes * half : lanes * (half + 1)] = block
    rows = rows_ref[...].astype(BF16)
    own = hidden_ref.shape[0]
    slab = rows.shape[0]
    all_ref[pl.ds(pl.multiple_of(depth * slab, slab), slab)] = rows
    slots = jnp.dot(along_ref[...], all_ref[...], preferred_element_type=F32).astype(BF16)
    span = out_ref.shape[1]
    for at in range(out_ref.shape[0]):
        out_ref[at] = slots[span * at : span * (at + 1)]
    here = lax.broadcasted_iota(jnp.int32, (8, slab), 0)
    there = lax.broadcasted_iota(jnp.int32, (8, slab), 1)
    pick = jnp.where(there == here + own * row, 1.0, 0.0).astype(BF16)
    hidden_ref[...] = jnp.dot(pick, rows, preferred_element_type=F32)[:own].astype(BF16)


def on_device(
    residual_in,
    gla_state,
    norm_gain,
    w_query,
    w_key,
    w_value,
    w_decay,
    decay_bias,
    head_gain,
    w_output,
    ffn_gain,
    router_group,
    router_expert,
    expert_ids,
    w_gate,
    w_up,
    w_down,
):
    depths, rows, cores = (lax.axis_size(a) for a in EP)
    heads = lax.axis_size("tp")
    slab = rows * cores
    parts = cores * heads
    far = depths * rows
    tokens = expert_ids.shape[0]
    seqs, width = residual_in.shape
    strip = w_query.shape[0]
    key_width, value_width = w_query.shape[1], w_value.shape[1]
    in_width = 3 * key_width + value_width
    held = depths * strip
    piece = width // parts

    n_experts = router_expert.shape[0]

    def experts_of():
        core = lax.axis_index("ep_2")
        return lax.axis_index(FAR) * cores, core, lax.axis_index(SLAB), slab

    vmem = pl.BlockSpec(memory_space=pltpu.VMEM)
    later = (residual_in, norm_gain, head_gain, ffn_gain, decay_bias, router_group.T)
    shapes = [
        jax.ShapeDtypeStruct((depths, strip, in_width + value_width), BF16),
        pltpu.VMEM((depths * cores * CAP, tokens), BF16),
        pltpu.VMEM((cores * CAP, tokens), BF16),
        pltpu.VMEM((CAP, n_experts), F32),
        *(pltpu.VMEM(a.shape, a.dtype) for a in later),
    ]
    spread, along, select, rival_lane, *later = pl.pallas_call(
        functools.partial(prepare, experts_of),
        out_shape=shapes,
        in_specs=[pl.BlockSpec(memory_space=pl.ANY)] * 12,
        out_specs=[pl.BlockSpec(memory_space=pl.ANY)] + [vmem] * (len(shapes) - 1),
        scratch_shapes=[
            pltpu.VMEM((expert_ids.shape[1], tokens), jnp.int32),
            pltpu.SemaphoreType.DMA((5 * depths + 7,)),
        ],
    )(w_query, w_key, w_value, w_decay, w_output.T, expert_ids.T, *later)
    residual_in, norm_gain, head_gain, ffn_gain, decay_bias, group_rows = later
    head_gain = head_gain.astype(F32)[None]
    ffn_gain = ffn_gain.astype(F32)[None]
    decay_bias = decay_bias[None]
    norm_gain = norm_gain.astype(F32)[None]

    tied = lax.optimization_barrier(
        (spread, residual_in, along, select, rival_lane, norm_gain)
        + (head_gain, ffn_gain, decay_bias)
    )
    spread, residual_in, along, select, rival_lane, norm_gain, *tied = tied
    head_gain, ffn_gain, decay_bias = tied
    gathered = exchange(spread, "ep_0")
    rows_in = lax.all_gather(residual_in, SLAB, axis=0, tiled=True)
    lhs, slab_res = pl.pallas_call(
        functools.partial(strips_of, lambda: lax.axis_index(SLAB), slab, strip),
        out_shape=[pltpu.VMEM((slab * seqs, held), BF16)] * 2,
        in_specs=[vmem] * 2,
        out_specs=[vmem] * 2,
    )(on_chip(rows_in), on_chip(norm_gain))
    gathered, lhs, slab_res = lax.optimization_barrier((gathered, lhs, slab_res))
    gathered = gathered.reshape(held, in_width + value_width)
    sums = jnp.dot(lhs, gathered[:, :in_width], preferred_element_type=F32).astype(BF16)
    arrived = exchange(sums.reshape(slab, seqs, in_width), SLAB)
    gated, new_state = pl.pallas_call(
        advance,
        out_shape=[
            pltpu.VMEM((slab, seqs, value_width), BF16),
            jax.ShapeDtypeStruct((seqs, key_width, value_width), F32),
        ],
        in_specs=[vmem] * 5,
        out_specs=[vmem, pl.BlockSpec(memory_space=pl.ANY)],
        scratch_shapes=[
            pltpu.VMEM((seqs, key_width, value_width), F32),
            pltpu.SemaphoreType.DMA((seqs * key_width // 64,)),
        ],
    )(*map(on_chip, (arrived, residual_in, decay_bias, head_gain, gla_state[:, 0])))

    slab_heads, slab_res = exchange(gated, SLAB, slab_res)
    slab_heads = slab_heads.reshape(slab * seqs, value_width)
    lines = slab * seqs // parts
    came = pl.pallas_call(
        pack,
        out_shape=pltpu.VMEM((slab * heads, lines, held), BF16),
        in_specs=[vmem] * 3,
        out_specs=vmem,
    )(*map(on_chip, (slab_heads, gathered, slab_res)))
    came = exchange(came, SLAB_TP)
    router = on_chip(router_expert)

    def at_place():
        return lax.axis_index("ep_0"), lax.axis_index("ep_1")

    outward, hidden = pl.pallas_call(
        functools.partial(dispatch, at_place),
        out_shape=[
            pltpu.VMEM((depths, cores * CAP, piece), BF16),
            pltpu.VMEM((cores * seqs, piece), BF16),
        ],
        in_specs=[vmem] * 3,
        out_specs=[vmem] * 2,
        scratch_shapes=[
            pltpu.VMEM((slab * seqs, piece), F32),
            pltpu.VMEM((tokens, piece), BF16),
        ],
    )(on_chip(came), on_chip(along), router)
    slot_part = exchange(outward, "ep_0").astype(F32).sum(axis=0).astype(BF16)
    slot_part = to_all(slot_part.reshape(cores, CAP, piece), heads)
    came = exchange(slot_part.reshape(parts, CAP, piece), CHIPS)
    operands = (came, ffn_gain, group_rows, rival_lane)
    operands += (w_gate[0], w_up[0], w_down[0])
    back = pl.pallas_call(
        functools.partial(mix, lambda: lax.axis_index(EP)),
        out_shape=pltpu.VMEM((parts, CAP, piece), BF16),
        in_specs=[vmem] * (1 + len(operands)),
        out_specs=vmem,
        scratch_shapes=[pltpu.VMEM((CAP, width), F32)],
    )(router, *map(on_chip, operands))
    summed = exchange(back, CHIPS).reshape(heads, cores, CAP, piece).astype(F32).sum(axis=0)
    dense = lax.dot_general(
        select,
        summed.astype(BF16).reshape(cores * CAP, piece),
        (((0,), (0,)), ((), ())),
        preferred_element_type=F32,
    ).astype(BF16)
    moe, hidden = exchange(dense.reshape(far, cores * seqs, piece), FAR, hidden)
    moe = moe.astype(F32).sum(axis=0)
    layer = (hidden.astype(F32) + moe).astype(BF16)
    last = to_all(layer.reshape(cores, seqs, piece), heads).reshape(parts, seqs, piece)
    layer_out = exchange(last, CHIPS).transpose(1, 0, 2).reshape(seqs, width)
    return (layer_out, new_state[:, None])


def solution(mesh):
    torus = Mesh(mesh.devices.reshape(8, 8, 2, mesh.shape["tp"]), (*EP, "tp"))
    in_specs = (
        P(EP, None),
        P(EP, "tp", None, None),
        P(),
        P(EP, "tp"),
        P(EP, "tp"),
        P(EP, "tp"),
        P(EP, "tp"),
        P("tp"),
        P(),
        P("tp", EP),
        P(),
        P(),
        P(),
        P(),
        P(EP, None, "tp"),
        P(EP, None, "tp"),
        P(EP, "tp", None),
    )
    out_specs = (P(EP, None), P(EP, "tp", None, None))
    return jax.shard_map(
        on_device, mesh=torus, in_specs=in_specs, out_specs=out_specs, check_vma=False
    )
```

```python
import functools

import jax
import jax.numpy as jnp
from jax import lax
from jax.experimental import pallas as pl
from jax.experimental.pallas import tpu as pltpu
from jax.sharding import Mesh
from jax.sharding import PartitionSpec as P


CAP = 16
EP = ("ep_0", "ep_1", "ep_2")
FAR = ("ep_0", "ep_1")
SLAB = ("ep_1", "ep_2")
SLAB_TP = ("ep_1", "ep_2", "tp")
CHIPS = ("tp", "ep_2")

EPSILON = 1e-06
GATE_SCALE = 16.0
F32 = jnp.float32
BF16 = jnp.bfloat16


def exchange(blocks, axes, *later):
    came = lax.all_to_all(blocks, axes, split_axis=0, concat_axis=0, tiled=True)
    return lax.optimization_barrier((came, *later)) if later else came


def on_chip(array):
    return pltpu.with_memory_space_constraint(array, pltpu.VMEM)


def to_all(shard, count):
    return jnp.broadcast_to(shard[None], (count, *shard.shape))


def prepare(experts_of, *refs):
    sources, (spread, along, select, rival, *kept) = refs[:12], refs[12:-3]
    own_w, ids, sems = refs[-3:]
    *weights, ids_in = sources[:6]
    width = 0
    copies = []
    for source in weights:
        place = own_w.at[:, pl.ds(width, source.shape[1])]
        copies.append(pltpu.make_async_copy(source, place, sems.at[len(copies)]))
        width += source.shape[1]
    fetched = len(copies)
    copies.append(pltpu.make_async_copy(ids_in, ids, sems.at[len(copies)]))
    for source, target in zip(sources[6:], kept, strict=True):
        copies.append(pltpu.make_async_copy(source, target, sems.at[len(copies)]))
    for copy in copies:
        copy.start()
    first, core, place, slab = experts_of()
    count = ids.shape[1]
    row = lax.broadcasted_iota(jnp.int32, (count, count), 0)
    col = lax.broadcasted_iota(jnp.int32, (count, count), 1)
    upper = jnp.where(row <= col, 1.0, 0.0).astype(BF16)
    for copy in copies[:fetched]:
        copy.wait()
    spreads = []
    for depth in range(spread.shape[0]):
        sem = sems.at[len(copies) + depth]
        spreads.append(pltpu.make_async_copy(own_w, spread.at[depth], sem))
        spreads[-1].start()
    copies[fetched].wait()
    one, two = ids[0:1, :], ids[1:2, :]
    spans = along.shape[0] // CAP
    cores = select.shape[0] // CAP
    index = lax.broadcasted_iota(jnp.int32, (spans + 8, count), 0)
    experts = index // cores * slab + place - core + index % cores
    experts = jnp.where(index < spans, experts, index - spans + first)
    named = (one == experts) | (two == experts)
    marks = jnp.where(named, 1.0, 0.0)
    ends = jnp.dot(marks.astype(BF16), upper, preferred_element_type=F32)
    slots = lax.broadcasted_iota(jnp.int32, (CAP, count), 0).astype(F32) + 1.0
    both = (one + two).astype(F32)
    own = first + core
    others = jnp.zeros((CAP, 1), F32)


    def slots_of(at):
        return jnp.where(ends[at : at + 1] == slots, marks[at : at + 1], 0.0)

    for span in range(spans):
        along[CAP * span : CAP * (span + 1)] = slots_of(span).astype(BF16)
    for c in range(cores):
        mine = slots_of(spans + c)
        select[CAP * c : CAP * (c + 1)] = mine.astype(BF16)
        total = jnp.sum(mine * both, axis=1, keepdims=True)
        others = jnp.where(core == c, total, others)
    lanes = lax.broadcasted_iota(jnp.int32, rival.shape, 1)
    rival[...] = jnp.where(lanes == others.astype(jnp.int32) - own, 1.0, 0.0)
    for copy in copies[fetched + 1 :] + spreads:
        copy.wait()


def strips_of(place_of, slab, strip, rows_ref, gain_ref, lhs_ref, res_ref):
    place = place_of()
    width, held = rows_ref.shape[1], res_ref.shape[1]
    feature = lax.broadcasted_iota(jnp.int32, (width, held), 0)
    lane = lax.broadcasted_iota(jnp.int32, (width, held), 1)
    taken = feature == lane // strip * (slab * strip) + place * strip + lane % strip
    pick = jnp.where(taken, 1.0, 0.0).astype(BF16)
    rows = rows_ref[...]
    scaled = (rows.astype(F32) * gain_ref[...]).astype(BF16)
    res_ref[...] = jnp.dot(rows, pick, preferred_element_type=F32).astype(BF16)
    lhs_ref[...] = jnp.dot(scaled, pick, preferred_element_type=F32).astype(BF16)


def advance(came_ref, res_ref, bias_ref, gain_ref, old_ref, out_ref, new_ref, held_ref, sems):
    seqs, key_width, value_width = old_ref.shape
    count = came_ref.shape[0]
    seq_of = lax.broadcasted_iota(jnp.int32, (8, count), 1) % seqs
    pick = jnp.where(seq_of == lax.broadcasted_iota(jnp.int32, (8, count), 0), 1.0, 0.0)
    total = jnp.dot(pick.astype(BF16), came_ref[...], preferred_element_type=F32)[:seqs]
    res = res_ref[...].astype(F32)
    total = total * lax.rsqrt(jnp.mean(res * res, axis=1, keepdims=True) + EPSILON)
    query = total[:, :key_width].astype(BF16).astype(F32) * key_width ** (-0.5)
    key = total[:, key_width : 2 * key_width].astype(BF16).astype(F32)
    value = total[:, 2 * key_width : 2 * key_width + value_width].astype(BF16).astype(F32)
    pre = total[:, 2 * key_width + value_width :] + bias_ref[...]
    log_decay = (jnp.minimum(pre, 0.0) - jnp.log1p(jnp.exp(-jnp.abs(pre)))) / GATE_SCALE
    down = jnp.concatenate([query, key, jnp.exp(log_decay), jnp.zeros_like(query)], axis=0).T
    copies = []
    gated = []
    for seq in range(seqs):
        read = jnp.zeros((8, value_width), F32)
        for at in range(0, key_width, 32):
            block = down[at : at + 32]
            query_col = block[:, seq : seq + 1]
            key_col = block[:, seqs + seq : seqs + seq + 1]
            alpha_col = block[:, 2 * seqs + seq : 2 * seqs + seq + 1]
            new = alpha_col * old_ref[seq, at : at + 32] + key_col * value[seq : seq + 1]
            held_ref[seq, at : at + 32] = new
            if at % 64:
                rows = pl.ds(at - 32, 64)
                copies.append(
                    pltpu.make_async_copy(
                        held_ref.at[seq, rows], new_ref.at[seq, rows], sems.at[len(copies)]
                    )
                )
                copies[-1].start()
            read = read + jnp.sum((query_col * new).reshape(4, 8, value_width), axis=0)
        read = jnp.sum(read, axis=0, keepdims=True)
        mean = jnp.mean(read * read, axis=1, keepdims=True)
        gated.append(read * lax.rsqrt(mean + EPSILON) * gain_ref[...])
    gated = jnp.concatenate(gated, axis=0).astype(BF16)
    for at in range(out_ref.shape[0]):
        out_ref[at] = gated
    for copy in copies:
        copy.wait()


def mix(
    which,
    expert_ref,
    came_ref,
    gain_ref,
    group_ref,
    rival_ref,
    gate_ref,
    up_ref,
    down_ref,
    out_ref,
    rows_ref,
):
    expert = which()
    size = came_ref.shape[2]
    for at in range(came_ref.shape[0]):
        rows_ref[:, size * at : size * (at + 1)] = came_ref[at].astype(F32)
    rows = rows_ref[...]
    mean = jnp.mean(rows * rows, axis=1, keepdims=True)
    rows = (rows * lax.rsqrt(mean + EPSILON) * gain_ref[...]).astype(BF16)
    gate = jnp.dot(rows, gate_ref[...], preferred_element_type=F32)
    up = jnp.dot(rows, up_ref[...], preferred_element_type=F32)
    over = (((1,), (1,)), ((), ()))
    groups = lax.dot_general(rows, group_ref[...], over, preferred_element_type=F32)
    logits = lax.dot_general(rows, expert_ref[...], over, preferred_element_type=F32)
    units = (gate * jax.nn.sigmoid(gate) * up).astype(BF16)
    output = jnp.dot(units, down_ref[...], preferred_element_type=F32)
    of_group = lax.broadcasted_iota(jnp.int32, groups.shape, 1)
    own = of_group == expert // (logits.shape[1] // groups.shape[1])
    group_logit = jnp.sum(jnp.where(own, groups, 0.0), axis=1, keepdims=True)
    share = 1.0 / jnp.sum(jnp.exp(groups - group_logit), axis=1, keepdims=True)
    lanes = lax.broadcasted_iota(jnp.int32, logits.shape, 1)
    chosen = jnp.sum(jnp.where(lanes == expert, logits, 0.0), axis=1, keepdims=True)
    rival = jnp.sum(logits * rival_ref[...], axis=1, keepdims=True)
    output = (output * (share * jax.nn.sigmoid(chosen - rival))).astype(BF16)
    piece = out_ref.shape[2]
    for at in range(out_ref.shape[0]):
        out_ref[at] = output[:, piece * at : piece * (at + 1)]


def pack(heads_ref, held_ref, res_ref, out_ref):
    value_width = heads_ref.shape[1]
    part = lax.dot_general(
        heads_ref[...],
        held_ref[:, held_ref.shape[1] - value_width :],
        (((1,), (1,)), ((), ())),
        preferred_element_type=F32,
    )
    with_res = (lax.axis_index("tp") == 0).astype(F32)
    part = part + res_ref[...].astype(F32) * with_res
    lines, lanes = out_ref.shape[1:]
    eighths = part.shape[0] // lines
    size = lanes // eighths
    group = lax.broadcasted_iota(jnp.int32, (2 * lines, lanes), 1) // size
    lower = lax.broadcasted_iota(jnp.int32, (2 * lines, lanes), 0) // lines
    for eighth in range(eighths):
        block = jnp.zeros((2 * lines, lanes), F32)
        for k in range(0, eighths, 2):
            rows = part[lines * k : lines * (k + 2)]
            for low in range(2):
                moved = pltpu.roll(rows, (size * (k + low - eighth)) % lanes, 1)
                block = jnp.where((group == k + low) & (lower == low), moved, block)
        block = (block[:lines] + block[lines:]).astype(BF16)
        quarter, core = eighth // 2, eighth % 2
        for row in range(out_ref.shape[0] // eighths):
            out_ref[eighths * row + eighths // 2 * core + quarter] = block


def dispatch(at_place, came_ref, along_ref, _, out_ref, hidden_ref, rows_ref, all_ref):
    depth, row = at_place()
    count, lines, lanes = came_ref.shape
    eighths = rows_ref.shape[0] // lines
    size = lanes // eighths
    heads = eighths // 2
    all_ref[...] = jnp.zeros_like(all_ref)
    hidden = []
    for at in range(count // heads):
        total = came_ref[heads * at].astype(F32)
        for head in range(1, heads):
            total = total + came_ref[heads * at + head].astype(F32)
        total = total.astype(BF16).astype(F32)
        both = jnp.concatenate([total, total], axis=0)
        back = pltpu.roll(both, lanes - size, 1)
        lower = lax.broadcasted_iota(jnp.int32, both.shape, 0) // lines
        hidden.append(jnp.where(lower == 0, both, back))
    group = lax.broadcasted_iota(jnp.int32, (2 * lines, lanes), 1) // size
    for k in range(0, eighths, 2):
        for half in range(2):
            block = jnp.zeros((2 * lines, lanes), F32)
            for m in range(eighths):
                moved = pltpu.roll(hidden[eighths * half + m], (size * (m - k)) % lanes, 1)
                block = jnp.where(group == m, moved, block)
            rows_ref[lines * k : lines * (k + 2), lanes * half : lanes * (half + 1)] = block
    rows = rows_ref[...].astype(BF16)
    own = hidden_ref.shape[0]
    slab = rows.shape[0]
    all_ref[pl.ds(pl.multiple_of(depth * slab, slab), slab)] = rows
    slots = jnp.dot(along_ref[...], all_ref[...], preferred_element_type=F32).astype(BF16)
    span = out_ref.shape[1]
    for at in range(out_ref.shape[0]):
        out_ref[at] = slots[span * at : span * (at + 1)]
    here = lax.broadcasted_iota(jnp.int32, (8, slab), 0)
    there = lax.broadcasted_iota(jnp.int32, (8, slab), 1)
    pick = jnp.where(there == here + own * row, 1.0, 0.0).astype(BF16)
    hidden_ref[...] = jnp.dot(pick, rows, preferred_element_type=F32)[:own].astype(BF16)


def on_device(
    residual_in,
    gla_state,
    norm_gain,
    w_query,
    w_key,
    w_value,
    w_decay,
    decay_bias,
    head_gain,
    w_output,
    ffn_gain,
    router_group,
    router_expert,
    expert_ids,
    w_gate,
    w_up,
    w_down,
):
    depths, rows, cores = (lax.axis_size(a) for a in EP)
    heads = lax.axis_size("tp")
    slab = rows * cores
    parts = cores * heads
    far = depths * rows
    tokens = expert_ids.shape[0]
    seqs, width = residual_in.shape
    strip = w_query.shape[0]
    key_width, value_width = w_query.shape[1], w_value.shape[1]
    in_width = 3 * key_width + value_width
    held = depths * strip
    piece = width // parts

    n_experts = router_expert.shape[0]

    def experts_of():
        core = lax.axis_index("ep_2")
        return lax.axis_index(FAR) * cores, core, lax.axis_index(SLAB), slab

    vmem = pl.BlockSpec(memory_space=pltpu.VMEM)
    later = (residual_in, norm_gain, head_gain, ffn_gain, decay_bias, router_group.T)
    shapes = [
        jax.ShapeDtypeStruct((depths, strip, in_width + value_width), BF16),
        pltpu.VMEM((depths * cores * CAP, tokens), BF16),
        pltpu.VMEM((cores * CAP, tokens), BF16),
        pltpu.VMEM((CAP, n_experts), F32),
        *(pltpu.VMEM(a.shape, a.dtype) for a in later),
    ]
    spread, along, select, rival_lane, *later = pl.pallas_call(
        functools.partial(prepare, experts_of),
        out_shape=shapes,
        in_specs=[pl.BlockSpec(memory_space=pl.ANY)] * 12,
        out_specs=[pl.BlockSpec(memory_space=pl.ANY)] + [vmem] * (len(shapes) - 1),
        scratch_shapes=[
            pltpu.VMEM((strip, in_width + value_width), BF16),
            pltpu.VMEM((expert_ids.shape[1], tokens), jnp.int32),
            pltpu.SemaphoreType.DMA((12 + depths,)),
        ],
    )(w_query, w_key, w_value, w_decay, w_output.T, expert_ids.T, *later)
    residual_in, norm_gain, head_gain, ffn_gain, decay_bias, group_rows = later
    head_gain = head_gain.astype(F32)[None]
    ffn_gain = ffn_gain.astype(F32)[None]
    decay_bias = decay_bias[None]
    norm_gain = norm_gain.astype(F32)[None]

    tied = lax.optimization_barrier(
        (spread, residual_in, along, select, rival_lane, norm_gain)
        + (head_gain, ffn_gain, decay_bias)
    )
    spread, residual_in, along, select, rival_lane, norm_gain, *tied = tied
    head_gain, ffn_gain, decay_bias = tied
    gathered = exchange(spread, "ep_0")
    rows_in = lax.all_gather(residual_in, SLAB, axis=0, tiled=True)
    lhs, slab_res = pl.pallas_call(
        functools.partial(strips_of, lambda: lax.axis_index(SLAB), slab, strip),
        out_shape=[pltpu.VMEM((slab * seqs, held), BF16)] * 2,
        in_specs=[vmem] * 2,
        out_specs=[vmem] * 2,
    )(on_chip(rows_in), on_chip(norm_gain))
    gathered, lhs, slab_res = lax.optimization_barrier((gathered, lhs, slab_res))
    gathered = gathered.reshape(held, in_width + value_width)
    sums = jnp.dot(lhs, gathered[:, :in_width], preferred_element_type=F32).astype(BF16)
    arrived = exchange(sums.reshape(slab, seqs, in_width), SLAB)
    gated, new_state = pl.pallas_call(
        advance,
        out_shape=[
            pltpu.VMEM((slab, seqs, value_width), BF16),
            jax.ShapeDtypeStruct((seqs, key_width, value_width), F32),
        ],
        in_specs=[vmem] * 5,
        out_specs=[vmem, pl.BlockSpec(memory_space=pl.ANY)],
        scratch_shapes=[
            pltpu.VMEM((seqs, key_width, value_width), F32),
            pltpu.SemaphoreType.DMA((seqs * key_width // 64,)),
        ],
    )(*map(on_chip, (arrived.reshape(slab * seqs, in_width), residual_in, decay_bias, head_gain, gla_state[:, 0])))

    slab_heads, slab_res = exchange(gated, SLAB, slab_res)
    slab_heads = slab_heads.reshape(slab * seqs, value_width)
    lines = slab * seqs // parts
    came = pl.pallas_call(
        pack,
        out_shape=pltpu.VMEM((slab * heads, lines, held), BF16),
        in_specs=[vmem] * 3,
        out_specs=vmem,
    )(*map(on_chip, (slab_heads, gathered, slab_res)))
    came = exchange(came, SLAB_TP)
    router = on_chip(router_expert)

    def at_place():
        return lax.axis_index("ep_0"), lax.axis_index("ep_1")

    outward, hidden = pl.pallas_call(
        functools.partial(dispatch, at_place),
        out_shape=[
            pltpu.VMEM((depths, cores * CAP, piece), BF16),
            pltpu.VMEM((cores * seqs, piece), BF16),
        ],
        in_specs=[vmem] * 3,
        out_specs=[vmem] * 2,
        scratch_shapes=[
            pltpu.VMEM((slab * seqs, piece), F32),
            pltpu.VMEM((tokens, piece), BF16),
        ],
    )(on_chip(came), on_chip(along), router)
    slot_part = exchange(outward, "ep_0").astype(F32).sum(axis=0).astype(BF16)
    slot_part = to_all(slot_part.reshape(cores, CAP, piece), heads)
    came = exchange(slot_part.reshape(parts, CAP, piece), CHIPS)
    operands = (came, ffn_gain, group_rows, rival_lane)
    operands += (w_gate[0], w_up[0], w_down[0])
    back = pl.pallas_call(
        functools.partial(mix, lambda: lax.axis_index(EP)),
        out_shape=pltpu.VMEM((parts, CAP, piece), BF16),
        in_specs=[vmem] * (1 + len(operands)),
        out_specs=vmem,
        scratch_shapes=[pltpu.VMEM((CAP, width), F32)],
    )(router, *map(on_chip, operands))
    summed = exchange(back, CHIPS).reshape(heads, cores, CAP, piece).astype(F32).sum(axis=0)
    dense = lax.dot_general(
        select,
        summed.astype(BF16).reshape(cores * CAP, piece),
        (((0,), (0,)), ((), ())),
        preferred_element_type=F32,
    ).astype(BF16)
    moe, hidden = exchange(dense.reshape(far, cores * seqs, piece), FAR, hidden)
    moe = moe.astype(F32).sum(axis=0)
    layer = (hidden.astype(F32) + moe).astype(BF16)
    last = to_all(layer.reshape(cores, seqs, piece), heads).reshape(parts, seqs, piece)
    layer_out = exchange(last, CHIPS).transpose(1, 0, 2).reshape(seqs, width)
    return (layer_out, new_state[:, None])


def solution(mesh):
    torus = Mesh(mesh.devices.reshape(8, 8, 2, mesh.shape["tp"]), (*EP, "tp"))
    in_specs = (
        P(EP, None),
        P(EP, "tp", None, None),
        P(),
        P(EP, "tp"),
        P(EP, "tp"),
        P(EP, "tp"),
        P(EP, "tp"),
        P("tp"),
        P(),
        P("tp", EP),
        P(),
        P(),
        P(),
        P(),
        P(EP, None, "tp"),
        P(EP, None, "tp"),
        P(EP, "tp", None),
    )
    out_specs = (P(EP, None), P(EP, "tp", None, None))
    return jax.shard_map(
        on_device, mesh=torus, in_specs=in_specs, out_specs=out_specs, check_vma=False
    )
```

```python
import functools

import jax
import jax.numpy as jnp
from jax import lax
from jax.experimental import pallas as pl
from jax.experimental.pallas import tpu as pltpu
from jax.sharding import Mesh
from jax.sharding import PartitionSpec as P


CAP = 16
EP = ("ep_0", "ep_1", "ep_2")
FAR = ("ep_0", "ep_1")
SLAB = ("ep_1", "ep_2")
SLAB_TP = ("ep_1", "ep_2", "tp")
CHIPS = ("tp", "ep_2")

EPSILON = 1e-06
GATE_SCALE = 16.0
F32 = jnp.float32
BF16 = jnp.bfloat16


def exchange(blocks, axes, *later):
    came = lax.all_to_all(blocks, axes, split_axis=0, concat_axis=0, tiled=True)
    return lax.optimization_barrier((came, *later)) if later else came


def on_chip(array):
    return pltpu.with_memory_space_constraint(array, pltpu.VMEM)


def to_all(shard, count):
    return jnp.broadcast_to(shard[None], (count, *shard.shape))


def prepare(experts_of, strip, *refs):
    sources, (spread, pick, along, select, rival, *kept) = refs[:12], refs[12:-3]
    own_w, ids, sems = refs[-3:]
    *weights, ids_in = sources[:6]
    width = 0
    copies = []
    for source in weights:
        place = own_w.at[:, pl.ds(width, source.shape[1])]
        copies.append(pltpu.make_async_copy(source, place, sems.at[len(copies)]))
        width += source.shape[1]
    fetched = len(copies)
    copies.append(pltpu.make_async_copy(ids_in, ids, sems.at[len(copies)]))
    for source, target in zip(sources[6:], kept, strict=True):
        copies.append(pltpu.make_async_copy(source, target, sems.at[len(copies)]))
    for copy in copies:
        copy.start()
    first, core, place, slab = experts_of()
    count = ids.shape[1]
    row = lax.broadcasted_iota(jnp.int32, (count, count), 0)
    col = lax.broadcasted_iota(jnp.int32, (count, count), 1)
    upper = jnp.where(row <= col, 1.0, 0.0).astype(BF16)
    feature = lax.broadcasted_iota(jnp.int32, (pick.shape[0] // spread.shape[0], 128), 0)
    lane = lax.broadcasted_iota(jnp.int32, feature.shape, 1)
    within = feature - place * strip == lane % strip
    for depth in range(spread.shape[0]):
        taken = within & (lane // strip == depth)
        at = feature.shape[0] * depth
        pick[at : at + feature.shape[0]] = jnp.where(taken, 1.0, 0.0).astype(BF16)
    for copy in copies[:fetched]:
        copy.wait()
    spreads = []
    for depth in range(spread.shape[0]):
        sem = sems.at[len(copies) + depth]
        spreads.append(pltpu.make_async_copy(own_w, spread.at[depth], sem))
        spreads[-1].start()
    copies[fetched].wait()
    one, two = ids[0:1, :], ids[1:2, :]
    spans = along.shape[0] // CAP
    cores = select.shape[0] // CAP
    index = lax.broadcasted_iota(jnp.int32, (spans + 8, count), 0)
    experts = index // cores * slab + place - core + index % cores
    experts = jnp.where(index < spans, experts, index - spans + first)
    named = (one == experts) | (two == experts)
    marks = jnp.where(named, 1.0, 0.0)
    ends = jnp.dot(marks.astype(BF16), upper, preferred_element_type=F32)
    slots = lax.broadcasted_iota(jnp.int32, (CAP, count), 0).astype(F32) + 1.0
    both = (one + two).astype(F32)
    own = first + core
    others = jnp.zeros((CAP, 1), F32)


    def slots_of(at):
        return jnp.where(ends[at : at + 1] == slots, marks[at : at + 1], 0.0)

    for span in range(spans):
        along[CAP * span : CAP * (span + 1)] = slots_of(span).astype(BF16)
    for c in range(cores):
        mine = slots_of(spans + c)
        select[CAP * c : CAP * (c + 1)] = mine.astype(BF16)
        total = jnp.sum(mine * both, axis=1, keepdims=True)
        others = jnp.where(core == c, total, others)
    lanes = lax.broadcasted_iota(jnp.int32, rival.shape, 1)
    rival[...] = jnp.where(lanes == others.astype(jnp.int32) - own, 1.0, 0.0)
    for copy in copies[fetched + 1 :] + spreads:
        copy.wait()


def strips_of(rows_ref, gain_ref, pick_ref, lhs_ref, res_ref):
    rows = rows_ref[...]
    pick = pick_ref[...]
    scaled = (rows.astype(F32) * gain_ref[...]).astype(BF16)
    res_ref[...] = jnp.dot(rows, pick, preferred_element_type=F32).astype(BF16)
    lhs_ref[...] = jnp.dot(scaled, pick, preferred_element_type=F32).astype(BF16)


def advance(came_ref, res_ref, bias_ref, gain_ref, old_ref, out_ref, new_ref, held_ref, sems):
    seqs, key_width, value_width = old_ref.shape
    count = came_ref.shape[0]
    seq_of = lax.broadcasted_iota(jnp.int32, (8, count), 1) % seqs
    pick = jnp.where(seq_of == lax.broadcasted_iota(jnp.int32, (8, count), 0), 1.0, 0.0)
    total = jnp.dot(pick.astype(BF16), came_ref[...], preferred_element_type=F32)[:seqs]
    res = res_ref[...].astype(F32)
    total = total * lax.rsqrt(jnp.mean(res * res, axis=1, keepdims=True) + EPSILON)
    query = total[:, :key_width].astype(BF16).astype(F32) * key_width ** (-0.5)
    key = total[:, key_width : 2 * key_width].astype(BF16).astype(F32)
    value = total[:, 2 * key_width : 2 * key_width + value_width].astype(BF16).astype(F32)
    pre = total[:, 2 * key_width + value_width :] + bias_ref[...]
    log_decay = (jnp.minimum(pre, 0.0) - jnp.log1p(jnp.exp(-jnp.abs(pre)))) / GATE_SCALE
    down = jnp.concatenate([query, key, jnp.exp(log_decay), jnp.zeros_like(query)], axis=0).T
    copies = []
    gated = []
    for seq in range(seqs):
        for at in range(0, key_width, 64):
            rows = slice(at, at + 64)
            key_col = down[rows, seqs + seq : seqs + seq + 1]
            alpha_col = down[rows, 2 * seqs + seq : 2 * seqs + seq + 1]
            new = alpha_col * old_ref[seq, rows] + key_col * value[seq : seq + 1]
            held_ref[seq, rows] = new
            source, target = held_ref.at[seq, pl.ds(at, 64)], new_ref.at[seq, pl.ds(at, 64)]
            copies.append(pltpu.make_async_copy(source, target, sems.at[len(copies)]))
            copies[-1].start()
    for seq in range(seqs):
        read = jnp.zeros((8, value_width), F32)
        for at in range(0, key_width, 64):
            rows = slice(at, at + 64)
            part = down[rows, seq : seq + 1] * held_ref[seq, rows]
            read = read + jnp.sum(part.reshape(8, 8, value_width), axis=0)
        read = jnp.sum(read, axis=0, keepdims=True)
        mean = jnp.mean(read * read, axis=1, keepdims=True)
        gated.append(read * lax.rsqrt(mean + EPSILON) * gain_ref[...])
    gated = jnp.concatenate(gated, axis=0).astype(BF16)
    for at in range(out_ref.shape[0]):
        out_ref[at] = gated
    for copy in copies:
        copy.wait()


def mix(
    which,
    expert_ref,
    came_ref,
    gain_ref,
    group_ref,
    rival_ref,
    gate_ref,
    up_ref,
    down_ref,
    out_ref,
    rows_ref,
):
    expert = which()
    size = came_ref.shape[2]
    for at in range(came_ref.shape[0]):
        rows_ref[:, size * at : size * (at + 1)] = came_ref[at].astype(F32)
    rows = rows_ref[...]
    mean = jnp.mean(rows * rows, axis=1, keepdims=True)
    rows = (rows * lax.rsqrt(mean + EPSILON) * gain_ref[...]).astype(BF16)
    gate = jnp.dot(rows, gate_ref[...], preferred_element_type=F32)
    up = jnp.dot(rows, up_ref[...], preferred_element_type=F32)
    over = (((1,), (1,)), ((), ()))
    groups = lax.dot_general(rows, group_ref[...], over, preferred_element_type=F32)
    logits = lax.dot_general(rows, expert_ref[...], over, preferred_element_type=F32)
    units = (gate * jax.nn.sigmoid(gate) * up).astype(BF16)
    output = jnp.dot(units, down_ref[...], preferred_element_type=F32)
    of_group = lax.broadcasted_iota(jnp.int32, groups.shape, 1)
    own = of_group == expert // (logits.shape[1] // groups.shape[1])
    group_logit = jnp.sum(jnp.where(own, groups, 0.0), axis=1, keepdims=True)
    share = 1.0 / jnp.sum(jnp.exp(groups - group_logit), axis=1, keepdims=True)
    lanes = lax.broadcasted_iota(jnp.int32, logits.shape, 1)
    chosen = jnp.sum(jnp.where(lanes == expert, logits, 0.0), axis=1, keepdims=True)
    rival = jnp.sum(logits * rival_ref[...], axis=1, keepdims=True)
    output = (output * (share * jax.nn.sigmoid(chosen - rival))).astype(BF16)
    piece = out_ref.shape[2]
    for at in range(out_ref.shape[0]):
        out_ref[at] = output[:, piece * at : piece * (at + 1)]


def pack(heads_ref, held_ref, res_ref, out_ref):
    value_width = heads_ref.shape[1]
    part = lax.dot_general(
        heads_ref[...],
        held_ref[:, held_ref.shape[1] - value_width :],
        (((1,), (1,)), ((), ())),
        preferred_element_type=F32,
    )
    with_res = (lax.axis_index("tp") == 0).astype(F32)
    part = part + res_ref[...].astype(F32) * with_res
    lines, lanes = out_ref.shape[1:]
    eighths = part.shape[0] // lines
    size = lanes // eighths
    group = lax.broadcasted_iota(jnp.int32, (2 * lines, lanes), 1) // size
    lower = lax.broadcasted_iota(jnp.int32, (2 * lines, lanes), 0) // lines
    for eighth in range(eighths):
        block = jnp.zeros((2 * lines, lanes), F32)
        for k in range(0, eighths, 2):
            rows = part[lines * k : lines * (k + 2)]
            for low in range(2):
                moved = pltpu.roll(rows, (size * (k + low - eighth)) % lanes, 1)
                block = jnp.where((group == k + low) & (lower == low), moved, block)
        block = (block[:lines] + block[lines:]).astype(BF16)
        quarter, core = eighth // 2, eighth % 2
        for row in range(out_ref.shape[0] // eighths):
            out_ref[eighths * row + eighths // 2 * core + quarter] = block


def dispatch(at_place, came_ref, along_ref, _, out_ref, hidden_ref, rows_ref, all_ref):
    depth, row = at_place()
    count, lines, lanes = came_ref.shape
    eighths = rows_ref.shape[0] // lines
    size = lanes // eighths
    heads = eighths // 2
    all_ref[...] = jnp.zeros_like(all_ref)
    hidden = []
    for at in range(count // heads):
        total = came_ref[heads * at].astype(F32)
        for head in range(1, heads):
            total = total + came_ref[heads * at + head].astype(F32)
        total = total.astype(BF16).astype(F32)
        both = jnp.concatenate([total, total], axis=0)
        back = pltpu.roll(both, lanes - size, 1)
        lower = lax.broadcasted_iota(jnp.int32, both.shape, 0) // lines
        hidden.append(jnp.where(lower == 0, both, back))
    group = lax.broadcasted_iota(jnp.int32, (2 * lines, lanes), 1) // size
    for k in range(0, eighths, 2):
        for half in range(2):
            block = jnp.zeros((2 * lines, lanes), F32)
            for m in range(eighths):
                moved = pltpu.roll(hidden[eighths * half + m], (size * (m - k)) % lanes, 1)
                block = jnp.where(group == m, moved, block)
            rows_ref[lines * k : lines * (k + 2), lanes * half : lanes * (half + 1)] = block
    rows = rows_ref[...].astype(BF16)
    own = hidden_ref.shape[0]
    slab = rows.shape[0]
    all_ref[pl.ds(pl.multiple_of(depth * slab, slab), slab)] = rows
    slots = jnp.dot(along_ref[...], all_ref[...], preferred_element_type=F32).astype(BF16)
    span = out_ref.shape[1]
    for at in range(out_ref.shape[0]):
        out_ref[at] = slots[span * at : span * (at + 1)]
    here = lax.broadcasted_iota(jnp.int32, (8, slab), 0)
    there = lax.broadcasted_iota(jnp.int32, (8, slab), 1)
    pick = jnp.where(there == here + own * row, 1.0, 0.0).astype(BF16)
    hidden_ref[...] = jnp.dot(pick, rows, preferred_element_type=F32)[:own].astype(BF16)


def on_device(
    residual_in,
    gla_state,
    norm_gain,
    w_query,
    w_key,
    w_value,
    w_decay,
    decay_bias,
    head_gain,
    w_output,
    ffn_gain,
    router_group,
    router_expert,
    expert_ids,
    w_gate,
    w_up,
    w_down,
):
    depths, rows, cores = (lax.axis_size(a) for a in EP)
    heads = lax.axis_size("tp")
    slab = rows * cores
    parts = cores * heads
    far = depths * rows
    tokens = expert_ids.shape[0]
    seqs, width = residual_in.shape
    strip = w_query.shape[0]
    key_width, value_width = w_query.shape[1], w_value.shape[1]
    in_width = 3 * key_width + value_width
    held = depths * strip
    piece = width // parts

    n_experts = router_expert.shape[0]

    def experts_of():
        core = lax.axis_index("ep_2")
        return lax.axis_index(FAR) * cores, core, lax.axis_index(SLAB), slab

    vmem = pl.BlockSpec(memory_space=pltpu.VMEM)
    later = (residual_in, norm_gain, head_gain, ffn_gain, decay_bias, router_group.T)
    shapes = [
        jax.ShapeDtypeStruct((depths, strip, in_width + value_width), BF16),
        pltpu.VMEM((width, held), BF16),
        pltpu.VMEM((depths * cores * CAP, tokens), BF16),
        pltpu.VMEM((cores * CAP, tokens), BF16),
        pltpu.VMEM((CAP, n_experts), F32),
        *(pltpu.VMEM(a.shape, a.dtype) for a in later),
    ]
    spread, pick, along, select, rival_lane, *later = pl.pallas_call(
        functools.partial(prepare, experts_of, strip),
        out_shape=shapes,
        in_specs=[pl.BlockSpec(memory_space=pl.ANY)] * 12,
        out_specs=[pl.BlockSpec(memory_space=pl.ANY)] + [vmem] * (len(shapes) - 1),
        scratch_shapes=[
            pltpu.VMEM((strip, in_width + value_width), BF16),
            pltpu.VMEM((expert_ids.shape[1], tokens), jnp.int32),
            pltpu.SemaphoreType.DMA((12 + depths,)),
        ],
    )(w_query, w_key, w_value, w_decay, w_output.T, expert_ids.T, *later)
    residual_in, norm_gain, head_gain, ffn_gain, decay_bias, group_rows = later
    head_gain = head_gain.astype(F32)[None]
    ffn_gain = ffn_gain.astype(F32)[None]
    decay_bias = decay_bias[None]
    norm_gain = norm_gain.astype(F32)[None]

    tied = lax.optimization_barrier(
        (spread, residual_in, pick, along, select, rival_lane, norm_gain)
        + (head_gain, ffn_gain, decay_bias)
    )
    spread, residual_in, pick, along, select, rival_lane, norm_gain, *tied = tied
    head_gain, ffn_gain, decay_bias = tied
    gathered = exchange(spread, "ep_0")
    rows_in = lax.all_gather(residual_in, SLAB, axis=0, tiled=True)
    lhs, slab_res = pl.pallas_call(
        strips_of,
        out_shape=[pltpu.VMEM((slab * seqs, held), BF16)] * 2,
        in_specs=[vmem] * 3,
        out_specs=[vmem] * 2,
    )(on_chip(rows_in), on_chip(norm_gain), on_chip(pick))
    gathered, lhs, slab_res = lax.optimization_barrier((gathered, lhs, slab_res))
    gathered = gathered.reshape(held, in_width + value_width)
    sums = jnp.dot(lhs, gathered[:, :in_width], preferred_element_type=F32).astype(BF16)
    arrived = exchange(sums.reshape(slab, seqs, in_width), SLAB)
    gated, new_state = pl.pallas_call(
        advance,
        out_shape=[
            pltpu.VMEM((slab, seqs, value_width), BF16),
            jax.ShapeDtypeStruct((seqs, key_width, value_width), F32),
        ],
        in_specs=[vmem] * 5,
        out_specs=[vmem, pl.BlockSpec(memory_space=pl.ANY)],
        scratch_shapes=[
            pltpu.VMEM((seqs, key_width, value_width), F32),
            pltpu.SemaphoreType.DMA((seqs * key_width // 64,)),
        ],
    )(*map(on_chip, (arrived.reshape(slab * seqs, in_width), residual_in, decay_bias, head_gain, gla_state[:, 0])))

    slab_heads, slab_res = exchange(gated, SLAB, slab_res)
    slab_heads = slab_heads.reshape(slab * seqs, value_width)
    lines = slab * seqs // parts
    came = pl.pallas_call(
        pack,
        out_shape=pltpu.VMEM((slab * heads, lines, held), BF16),
        in_specs=[vmem] * 3,
        out_specs=vmem,
    )(*map(on_chip, (slab_heads, gathered, slab_res)))
    came = exchange(came, SLAB_TP)
    router = on_chip(router_expert)

    def at_place():
        return lax.axis_index("ep_0"), lax.axis_index("ep_1")

    outward, hidden = pl.pallas_call(
        functools.partial(dispatch, at_place),
        out_shape=[
            pltpu.VMEM((depths, cores * CAP, piece), BF16),
            pltpu.VMEM((cores * seqs, piece), BF16),
        ],
        in_specs=[vmem] * 3,
        out_specs=[vmem] * 2,
        scratch_shapes=[
            pltpu.VMEM((slab * seqs, piece), F32),
            pltpu.VMEM((tokens, piece), BF16),
        ],
    )(on_chip(came), on_chip(along), router)
    slot_part = exchange(outward, "ep_0").astype(F32).sum(axis=0).astype(BF16)
    slot_part = to_all(slot_part.reshape(cores, CAP, piece), heads)
    came = exchange(slot_part.reshape(parts, CAP, piece), CHIPS)
    operands = (came, ffn_gain, group_rows, rival_lane)
    operands += (w_gate[0], w_up[0], w_down[0])
    back = pl.pallas_call(
        functools.partial(mix, lambda: lax.axis_index(EP)),
        out_shape=pltpu.VMEM((parts, CAP, piece), BF16),
        in_specs=[vmem] * (1 + len(operands)),
        out_specs=vmem,
        scratch_shapes=[pltpu.VMEM((CAP, width), F32)],
    )(router, *map(on_chip, operands))
    summed = exchange(back, CHIPS).reshape(heads, cores, CAP, piece).astype(F32).sum(axis=0)
    dense = lax.dot_general(
        select,
        summed.astype(BF16).reshape(cores * CAP, piece),
        (((0,), (0,)), ((), ())),
        preferred_element_type=F32,
    ).astype(BF16)
    moe, hidden = exchange(dense.reshape(far, cores * seqs, piece), FAR, hidden)
    moe = moe.astype(F32).sum(axis=0)
    layer = (hidden.astype(F32) + moe).astype(BF16)
    last = to_all(layer.reshape(cores, seqs, piece), heads).reshape(parts, seqs, piece)
    layer_out = exchange(last, CHIPS).transpose(1, 0, 2).reshape(seqs, width)
    return (layer_out, new_state[:, None])


def solution(mesh):
    torus = Mesh(mesh.devices.reshape(8, 8, 2, mesh.shape["tp"]), (*EP, "tp"))
    in_specs = (
        P(EP, None),
        P(EP, "tp", None, None),
        P(),
        P(EP, "tp"),
        P(EP, "tp"),
        P(EP, "tp"),
        P(EP, "tp"),
        P("tp"),
        P(),
        P("tp", EP),
        P(),
        P(),
        P(),
        P(),
        P(EP, None, "tp"),
        P(EP, None, "tp"),
        P(EP, "tp", None),
    )
    out_specs = (P(EP, None), P(EP, "tp", None, None))
    return jax.shard_map(
        on_device, mesh=torus, in_specs=in_specs, out_specs=out_specs, check_vma=False
    )
```

```python
import functools

import jax
import jax.numpy as jnp
from jax import lax
from jax.experimental import pallas as pl
from jax.experimental.pallas import tpu as pltpu
from jax.sharding import Mesh
from jax.sharding import PartitionSpec as P


CAP = 16
EP = ("ep_0", "ep_1", "ep_2")
FAR = ("ep_0", "ep_1")
SLAB = ("ep_1", "ep_2")
SLAB_TP = ("ep_1", "ep_2", "tp")
CHIPS = ("tp", "ep_2")

EPSILON = 1e-06
GATE_SCALE = 16.0
F32 = jnp.float32
BF16 = jnp.bfloat16


def exchange(blocks, axes, *later):
    came = lax.all_to_all(blocks, axes, split_axis=0, concat_axis=0, tiled=True)
    return lax.optimization_barrier((came, *later)) if later else came


def on_chip(array):
    return pltpu.with_memory_space_constraint(array, pltpu.VMEM)


def kernel_call(body, **settings):
    params = pltpu.CompilerParams(vmem_limit_bytes=6 * 2**20)
    return pl.pallas_call(body, compiler_params=params, **settings)


def to_all(shard, count):
    return jnp.broadcast_to(shard[None], (count, *shard.shape))


def prepare(experts_of, strip, *refs):
    sources, (spread, pick, along, select, rival, *kept) = refs[:12], refs[12:-3]
    own_w, ids, sems = refs[-3:]
    *weights, ids_in = sources[:6]
    width = 0
    copies = []
    for source in weights:
        place = own_w.at[:, pl.ds(width, source.shape[1])]
        copies.append(pltpu.make_async_copy(source, place, sems.at[len(copies)]))
        width += source.shape[1]
    fetched = len(copies)
    copies.append(pltpu.make_async_copy(ids_in, ids, sems.at[len(copies)]))
    for source, target in zip(sources[6:], kept, strict=True):
        copies.append(pltpu.make_async_copy(source, target, sems.at[len(copies)]))
    for copy in copies:
        copy.start()
    first, core, place, slab = experts_of()
    count = ids.shape[1]
    row = lax.broadcasted_iota(jnp.int32, (count, count), 0)
    col = lax.broadcasted_iota(jnp.int32, (count, count), 1)
    upper = jnp.where(row <= col, 1.0, 0.0).astype(BF16)
    feature = lax.broadcasted_iota(jnp.int32, (pick.shape[0] // spread.shape[0], 128), 0)
    lane = lax.broadcasted_iota(jnp.int32, feature.shape, 1)
    within = feature - place * strip == lane % strip
    for depth in range(spread.shape[0]):
        taken = within & (lane // strip == depth)
        at = feature.shape[0] * depth
        pick[at : at + feature.shape[0]] = jnp.where(taken, 1.0, 0.0).astype(BF16)
    for copy in copies[:fetched]:
        copy.wait()
    spreads = []
    for depth in range(spread.shape[0]):
        sem = sems.at[len(copies) + depth]
        spreads.append(pltpu.make_async_copy(own_w, spread.at[depth], sem))
        spreads[-1].start()
    copies[fetched].wait()
    one, two = ids[0:1, :], ids[1:2, :]
    spans = along.shape[0] // CAP
    cores = select.shape[0] // CAP
    index = lax.broadcasted_iota(jnp.int32, (spans + 8, count), 0)
    experts = index // cores * slab + place - core + index % cores
    experts = jnp.where(index < spans, experts, index - spans + first)
    named = (one == experts) | (two == experts)
    marks = jnp.where(named, 1.0, 0.0)
    ends = jnp.dot(marks.astype(BF16), upper, preferred_element_type=F32)
    slots = lax.broadcasted_iota(jnp.int32, (CAP, count), 0).astype(F32) + 1.0
    both = (one + two).astype(F32)
    own = first + core
    others = jnp.zeros((CAP, 1), F32)


    def slots_of(at):
        return jnp.where(ends[at : at + 1] == slots, marks[at : at + 1], 0.0)

    for span in range(spans):
        along[CAP * span : CAP * (span + 1)] = slots_of(span).astype(BF16)
    for c in range(cores):
        mine = slots_of(spans + c)
        select[CAP * c : CAP * (c + 1)] = mine.astype(BF16)
        total = jnp.sum(mine * both, axis=1, keepdims=True)
        others = jnp.where(core == c, total, others)
    lanes = lax.broadcasted_iota(jnp.int32, rival.shape, 1)
    rival[...] = jnp.where(lanes == others.astype(jnp.int32) - own, 1.0, 0.0)
    for copy in copies[fetched + 1 :] + spreads:
        copy.wait()


def strips_of(rows_ref, gain_ref, pick_ref, lhs_ref, res_ref):
    rows = rows_ref[...]
    pick = pick_ref[...]
    scaled = (rows.astype(F32) * gain_ref[...]).astype(BF16)
    res_ref[...] = jnp.dot(rows, pick, preferred_element_type=F32).astype(BF16)
    lhs_ref[...] = jnp.dot(scaled, pick, preferred_element_type=F32).astype(BF16)


def advance(came_ref, res_ref, bias_ref, gain_ref, old_ref, out_ref, held_ref):
    seqs, key_width, value_width = old_ref.shape
    count = came_ref.shape[0]
    seq_of = lax.broadcasted_iota(jnp.int32, (8, count), 1) % seqs
    pick = jnp.where(seq_of == lax.broadcasted_iota(jnp.int32, (8, count), 0), 1.0, 0.0)
    total = jnp.dot(pick.astype(BF16), came_ref[...], preferred_element_type=F32)[:seqs]
    res = res_ref[...].astype(F32)
    total = total * lax.rsqrt(jnp.mean(res * res, axis=1, keepdims=True) + EPSILON)
    query = total[:, :key_width].astype(BF16).astype(F32) * key_width ** (-0.5)
    key = total[:, key_width : 2 * key_width].astype(BF16).astype(F32)
    value = total[:, 2 * key_width : 2 * key_width + value_width].astype(BF16).astype(F32)
    pre = total[:, 2 * key_width + value_width :] + bias_ref[...]
    log_decay = (jnp.minimum(pre, 0.0) - jnp.log1p(jnp.exp(-jnp.abs(pre)))) / GATE_SCALE
    down = jnp.concatenate([query, key, jnp.exp(log_decay), jnp.zeros_like(query)], axis=0).T
    gated = []
    for seq in range(seqs):
        for at in range(0, key_width, 64):
            rows = slice(at, at + 64)
            key_col = down[rows, seqs + seq : seqs + seq + 1]
            alpha_col = down[rows, 2 * seqs + seq : 2 * seqs + seq + 1]
            new = alpha_col * old_ref[seq, rows] + key_col * value[seq : seq + 1]
            held_ref[seq, rows] = new
    for seq in range(seqs):
        read = jnp.zeros((8, value_width), F32)
        for at in range(0, key_width, 64):
            rows = slice(at, at + 64)
            part = down[rows, seq : seq + 1] * held_ref[seq, rows]
            read = read + jnp.sum(part.reshape(8, 8, value_width), axis=0)
        read = jnp.sum(read, axis=0, keepdims=True)
        mean = jnp.mean(read * read, axis=1, keepdims=True)
        gated.append(read * lax.rsqrt(mean + EPSILON) * gain_ref[...])
    gated = jnp.concatenate(gated, axis=0).astype(BF16)
    for at in range(out_ref.shape[0]):
        out_ref[at] = gated


def mix(
    which,
    expert_ref,
    came_ref,
    gain_ref,
    group_ref,
    rival_ref,
    gate_ref,
    up_ref,
    down_ref,
    state_ref,
    out_ref,
    new_ref,
    rows_ref,
    router_ref,
    sems,
):
    fetch = pltpu.make_async_copy(expert_ref, router_ref, sems.at[0])
    fetch.start()
    copy = pltpu.make_async_copy(state_ref, new_ref, sems.at[1])
    copy.start()
    expert = which()
    size = came_ref.shape[2]
    for at in range(came_ref.shape[0]):
        rows_ref[:, size * at : size * (at + 1)] = came_ref[at].astype(F32)
    rows = rows_ref[...]
    mean = jnp.mean(rows * rows, axis=1, keepdims=True)
    rows = (rows * lax.rsqrt(mean + EPSILON) * gain_ref[...]).astype(BF16)
    gate = jnp.dot(rows, gate_ref[...], preferred_element_type=F32)
    up = jnp.dot(rows, up_ref[...], preferred_element_type=F32)
    over = (((1,), (1,)), ((), ()))
    groups = lax.dot_general(rows, group_ref[...], over, preferred_element_type=F32)
    units = (gate * jax.nn.sigmoid(gate) * up).astype(BF16)
    output = jnp.dot(units, down_ref[...], preferred_element_type=F32)
    fetch.wait()
    logits = lax.dot_general(rows, router_ref[...], over, preferred_element_type=F32)
    of_group = lax.broadcasted_iota(jnp.int32, groups.shape, 1)
    own = of_group == expert // (logits.shape[1] // groups.shape[1])
    group_logit = jnp.sum(jnp.where(own, groups, 0.0), axis=1, keepdims=True)
    share = 1.0 / jnp.sum(jnp.exp(groups - group_logit), axis=1, keepdims=True)
    lanes = lax.broadcasted_iota(jnp.int32, logits.shape, 1)
    chosen = jnp.sum(jnp.where(lanes == expert, logits, 0.0), axis=1, keepdims=True)
    rival = jnp.sum(logits * rival_ref[...], axis=1, keepdims=True)
    output = (output * (share * jax.nn.sigmoid(chosen - rival))).astype(BF16)
    piece = out_ref.shape[2]
    for at in range(out_ref.shape[0]):
        out_ref[at] = output[:, piece * at : piece * (at + 1)]
    copy.wait()


def pack(heads_ref, held_ref, res_ref, _, out_ref, __):
    value_width = heads_ref.shape[1]
    part = lax.dot_general(
        heads_ref[...],
        held_ref[:, held_ref.shape[1] - value_width :],
        (((1,), (1,)), ((), ())),
        preferred_element_type=F32,
    )
    with_res = (lax.axis_index("tp") == 0).astype(F32)
    part = part + res_ref[...].astype(F32) * with_res
    lines, lanes = out_ref.shape[1:]
    eighths = part.shape[0] // lines
    size = lanes // eighths
    group = lax.broadcasted_iota(jnp.int32, (2 * lines, lanes), 1) // size
    lower = lax.broadcasted_iota(jnp.int32, (2 * lines, lanes), 0) // lines
    for eighth in range(eighths):
        block = jnp.zeros((2 * lines, lanes), F32)
        for k in range(0, eighths, 2):
            rows = part[lines * k : lines * (k + 2)]
            for low in range(2):
                moved = pltpu.roll(rows, (size * (k + low - eighth)) % lanes, 1)
                block = jnp.where((group == k + low) & (lower == low), moved, block)
        block = (block[:lines] + block[lines:]).astype(BF16)
        quarter, core = eighth // 2, eighth % 2
        for row in range(out_ref.shape[0] // eighths):
            out_ref[eighths * row + eighths // 2 * core + quarter] = block


def dispatch(at_place, came_ref, along_ref, _, out_ref, hidden_ref, __, rows_ref, all_ref):
    depth, row = at_place()
    count, lines, lanes = came_ref.shape
    eighths = rows_ref.shape[0] // lines
    size = lanes // eighths
    heads = eighths // 2
    all_ref[...] = jnp.zeros_like(all_ref)
    hidden = []
    for at in range(count // heads):
        total = came_ref[heads * at].astype(F32)
        for head in range(1, heads):
            total = total + came_ref[heads * at + head].astype(F32)
        total = total.astype(BF16).astype(F32)
        both = jnp.concatenate([total, total], axis=0)
        back = pltpu.roll(both, lanes - size, 1)
        lower = lax.broadcasted_iota(jnp.int32, both.shape, 0) // lines
        hidden.append(jnp.where(lower == 0, both, back))
    group = lax.broadcasted_iota(jnp.int32, (2 * lines, lanes), 1) // size
    for k in range(0, eighths, 2):
        for half in range(2):
            block = jnp.zeros((2 * lines, lanes), F32)
            for m in range(eighths):
                moved = pltpu.roll(hidden[eighths * half + m], (size * (m - k)) % lanes, 1)
                block = jnp.where(group == m, moved, block)
            rows_ref[lines * k : lines * (k + 2), lanes * half : lanes * (half + 1)] = block
    rows = rows_ref[...].astype(BF16)
    own = hidden_ref.shape[0]
    slab = rows.shape[0]
    all_ref[pl.ds(pl.multiple_of(depth * slab, slab), slab)] = rows
    slots = jnp.dot(along_ref[...], all_ref[...], preferred_element_type=F32).astype(BF16)
    span = out_ref.shape[1]
    for at in range(out_ref.shape[0]):
        out_ref[at] = slots[span * at : span * (at + 1)]
    here = lax.broadcasted_iota(jnp.int32, (8, slab), 0)
    there = lax.broadcasted_iota(jnp.int32, (8, slab), 1)
    pick = jnp.where(there == here + own * row, 1.0, 0.0).astype(BF16)
    hidden_ref[...] = jnp.dot(pick, rows, preferred_element_type=F32)[:own].astype(BF16)


def on_device(
    residual_in,
    gla_state,
    norm_gain,
    w_query,
    w_key,
    w_value,
    w_decay,
    decay_bias,
    head_gain,
    w_output,
    ffn_gain,
    router_group,
    router_expert,
    expert_ids,
    w_gate,
    w_up,
    w_down,
):
    depths, rows, cores = (lax.axis_size(a) for a in EP)
    heads = lax.axis_size("tp")
    slab = rows * cores
    parts = cores * heads
    far = depths * rows
    tokens = expert_ids.shape[0]
    seqs, width = residual_in.shape
    strip = w_query.shape[0]
    key_width, value_width = w_query.shape[1], w_value.shape[1]
    in_width = 3 * key_width + value_width
    held = depths * strip
    piece = width // parts

    n_experts = router_expert.shape[0]

    def experts_of():
        core = lax.axis_index("ep_2")
        return lax.axis_index(FAR) * cores, core, lax.axis_index(SLAB), slab

    vmem = pl.BlockSpec(memory_space=pltpu.VMEM)
    later = (residual_in, norm_gain, head_gain, ffn_gain, decay_bias, router_group.T)
    shapes = [
        jax.ShapeDtypeStruct((depths, strip, in_width + value_width), BF16),
        pltpu.VMEM((width, held), BF16),
        pltpu.VMEM((depths * cores * CAP, tokens), BF16),
        pltpu.VMEM((cores * CAP, tokens), BF16),
        pltpu.VMEM((CAP, n_experts), F32),
        *(pltpu.VMEM(a.shape, a.dtype) for a in later),
    ]
    spread, pick, along, select, rival_lane, *later = pl.pallas_call(
        functools.partial(prepare, experts_of, strip),
        out_shape=shapes,
        in_specs=[pl.BlockSpec(memory_space=pl.ANY)] * 12,
        out_specs=[pl.BlockSpec(memory_space=pl.ANY)] + [vmem] * (len(shapes) - 1),
        scratch_shapes=[
            pltpu.VMEM((strip, in_width + value_width), BF16),
            pltpu.VMEM((expert_ids.shape[1], tokens), jnp.int32),
            pltpu.SemaphoreType.DMA((12 + depths,)),
        ],
    )(w_query, w_key, w_value, w_decay, w_output.T, expert_ids.T, *later)
    residual_in, norm_gain, head_gain, ffn_gain, decay_bias, group_rows = later
    head_gain = head_gain.astype(F32)[None]
    ffn_gain = ffn_gain.astype(F32)[None]
    decay_bias = decay_bias[None]
    norm_gain = norm_gain.astype(F32)[None]

    tied = lax.optimization_barrier(
        (spread, residual_in, pick, along, select, rival_lane, norm_gain)
        + (head_gain, ffn_gain, decay_bias)
    )
    spread, residual_in, pick, along, select, rival_lane, norm_gain, *tied = tied
    head_gain, ffn_gain, decay_bias = tied
    gathered = exchange(spread, "ep_0")
    rows_in = lax.all_gather(residual_in, SLAB, axis=0, tiled=True)
    lhs, slab_res = kernel_call(
        strips_of,
        out_shape=[pltpu.VMEM((slab * seqs, held), BF16)] * 2,
        in_specs=[vmem] * 3,
        out_specs=[vmem] * 2,
    )(on_chip(rows_in), on_chip(norm_gain), on_chip(pick))
    gathered, lhs, slab_res = lax.optimization_barrier((gathered, lhs, slab_res))
    gathered = gathered.reshape(held, in_width + value_width)
    sums = jnp.dot(lhs, gathered[:, :in_width], preferred_element_type=F32).astype(BF16)
    arrived = exchange(sums.reshape(slab, seqs, in_width), SLAB)
    gated, new_state = kernel_call(
        advance,
        out_shape=[
            pltpu.VMEM((slab, seqs, value_width), BF16),
            pltpu.VMEM((seqs, key_width, value_width), F32),
        ],
        in_specs=[vmem] * 5,
        out_specs=[vmem] * 2,
    )(*map(on_chip, (arrived.reshape(slab * seqs, in_width), residual_in, decay_bias, head_gain, gla_state[:, 0])))

    slab_heads, slab_res = exchange(gated, SLAB, slab_res)
    slab_heads = slab_heads.reshape(slab * seqs, value_width)
    lines = slab * seqs // parts
    state = pltpu.VMEM(new_state.shape, F32)
    came, new_state = kernel_call(
        pack,
        out_shape=[pltpu.VMEM((slab * heads, lines, held), BF16), state],
        in_specs=[vmem] * 4,
        out_specs=[vmem] * 2,
        input_output_aliases={3: 1},
    )(*map(on_chip, (slab_heads, gathered, slab_res, new_state)))
    came = exchange(came, SLAB_TP)

    def at_place():
        return lax.axis_index("ep_0"), lax.axis_index("ep_1")

    outward, hidden, new_state = kernel_call(
        functools.partial(dispatch, at_place),
        out_shape=[
            pltpu.VMEM((depths, cores * CAP, piece), BF16),
            pltpu.VMEM((cores * seqs, piece), BF16),
            state,
        ],
        in_specs=[vmem] * 3,
        out_specs=[vmem] * 3,
        scratch_shapes=[
            pltpu.VMEM((slab * seqs, piece), F32),
            pltpu.VMEM((tokens, piece), BF16),
        ],
        input_output_aliases={2: 2},
    )(on_chip(came), on_chip(along), on_chip(new_state))
    slot_part = exchange(outward, "ep_0").astype(F32).sum(axis=0).astype(BF16)
    slot_part = to_all(slot_part.reshape(cores, CAP, piece), heads)
    came = exchange(slot_part.reshape(parts, CAP, piece), CHIPS)
    operands = (came, ffn_gain, group_rows, rival_lane)
    operands += (w_gate[0], w_up[0], w_down[0], new_state)
    back, new_state = kernel_call(
        functools.partial(mix, lambda: lax.axis_index(EP)),
        out_shape=[
            pltpu.VMEM((parts, CAP, piece), BF16),
            jax.ShapeDtypeStruct(new_state.shape, F32),
        ],
        in_specs=[pl.BlockSpec(memory_space=pl.ANY)] + [vmem] * len(operands),
        out_specs=[vmem, pl.BlockSpec(memory_space=pl.ANY)],
        scratch_shapes=[
            pltpu.VMEM((CAP, width), F32),
            pltpu.VMEM(router_expert.shape, BF16),
            pltpu.SemaphoreType.DMA((2,)),
        ],
    )(router_expert, *map(on_chip, operands))
    summed = exchange(back, CHIPS).reshape(heads, cores, CAP, piece).astype(F32).sum(axis=0)
    dense = lax.dot_general(
        select,
        summed.astype(BF16).reshape(cores * CAP, piece),
        (((0,), (0,)), ((), ())),
        preferred_element_type=F32,
    ).astype(BF16)
    moe, hidden = exchange(dense.reshape(far, cores * seqs, piece), FAR, hidden)
    moe = moe.astype(F32).sum(axis=0)
    layer = (hidden.astype(F32) + moe).astype(BF16)
    last = to_all(layer.reshape(cores, seqs, piece), heads).reshape(parts, seqs, piece)
    layer_out = exchange(last, CHIPS).transpose(1, 0, 2).reshape(seqs, width)
    return (layer_out, new_state[:, None])


def solution(mesh):
    torus = Mesh(mesh.devices.reshape(8, 8, 2, mesh.shape["tp"]), (*EP, "tp"))
    in_specs = (
        P(EP, None),
        P(EP, "tp", None, None),
        P(),
        P(EP, "tp"),
        P(EP, "tp"),
        P(EP, "tp"),
        P(EP, "tp"),
        P("tp"),
        P(),
        P("tp", EP),
        P(),
        P(),
        P(),
        P(),
        P(EP, None, "tp"),
        P(EP, None, "tp"),
        P(EP, "tp", None),
    )
    out_specs = (P(EP, None), P(EP, "tp", None, None))
    return jax.shard_map(
        on_device, mesh=torus, in_specs=in_specs, out_specs=out_specs, check_vma=False
    )
```

```python
import functools

import jax
import jax.numpy as jnp
from jax import lax
from jax.experimental import pallas as pl
from jax.experimental.pallas import tpu as pltpu
from jax.sharding import Mesh
from jax.sharding import PartitionSpec as P


CAP = 16
EP = ("ep_0", "ep_1", "ep_2")
FAR = ("ep_0", "ep_1")
SLAB = ("ep_1", "ep_2")
SLAB_TP = ("ep_1", "ep_2", "tp")
CHIPS = ("tp", "ep_2")

EPSILON = 1e-06
GATE_SCALE = 16.0
F32 = jnp.float32
BF16 = jnp.bfloat16


def exchange(blocks, axes, *later):
    came = lax.all_to_all(blocks, axes, split_axis=0, concat_axis=0, tiled=True)
    return lax.optimization_barrier((came, *later)) if later else came


def on_chip(array):
    return pltpu.with_memory_space_constraint(array, pltpu.VMEM)


def kernel_call(body, **settings):
    params = pltpu.CompilerParams(vmem_limit_bytes=6 * 2**20)
    return pl.pallas_call(body, compiler_params=params, **settings)


def to_all(shard, count):
    return jnp.broadcast_to(shard[None], (count, *shard.shape))


def prepare(experts_of, strip, *refs):
    sources, (spread, pick, along, select, rival, *kept) = refs[:12], refs[12:-3]
    own_w, ids, sems = refs[-3:]
    *weights, ids_in = sources[:6]
    width = 0
    copies = []
    for source in weights:
        place = own_w.at[:, pl.ds(width, source.shape[1])]
        copies.append(pltpu.make_async_copy(source, place, sems.at[len(copies)]))
        width += source.shape[1]
    fetched = len(copies)
    copies.append(pltpu.make_async_copy(ids_in, ids, sems.at[len(copies)]))
    for source, target in zip(sources[6:], kept, strict=True):
        copies.append(pltpu.make_async_copy(source, target, sems.at[len(copies)]))
    for copy in copies:
        copy.start()
    first, core, place, slab = experts_of()
    count = ids.shape[1]
    row = lax.broadcasted_iota(jnp.int32, (count, count), 0)
    col = lax.broadcasted_iota(jnp.int32, (count, count), 1)
    upper = jnp.where(row <= col, 1.0, 0.0).astype(BF16)
    feature = lax.broadcasted_iota(jnp.int32, (pick.shape[0] // spread.shape[0], 128), 0)
    lane = lax.broadcasted_iota(jnp.int32, feature.shape, 1)
    within = feature - place * strip == lane % strip
    for depth in range(spread.shape[0]):
        taken = within & (lane // strip == depth)
        at = feature.shape[0] * depth
        pick[at : at + feature.shape[0]] = jnp.where(taken, 1.0, 0.0).astype(BF16)
    for copy in copies[:fetched]:
        copy.wait()
    spreads = []
    for depth in range(spread.shape[0]):
        sem = sems.at[len(copies) + depth]
        spreads.append(pltpu.make_async_copy(own_w, spread.at[depth], sem))
        spreads[-1].start()
    copies[fetched].wait()
    one, two = ids[0:1, :], ids[1:2, :]
    spans = along.shape[0] // CAP
    cores = select.shape[0] // CAP
    index = lax.broadcasted_iota(jnp.int32, (spans + 8, count), 0)
    experts = index // cores * slab + place - core + index % cores
    experts = jnp.where(index < spans, experts, index - spans + first)
    named = (one == experts) | (two == experts)
    marks = jnp.where(named, 1.0, 0.0)
    ends = jnp.dot(marks.astype(BF16), upper, preferred_element_type=F32)
    slots = lax.broadcasted_iota(jnp.int32, (CAP, count), 0).astype(F32) + 1.0
    both = (one + two).astype(F32)
    own = first + core
    others = jnp.zeros((CAP, 1), F32)


    def slots_of(at):
        return jnp.where(ends[at : at + 1] == slots, marks[at : at + 1], 0.0)

    for span in range(spans):
        along[CAP * span : CAP * (span + 1)] = slots_of(span).astype(BF16)
    for c in range(cores):
        mine = slots_of(spans + c)
        select[CAP * c : CAP * (c + 1)] = mine.astype(BF16)
        total = jnp.sum(mine * both, axis=1, keepdims=True)
        others = jnp.where(core == c, total, others)
    lanes = lax.broadcasted_iota(jnp.int32, rival.shape, 1)
    rival[...] = jnp.where(lanes == others.astype(jnp.int32) - own, 1.0, 0.0)
    for copy in copies[fetched + 1 :] + spreads:
        copy.wait()


def strips_of(rows_ref, gain_ref, pick_ref, lhs_ref, res_ref):
    rows = rows_ref[...]
    pick = pick_ref[...]
    scaled = (rows.astype(F32) * gain_ref[...]).astype(BF16)
    res_ref[...] = jnp.dot(rows, pick, preferred_element_type=F32).astype(BF16)
    lhs_ref[...] = jnp.dot(scaled, pick, preferred_element_type=F32).astype(BF16)


def advance(came_ref, res_ref, bias_ref, gain_ref, old_ref, out_ref, held_ref):
    seqs, key_width, value_width = old_ref.shape
    count = came_ref.shape[0]
    seq_of = lax.broadcasted_iota(jnp.int32, (8, count), 1) % seqs
    pick = jnp.where(seq_of == lax.broadcasted_iota(jnp.int32, (8, count), 0), 1.0, 0.0)
    total = jnp.dot(pick.astype(BF16), came_ref[...], preferred_element_type=F32)[:seqs]
    res = res_ref[...].astype(F32)
    total = total * lax.rsqrt(jnp.mean(res * res, axis=1, keepdims=True) + EPSILON)
    query = total[:, :key_width].astype(BF16).astype(F32) * key_width ** (-0.5)
    key = total[:, key_width : 2 * key_width].astype(BF16).astype(F32)
    value = total[:, 2 * key_width : 2 * key_width + value_width].astype(BF16).astype(F32)
    pre = total[:, 2 * key_width + value_width :] + bias_ref[...]
    log_decay = (jnp.minimum(pre, 0.0) - jnp.log1p(jnp.exp(-jnp.abs(pre)))) / GATE_SCALE
    down = jnp.concatenate([query, key, jnp.exp(log_decay), jnp.zeros_like(query)], axis=0).T
    gated = []
    for seq in range(seqs):
        for at in range(0, key_width, 64):
            rows = slice(at, at + 64)
            key_col = down[rows, seqs + seq : seqs + seq + 1]
            alpha_col = down[rows, 2 * seqs + seq : 2 * seqs + seq + 1]
            new = alpha_col * old_ref[seq, rows] + key_col * value[seq : seq + 1]
            held_ref[seq, rows] = new
    for seq in range(seqs):
        read = jnp.zeros((8, value_width), F32)
        for at in range(0, key_width, 64):
            rows = slice(at, at + 64)
            part = down[rows, seq : seq + 1] * held_ref[seq, rows]
            read = read + jnp.sum(part.reshape(8, 8, value_width), axis=0)
        read = jnp.sum(read, axis=0, keepdims=True)
        mean = jnp.mean(read * read, axis=1, keepdims=True)
        gated.append(read * lax.rsqrt(mean + EPSILON) * gain_ref[...])
    gated = jnp.concatenate(gated, axis=0).astype(BF16)
    for at in range(out_ref.shape[0]):
        out_ref[at] = gated


def mix(
    which,
    expert_ref,
    came_ref,
    gain_ref,
    group_ref,
    rival_ref,
    gate_ref,
    up_ref,
    down_ref,
    state_ref,
    out_ref,
    new_ref,
    rows_ref,
    router_ref,
    sems,
):
    fetch = pltpu.make_async_copy(expert_ref, router_ref, sems.at[0])
    fetch.start()
    copies = []
    for seq in range(state_ref.shape[0]):
        for at in range(0, state_ref.shape[1], 64):
            source, target = state_ref.at[seq, pl.ds(at, 64)], new_ref.at[seq, pl.ds(at, 64)]
            copies.append(pltpu.make_async_copy(source, target, sems.at[1 + len(copies)]))
            copies[-1].start()
    expert = which()
    size = came_ref.shape[2]
    for at in range(came_ref.shape[0]):
        rows_ref[:, size * at : size * (at + 1)] = came_ref[at].astype(F32)
    rows = rows_ref[...]
    mean = jnp.mean(rows * rows, axis=1, keepdims=True)
    rows = (rows * lax.rsqrt(mean + EPSILON) * gain_ref[...]).astype(BF16)
    gate = jnp.dot(rows, gate_ref[...], preferred_element_type=F32)
    up = jnp.dot(rows, up_ref[...], preferred_element_type=F32)
    floats = rows.astype(F32)
    count = group_ref.shape[0]
    group_rows = group_ref[...].astype(F32)
    groups = [
        jnp.sum(floats * group_rows[at : at + 1], axis=1, keepdims=True) for at in range(count)
    ]
    units = (gate * jax.nn.sigmoid(gate) * up).astype(BF16)
    output = jnp.dot(units, down_ref[...], preferred_element_type=F32)
    experts = router_ref.shape[0]
    own = expert // (experts // count)
    group_logit = groups[0]
    for at in range(1, count):
        group_logit = jnp.where(own == at, groups[at], group_logit)
    total = jnp.zeros_like(group_logit)
    for logit in groups:
        total = total + jnp.exp(logit - group_logit)
    share = 1.0 / total
    lanes = lax.broadcasted_iota(jnp.int32, rival_ref.shape, 1)
    apart = jnp.where(lanes == expert, 1.0, 0.0) - rival_ref[...]
    fetch.wait()
    apart = jnp.dot(apart.astype(BF16), router_ref[...], preferred_element_type=F32)
    lead = jnp.sum(floats * apart, axis=1, keepdims=True)
    output = (output * (share * jax.nn.sigmoid(lead))).astype(BF16)
    piece = out_ref.shape[2]
    for at in range(out_ref.shape[0]):
        out_ref[at] = output[:, piece * at : piece * (at + 1)]
    for copy in copies:
        copy.wait()


def pack(heads_ref, held_ref, res_ref, _, out_ref, __):
    value_width = heads_ref.shape[1]
    part = lax.dot_general(
        heads_ref[...],
        held_ref[:, held_ref.shape[1] - value_width :],
        (((1,), (1,)), ((), ())),
        preferred_element_type=F32,
    )
    with_res = (lax.axis_index("tp") == 0).astype(F32)
    part = part + res_ref[...].astype(F32) * with_res
    lines, lanes = out_ref.shape[1:]
    eighths = part.shape[0] // lines
    size = lanes // eighths
    group = lax.broadcasted_iota(jnp.int32, (2 * lines, lanes), 1) // size
    lower = lax.broadcasted_iota(jnp.int32, (2 * lines, lanes), 0) // lines
    for eighth in range(eighths):
        block = jnp.zeros((2 * lines, lanes), F32)
        for k in range(0, eighths, 2):
            rows = part[lines * k : lines * (k + 2)]
            for low in range(2):
                moved = pltpu.roll(rows, (size * (k + low - eighth)) % lanes, 1)
                block = jnp.where((group == k + low) & (lower == low), moved, block)
        block = (block[:lines] + block[lines:]).astype(BF16)
        quarter, core = eighth // 2, eighth % 2
        for row in range(out_ref.shape[0] // eighths):
            out_ref[eighths * row + eighths // 2 * core + quarter] = block


def dispatch(at_place, came_ref, along_ref, _, out_ref, hidden_ref, __, rows_ref, all_ref):
    depth, row = at_place()
    count, lines, lanes = came_ref.shape
    eighths = rows_ref.shape[0] // lines
    size = lanes // eighths
    heads = eighths // 2
    all_ref[...] = jnp.zeros_like(all_ref)
    hidden = []
    for at in range(count // heads):
        total = came_ref[heads * at].astype(F32)
        for head in range(1, heads):
            total = total + came_ref[heads * at + head].astype(F32)
        total = total.astype(BF16).astype(F32)
        both = jnp.concatenate([total, total], axis=0)
        back = pltpu.roll(both, lanes - size, 1)
        lower = lax.broadcasted_iota(jnp.int32, both.shape, 0) // lines
        hidden.append(jnp.where(lower == 0, both, back))
    group = lax.broadcasted_iota(jnp.int32, (2 * lines, lanes), 1) // size
    for k in range(0, eighths, 2):
        for half in range(2):
            block = jnp.zeros((2 * lines, lanes), F32)
            for m in range(eighths):
                moved = pltpu.roll(hidden[eighths * half + m], (size * (m - k)) % lanes, 1)
                block = jnp.where(group == m, moved, block)
            rows_ref[lines * k : lines * (k + 2), lanes * half : lanes * (half + 1)] = block
    rows = rows_ref[...].astype(BF16)
    own = hidden_ref.shape[0]
    slab = rows.shape[0]
    all_ref[pl.ds(pl.multiple_of(depth * slab, slab), slab)] = rows
    slots = jnp.dot(along_ref[...], all_ref[...], preferred_element_type=F32).astype(BF16)
    span = out_ref.shape[1]
    for at in range(out_ref.shape[0]):
        out_ref[at] = slots[span * at : span * (at + 1)]
    here = lax.broadcasted_iota(jnp.int32, (8, slab), 0)
    there = lax.broadcasted_iota(jnp.int32, (8, slab), 1)
    pick = jnp.where(there == here + own * row, 1.0, 0.0).astype(BF16)
    hidden_ref[...] = jnp.dot(pick, rows, preferred_element_type=F32)[:own].astype(BF16)


def on_device(
    residual_in,
    gla_state,
    norm_gain,
    w_query,
    w_key,
    w_value,
    w_decay,
    decay_bias,
    head_gain,
    w_output,
    ffn_gain,
    router_group,
    router_expert,
    expert_ids,
    w_gate,
    w_up,
    w_down,
):
    depths, rows, cores = (lax.axis_size(a) for a in EP)
    heads = lax.axis_size("tp")
    slab = rows * cores
    parts = cores * heads
    far = depths * rows
    tokens = expert_ids.shape[0]
    seqs, width = residual_in.shape
    strip = w_query.shape[0]
    key_width, value_width = w_query.shape[1], w_value.shape[1]
    in_width = 3 * key_width + value_width
    held = depths * strip
    piece = width // parts

    n_experts = router_expert.shape[0]

    def experts_of():
        core = lax.axis_index("ep_2")
        return lax.axis_index(FAR) * cores, core, lax.axis_index(SLAB), slab

    vmem = pl.BlockSpec(memory_space=pltpu.VMEM)
    later = (residual_in, norm_gain, head_gain, ffn_gain, decay_bias, router_group.T)
    shapes = [
        jax.ShapeDtypeStruct((depths, strip, in_width + value_width), BF16),
        pltpu.VMEM((width, held), BF16),
        pltpu.VMEM((depths * cores * CAP, tokens), BF16),
        pltpu.VMEM((cores * CAP, tokens), BF16),
        pltpu.VMEM((CAP, n_experts), F32),
        *(pltpu.VMEM(a.shape, a.dtype) for a in later),
    ]
    spread, pick, along, select, rival_lane, *later = pl.pallas_call(
        functools.partial(prepare, experts_of, strip),
        out_shape=shapes,
        in_specs=[pl.BlockSpec(memory_space=pl.ANY)] * 12,
        out_specs=[pl.BlockSpec(memory_space=pl.ANY)] + [vmem] * (len(shapes) - 1),
        scratch_shapes=[
            pltpu.VMEM((strip, in_width + value_width), BF16),
            pltpu.VMEM((expert_ids.shape[1], tokens), jnp.int32),
            pltpu.SemaphoreType.DMA((12 + depths,)),
        ],
    )(w_query, w_key, w_value, w_decay, w_output.T, expert_ids.T, *later)
    residual_in, norm_gain, head_gain, ffn_gain, decay_bias, group_rows = later
    head_gain = head_gain.astype(F32)[None]
    ffn_gain = ffn_gain.astype(F32)[None]
    decay_bias = decay_bias[None]
    norm_gain = norm_gain.astype(F32)[None]

    tied = lax.optimization_barrier(
        (spread, residual_in, pick, along, select, rival_lane, norm_gain)
        + (head_gain, ffn_gain, decay_bias)
    )
    spread, residual_in, pick, along, select, rival_lane, norm_gain, *tied = tied
    head_gain, ffn_gain, decay_bias = tied
    gathered = exchange(spread, "ep_0")
    rows_in = lax.all_gather(residual_in, SLAB, axis=0, tiled=True)
    lhs, slab_res = kernel_call(
        strips_of,
        out_shape=[pltpu.VMEM((slab * seqs, held), BF16)] * 2,
        in_specs=[vmem] * 3,
        out_specs=[vmem] * 2,
    )(on_chip(rows_in), on_chip(norm_gain), on_chip(pick))
    gathered, lhs, slab_res = lax.optimization_barrier((gathered, lhs, slab_res))
    gathered = gathered.reshape(held, in_width + value_width)
    sums = jnp.dot(lhs, gathered[:, :in_width], preferred_element_type=F32).astype(BF16)
    arrived = exchange(sums.reshape(slab, seqs, in_width), SLAB)
    gated, new_state = kernel_call(
        advance,
        out_shape=[
            pltpu.VMEM((slab, seqs, value_width), BF16),
            pltpu.VMEM((seqs, key_width, value_width), F32),
        ],
        in_specs=[vmem] * 5,
        out_specs=[vmem] * 2,
    )(*map(on_chip, (arrived.reshape(slab * seqs, in_width), residual_in, decay_bias, head_gain, gla_state[:, 0])))

    slab_heads, slab_res = exchange(gated, SLAB, slab_res)
    slab_heads = slab_heads.reshape(slab * seqs, value_width)
    lines = slab * seqs // parts
    state = pltpu.VMEM(new_state.shape, F32)
    came, new_state = kernel_call(
        pack,
        out_shape=[pltpu.VMEM((slab * heads, lines, held), BF16), state],
        in_specs=[vmem] * 4,
        out_specs=[vmem] * 2,
        input_output_aliases={3: 1},
    )(*map(on_chip, (slab_heads, gathered, slab_res, new_state)))
    came = exchange(came, SLAB_TP)

    def at_place():
        return lax.axis_index("ep_0"), lax.axis_index("ep_1")

    outward, hidden, new_state = kernel_call(
        functools.partial(dispatch, at_place),
        out_shape=[
            pltpu.VMEM((depths, cores * CAP, piece), BF16),
            pltpu.VMEM((cores * seqs, piece), BF16),
            state,
        ],
        in_specs=[vmem] * 3,
        out_specs=[vmem] * 3,
        scratch_shapes=[
            pltpu.VMEM((slab * seqs, piece), F32),
            pltpu.VMEM((tokens, piece), BF16),
        ],
        input_output_aliases={2: 2},
    )(on_chip(came), on_chip(along), on_chip(new_state))
    slot_part = exchange(outward, "ep_0").astype(F32).sum(axis=0).astype(BF16)
    slot_part = to_all(slot_part.reshape(cores, CAP, piece), heads)
    came = exchange(slot_part.reshape(parts, CAP, piece), CHIPS)
    operands = (came, ffn_gain, group_rows, rival_lane)
    operands += (w_gate[0], w_up[0], w_down[0], new_state)
    back, new_state = kernel_call(
        functools.partial(mix, lambda: lax.axis_index(EP)),
        out_shape=[
            pltpu.VMEM((parts, CAP, piece), BF16),
            jax.ShapeDtypeStruct(new_state.shape, F32),
        ],
        in_specs=[pl.BlockSpec(memory_space=pl.ANY)] + [vmem] * len(operands),
        out_specs=[vmem, pl.BlockSpec(memory_space=pl.ANY)],
        scratch_shapes=[
            pltpu.VMEM((CAP, width), F32),
            pltpu.VMEM(router_expert.shape, BF16),
            pltpu.SemaphoreType.DMA((1 + seqs * key_width // 64,)),
        ],
    )(router_expert, *map(on_chip, operands))
    summed = exchange(back, CHIPS).reshape(heads, cores, CAP, piece).astype(F32).sum(axis=0)
    dense = lax.dot_general(
        select,
        summed.astype(BF16).reshape(cores * CAP, piece),
        (((0,), (0,)), ((), ())),
        preferred_element_type=F32,
    ).astype(BF16)
    moe, hidden = exchange(dense.reshape(far, cores * seqs, piece), FAR, hidden)
    moe = moe.astype(F32).sum(axis=0)
    layer = (hidden.astype(F32) + moe).astype(BF16)
    last = to_all(layer.reshape(cores, seqs, piece), heads).reshape(parts, seqs, piece)
    layer_out = exchange(last, CHIPS).transpose(1, 0, 2).reshape(seqs, width)
    return (layer_out, new_state[:, None])


def solution(mesh):
    torus = Mesh(mesh.devices.reshape(8, 8, 2, mesh.shape["tp"]), (*EP, "tp"))
    in_specs = (
        P(EP, None),
        P(EP, "tp", None, None),
        P(),
        P(EP, "tp"),
        P(EP, "tp"),
        P(EP, "tp"),
        P(EP, "tp"),
        P("tp"),
        P(),
        P("tp", EP),
        P(),
        P(),
        P(),
        P(),
        P(EP, None, "tp"),
        P(EP, None, "tp"),
        P(EP, "tp", None),
    )
    out_specs = (P(EP, None), P(EP, "tp", None, None))
    return jax.shard_map(
        on_device, mesh=torus, in_specs=in_specs, out_specs=out_specs, check_vma=False
    )
```

```python
import functools

import jax
import jax.numpy as jnp
from jax import lax
from jax.experimental import pallas as pl
from jax.experimental.pallas import tpu as pltpu
from jax.sharding import Mesh
from jax.sharding import PartitionSpec as P


CAP = 16
EP = ("ep_0", "ep_1", "ep_2")
FAR = ("ep_0", "ep_1")
SLAB = ("ep_1", "ep_2")
SLAB_TP = ("ep_1", "ep_2", "tp")
CHIPS = ("tp", "ep_2")

EPSILON = 1e-06
GATE_SCALE = 16.0
F32 = jnp.float32
BF16 = jnp.bfloat16


def exchange(blocks, axes, *later):
    came = lax.all_to_all(blocks, axes, split_axis=0, concat_axis=0, tiled=True)
    return lax.optimization_barrier((came, *later)) if later else came


def on_chip(array):
    return pltpu.with_memory_space_constraint(array, pltpu.VMEM)


def kernel_call(body, **settings):
    params = pltpu.CompilerParams(vmem_limit_bytes=6 * 2**20)
    return pl.pallas_call(body, compiler_params=params, **settings)


def to_all(shard, count):
    return jnp.broadcast_to(shard[None], (count, *shard.shape))


def prepare(experts_of, strip, *refs):
    sources, (spread, pick, along, select, rival, *kept) = refs[:12], refs[12:-3]
    own_w, ids, sems = refs[-3:]
    *weights, ids_in = sources[:6]
    width = 0
    copies = []
    for source in weights:
        place = own_w.at[:, pl.ds(width, source.shape[1])]
        copies.append(pltpu.make_async_copy(source, place, sems.at[len(copies)]))
        width += source.shape[1]
    fetched = len(copies)
    copies.append(pltpu.make_async_copy(ids_in, ids, sems.at[len(copies)]))
    for source, target in zip(sources[6:], kept, strict=True):
        copies.append(pltpu.make_async_copy(source, target, sems.at[len(copies)]))
    for copy in copies:
        copy.start()
    first, core, place, slab = experts_of()
    count = ids.shape[1]
    row = lax.broadcasted_iota(jnp.int32, (count, count), 0)
    col = lax.broadcasted_iota(jnp.int32, (count, count), 1)
    upper = jnp.where(row <= col, 1.0, 0.0).astype(BF16)
    feature = lax.broadcasted_iota(jnp.int32, (pick.shape[0] // spread.shape[0], 128), 0)
    lane = lax.broadcasted_iota(jnp.int32, feature.shape, 1)
    within = feature - place * strip == lane % strip
    for depth in range(spread.shape[0]):
        taken = within & (lane // strip == depth)
        at = feature.shape[0] * depth
        pick[at : at + feature.shape[0]] = jnp.where(taken, 1.0, 0.0).astype(BF16)
    for copy in copies[:fetched]:
        copy.wait()
    spreads = []
    for depth in range(spread.shape[0]):
        sem = sems.at[len(copies) + depth]
        spreads.append(pltpu.make_async_copy(own_w, spread.at[depth], sem))
        spreads[-1].start()
    copies[fetched].wait()
    one, two = ids[0:1, :], ids[1:2, :]
    spans = along.shape[0] // CAP
    cores = select.shape[0] // CAP
    index = lax.broadcasted_iota(jnp.int32, (spans + 8, count), 0)
    experts = index // cores * slab + place - core + index % cores
    experts = jnp.where(index < spans, experts, index - spans + first)
    named = (one == experts) | (two == experts)
    marks = jnp.where(named, 1.0, 0.0)
    ends = jnp.dot(marks.astype(BF16), upper, preferred_element_type=F32)
    slots = lax.broadcasted_iota(jnp.int32, (CAP, count), 0).astype(F32) + 1.0
    both = (one + two).astype(F32)
    own = first + core
    others = jnp.zeros((CAP, 1), F32)


    def slots_of(at):
        return jnp.where(ends[at : at + 1] == slots, marks[at : at + 1], 0.0)

    for span in range(spans):
        along[CAP * span : CAP * (span + 1)] = slots_of(span).astype(BF16)
    for c in range(cores):
        mine = slots_of(spans + c)
        select[CAP * c : CAP * (c + 1)] = mine.astype(BF16)
        total = jnp.sum(mine * both, axis=1, keepdims=True)
        others = jnp.where(core == c, total, others)
    lanes = lax.broadcasted_iota(jnp.int32, rival.shape, 1)
    rival[...] = jnp.where(lanes == others.astype(jnp.int32) - own, 1.0, 0.0)
    for copy in copies[fetched + 1 :] + spreads:
        copy.wait()


def strips_of(rows_ref, gain_ref, pick_ref, lhs_ref, res_ref):
    rows = rows_ref[...]
    pick = pick_ref[...]
    scaled = (rows.astype(F32) * gain_ref[...]).astype(BF16)
    res_ref[...] = jnp.dot(rows, pick, preferred_element_type=F32).astype(BF16)
    lhs_ref[...] = jnp.dot(scaled, pick, preferred_element_type=F32).astype(BF16)


def advance(came_ref, res_ref, bias_ref, gain_ref, old_ref, out_ref, held_ref):
    seqs, key_width, value_width = old_ref.shape
    count = came_ref.shape[0]
    seq_of = lax.broadcasted_iota(jnp.int32, (8, count), 1) % seqs
    pick = jnp.where(seq_of == lax.broadcasted_iota(jnp.int32, (8, count), 0), 1.0, 0.0)
    total = jnp.dot(pick.astype(BF16), came_ref[...], preferred_element_type=F32)[:seqs]
    res = res_ref[...].astype(F32)
    total = total * lax.rsqrt(jnp.mean(res * res, axis=1, keepdims=True) + EPSILON)
    query = total[:, :key_width].astype(BF16).astype(F32) * key_width ** (-0.5)
    key = total[:, key_width : 2 * key_width].astype(BF16).astype(F32)
    value = total[:, 2 * key_width : 2 * key_width + value_width].astype(BF16).astype(F32)
    pre = total[:, 2 * key_width + value_width :] + bias_ref[...]
    log_decay = (jnp.minimum(pre, 0.0) - jnp.log1p(jnp.exp(-jnp.abs(pre)))) / GATE_SCALE
    down = jnp.concatenate([query, key, jnp.exp(log_decay), jnp.zeros_like(query)], axis=0).T
    gated = []
    for seq in range(seqs):
        for at in range(0, key_width, 64):
            rows = slice(at, at + 64)
            key_col = down[rows, seqs + seq : seqs + seq + 1]
            alpha_col = down[rows, 2 * seqs + seq : 2 * seqs + seq + 1]
            new = alpha_col * old_ref[seq, rows] + key_col * value[seq : seq + 1]
            held_ref[seq, rows] = new
    for seq in range(seqs):
        read = jnp.zeros((8, value_width), F32)
        for at in range(0, key_width, 64):
            rows = slice(at, at + 64)
            part = down[rows, seq : seq + 1] * held_ref[seq, rows]
            read = read + jnp.sum(part.reshape(8, 8, value_width), axis=0)
        read = jnp.sum(read, axis=0, keepdims=True)
        mean = jnp.mean(read * read, axis=1, keepdims=True)
        gated.append(read * lax.rsqrt(mean + EPSILON) * gain_ref[...])
    gated = jnp.concatenate(gated, axis=0).astype(BF16)
    for at in range(out_ref.shape[0]):
        out_ref[at] = gated


def mix(
    which,
    router_ref,
    came_ref,
    gain_ref,
    group_ref,
    rival_ref,
    gate_ref,
    up_ref,
    down_ref,
    state_ref,
    out_ref,
    new_ref,
    rows_ref,
    sems,
):
    copies = []
    for seq in range(state_ref.shape[0]):
        for at in range(0, state_ref.shape[1], 64):
            source, target = state_ref.at[seq, pl.ds(at, 64)], new_ref.at[seq, pl.ds(at, 64)]
            copies.append(pltpu.make_async_copy(source, target, sems.at[len(copies)]))
            copies[-1].start()
    expert = which()
    size = came_ref.shape[2]
    for at in range(came_ref.shape[0]):
        rows_ref[:, size * at : size * (at + 1)] = came_ref[at].astype(F32)
    rows = rows_ref[...]
    mean = jnp.mean(rows * rows, axis=1, keepdims=True)
    rows = (rows * lax.rsqrt(mean + EPSILON) * gain_ref[...]).astype(BF16)
    gate = jnp.dot(rows, gate_ref[...], preferred_element_type=F32)
    up = jnp.dot(rows, up_ref[...], preferred_element_type=F32)
    floats = rows.astype(F32)
    count = group_ref.shape[0]
    group_rows = group_ref[...].astype(F32)
    groups = [
        jnp.sum(floats * group_rows[at : at + 1], axis=1, keepdims=True) for at in range(count)
    ]
    units = (gate * jax.nn.sigmoid(gate) * up).astype(BF16)
    output = jnp.dot(units, down_ref[...], preferred_element_type=F32)
    experts = router_ref.shape[0]
    own = expert // (experts // count)
    group_logit = groups[0]
    for at in range(1, count):
        group_logit = jnp.where(own == at, groups[at], group_logit)
    total = jnp.zeros_like(group_logit)
    for logit in groups:
        total = total + jnp.exp(logit - group_logit)
    share = 1.0 / total
    lanes = lax.broadcasted_iota(jnp.int32, rival_ref.shape, 1)
    apart = jnp.where(lanes == expert, 1.0, 0.0) - rival_ref[...]
    apart = jnp.dot(apart.astype(BF16), router_ref[...], preferred_element_type=F32)
    lead = jnp.sum(floats * apart, axis=1, keepdims=True)
    output = (output * (share * jax.nn.sigmoid(lead))).astype(BF16)
    piece = out_ref.shape[2]
    for at in range(out_ref.shape[0]):
        out_ref[at] = output[:, piece * at : piece * (at + 1)]
    for copy in copies:
        copy.wait()


def pack(heads_ref, held_ref, res_ref, _, out_ref, __):
    value_width = heads_ref.shape[1]
    part = lax.dot_general(
        heads_ref[...],
        held_ref[:, held_ref.shape[1] - value_width :],
        (((1,), (1,)), ((), ())),
        preferred_element_type=F32,
    )
    with_res = (lax.axis_index("tp") == 0).astype(F32)
    part = part + res_ref[...].astype(F32) * with_res
    lines, lanes = out_ref.shape[1:]
    eighths = part.shape[0] // lines
    size = lanes // eighths
    group = lax.broadcasted_iota(jnp.int32, (2 * lines, lanes), 1) // size
    lower = lax.broadcasted_iota(jnp.int32, (2 * lines, lanes), 0) // lines
    for eighth in range(eighths):
        block = jnp.zeros((2 * lines, lanes), F32)
        for k in range(0, eighths, 2):
            rows = part[lines * k : lines * (k + 2)]
            for low in range(2):
                moved = pltpu.roll(rows, (size * (k + low - eighth)) % lanes, 1)
                block = jnp.where((group == k + low) & (lower == low), moved, block)
        block = (block[:lines] + block[lines:]).astype(BF16)
        quarter, core = eighth // 2, eighth % 2
        for row in range(out_ref.shape[0] // eighths):
            out_ref[eighths * row + eighths // 2 * core + quarter] = block


def dispatch(at_place, came_ref, along_ref, _, out_ref, hidden_ref, __, rows_ref, all_ref):
    depth, row = at_place()
    count, lines, lanes = came_ref.shape
    eighths = rows_ref.shape[0] // lines
    size = lanes // eighths
    heads = eighths // 2
    all_ref[...] = jnp.zeros_like(all_ref)
    hidden = []
    for at in range(count // heads):
        total = came_ref[heads * at].astype(F32)
        for head in range(1, heads):
            total = total + came_ref[heads * at + head].astype(F32)
        total = total.astype(BF16).astype(F32)
        both = jnp.concatenate([total, total], axis=0)
        back = pltpu.roll(both, lanes - size, 1)
        lower = lax.broadcasted_iota(jnp.int32, both.shape, 0) // lines
        hidden.append(jnp.where(lower == 0, both, back))
    group = lax.broadcasted_iota(jnp.int32, (2 * lines, lanes), 1) // size
    for k in range(0, eighths, 2):
        for half in range(2):
            block = jnp.zeros((2 * lines, lanes), F32)
            for m in range(eighths):
                moved = pltpu.roll(hidden[eighths * half + m], (size * (m - k)) % lanes, 1)
                block = jnp.where(group == m, moved, block)
            rows_ref[lines * k : lines * (k + 2), lanes * half : lanes * (half + 1)] = block
    rows = rows_ref[...].astype(BF16)
    own = hidden_ref.shape[0]
    slab = rows.shape[0]
    all_ref[pl.ds(pl.multiple_of(depth * slab, slab), slab)] = rows
    slots = jnp.dot(along_ref[...], all_ref[...], preferred_element_type=F32).astype(BF16)
    span = out_ref.shape[1]
    for at in range(out_ref.shape[0]):
        out_ref[at] = slots[span * at : span * (at + 1)]
    here = lax.broadcasted_iota(jnp.int32, (8, slab), 0)
    there = lax.broadcasted_iota(jnp.int32, (8, slab), 1)
    pick = jnp.where(there == here + own * row, 1.0, 0.0).astype(BF16)
    hidden_ref[...] = jnp.dot(pick, rows, preferred_element_type=F32)[:own].astype(BF16)


def on_device(
    residual_in,
    gla_state,
    norm_gain,
    w_query,
    w_key,
    w_value,
    w_decay,
    decay_bias,
    head_gain,
    w_output,
    ffn_gain,
    router_group,
    router_expert,
    expert_ids,
    w_gate,
    w_up,
    w_down,
):
    depths, rows, cores = (lax.axis_size(a) for a in EP)
    heads = lax.axis_size("tp")
    slab = rows * cores
    parts = cores * heads
    far = depths * rows
    tokens = expert_ids.shape[0]
    seqs, width = residual_in.shape
    strip = w_query.shape[0]
    key_width, value_width = w_query.shape[1], w_value.shape[1]
    in_width = 3 * key_width + value_width
    held = depths * strip
    piece = width // parts

    n_experts = router_expert.shape[0]

    def experts_of():
        core = lax.axis_index("ep_2")
        return lax.axis_index(FAR) * cores, core, lax.axis_index(SLAB), slab

    vmem = pl.BlockSpec(memory_space=pltpu.VMEM)
    later = (residual_in, norm_gain, head_gain, ffn_gain, decay_bias, router_group.T)
    shapes = [
        jax.ShapeDtypeStruct((depths, strip, in_width + value_width), BF16),
        pltpu.VMEM((width, held), BF16),
        pltpu.VMEM((depths * cores * CAP, tokens), BF16),
        pltpu.VMEM((cores * CAP, tokens), BF16),
        pltpu.VMEM((CAP, n_experts), F32),
        *(pltpu.VMEM(a.shape, a.dtype) for a in later),
    ]
    spread, pick, along, select, rival_lane, *later = pl.pallas_call(
        functools.partial(prepare, experts_of, strip),
        out_shape=shapes,
        in_specs=[pl.BlockSpec(memory_space=pl.ANY)] * 12,
        out_specs=[pl.BlockSpec(memory_space=pl.ANY)] + [vmem] * (len(shapes) - 1),
        scratch_shapes=[
            pltpu.VMEM((strip, in_width + value_width), BF16),
            pltpu.VMEM((expert_ids.shape[1], tokens), jnp.int32),
            pltpu.SemaphoreType.DMA((12 + depths,)),
        ],
    )(w_query, w_key, w_value, w_decay, w_output.T, expert_ids.T, *later)
    residual_in, norm_gain, head_gain, ffn_gain, decay_bias, group_rows = later
    head_gain = head_gain.astype(F32)[None]
    ffn_gain = ffn_gain.astype(F32)[None]
    decay_bias = decay_bias[None]
    norm_gain = norm_gain.astype(F32)[None]

    tied = lax.optimization_barrier(
        (spread, residual_in, pick, along, select, rival_lane, norm_gain)
        + (head_gain, ffn_gain, decay_bias)
    )
    spread, residual_in, pick, along, select, rival_lane, norm_gain, *tied = tied
    head_gain, ffn_gain, decay_bias = tied
    gathered = exchange(spread, "ep_0")
    rows_in = lax.all_gather(residual_in, SLAB, axis=0, tiled=True)
    lhs, slab_res = kernel_call(
        strips_of,
        out_shape=[pltpu.VMEM((slab * seqs, held), BF16)] * 2,
        in_specs=[vmem] * 3,
        out_specs=[vmem] * 2,
    )(on_chip(rows_in), on_chip(norm_gain), on_chip(pick))
    gathered, lhs, slab_res = lax.optimization_barrier((gathered, lhs, slab_res))
    gathered = gathered.reshape(held, in_width + value_width)
    sums = jnp.dot(lhs, gathered[:, :in_width], preferred_element_type=F32).astype(BF16)
    arrived = exchange(sums.reshape(slab, seqs, in_width), SLAB)
    gated, new_state = kernel_call(
        advance,
        out_shape=[
            pltpu.VMEM((slab, seqs, value_width), BF16),
            pltpu.VMEM((seqs, key_width, value_width), F32),
        ],
        in_specs=[vmem] * 5,
        out_specs=[vmem] * 2,
    )(*map(on_chip, (arrived.reshape(slab * seqs, in_width), residual_in, decay_bias, head_gain, gla_state[:, 0])))

    slab_heads, slab_res = exchange(gated, SLAB, slab_res)
    slab_heads = slab_heads.reshape(slab * seqs, value_width)
    lines = slab * seqs // parts
    state = pltpu.VMEM(new_state.shape, F32)
    came, new_state = kernel_call(
        pack,
        out_shape=[pltpu.VMEM((slab * heads, lines, held), BF16), state],
        in_specs=[vmem] * 4,
        out_specs=[vmem] * 2,
        input_output_aliases={3: 1},
    )(*map(on_chip, (slab_heads, gathered, slab_res, new_state)))
    came = exchange(came, SLAB_TP)

    def at_place():
        return lax.axis_index("ep_0"), lax.axis_index("ep_1")

    outward, hidden, new_state = kernel_call(
        functools.partial(dispatch, at_place),
        out_shape=[
            pltpu.VMEM((depths, cores * CAP, piece), BF16),
            pltpu.VMEM((cores * seqs, piece), BF16),
            state,
        ],
        in_specs=[vmem] * 3,
        out_specs=[vmem] * 3,
        scratch_shapes=[
            pltpu.VMEM((slab * seqs, piece), F32),
            pltpu.VMEM((tokens, piece), BF16),
        ],
        input_output_aliases={2: 2},
    )(on_chip(came), on_chip(along), on_chip(new_state))
    slot_part = exchange(outward, "ep_0").astype(F32).sum(axis=0).astype(BF16)
    slot_part = to_all(slot_part.reshape(cores, CAP, piece), heads)
    came = exchange(slot_part.reshape(parts, CAP, piece), CHIPS)
    operands = (router_expert, came, ffn_gain, group_rows, rival_lane)
    operands += (w_gate[0], w_up[0], w_down[0], new_state)
    back, new_state = kernel_call(
        functools.partial(mix, lambda: lax.axis_index(EP)),
        out_shape=[
            pltpu.VMEM((parts, CAP, piece), BF16),
            jax.ShapeDtypeStruct(new_state.shape, F32),
        ],
        in_specs=[vmem] * len(operands),
        out_specs=[vmem, pl.BlockSpec(memory_space=pl.ANY)],
        scratch_shapes=[
            pltpu.VMEM((CAP, width), F32),
            pltpu.SemaphoreType.DMA((seqs * key_width // 64,)),
        ],
    )(*map(on_chip, operands))
    summed = exchange(back, CHIPS).reshape(heads, cores, CAP, piece).astype(F32).sum(axis=0)
    dense = lax.dot_general(
        select,
        summed.astype(BF16).reshape(cores * CAP, piece),
        (((0,), (0,)), ((), ())),
        preferred_element_type=F32,
    ).astype(BF16)
    moe, hidden = exchange(dense.reshape(far, cores * seqs, piece), FAR, hidden)
    moe = moe.astype(F32).sum(axis=0)
    layer = (hidden.astype(F32) + moe).astype(BF16)
    last = to_all(layer.reshape(cores, seqs, piece), heads).reshape(parts, seqs, piece)
    layer_out = exchange(last, CHIPS).transpose(1, 0, 2).reshape(seqs, width)
    return (layer_out, new_state[:, None])


def solution(mesh):
    torus = Mesh(mesh.devices.reshape(8, 8, 2, mesh.shape["tp"]), (*EP, "tp"))
    in_specs = (
        P(EP, None),
        P(EP, "tp", None, None),
        P(),
        P(EP, "tp"),
        P(EP, "tp"),
        P(EP, "tp"),
        P(EP, "tp"),
        P("tp"),
        P(),
        P("tp", EP),
        P(),
        P(),
        P(),
        P(),
        P(EP, None, "tp"),
        P(EP, None, "tp"),
        P(EP, "tp", None),
    )
    out_specs = (P(EP, None), P(EP, "tp", None, None))
    return jax.shard_map(
        on_device, mesh=torus, in_specs=in_specs, out_specs=out_specs, check_vma=False
    )
```

```python
import functools

import jax
import jax.numpy as jnp
from jax import lax
from jax.experimental import pallas as pl
from jax.experimental.pallas import tpu as pltpu
from jax.sharding import Mesh
from jax.sharding import PartitionSpec as P


CAP = 16
EP = ("ep_0", "ep_1", "ep_2")
FAR = ("ep_0", "ep_1")
SLAB = ("ep_1", "ep_2")
SLAB_TP = ("ep_1", "ep_2", "tp")
CHIPS = ("tp", "ep_2")

EPSILON = 1e-06
GATE_SCALE = 16.0
F32 = jnp.float32
BF16 = jnp.bfloat16


def exchange(blocks, axes, *later):
    came = lax.all_to_all(blocks, axes, split_axis=0, concat_axis=0, tiled=True)
    return lax.optimization_barrier((came, *later)) if later else came


def on_chip(array):
    return pltpu.with_memory_space_constraint(array, pltpu.VMEM)


def kernel_call(body, **settings):
    params = pltpu.CompilerParams(vmem_limit_bytes=6 * 2**20)
    return pl.pallas_call(body, compiler_params=params, **settings)


def to_all(shard, count):
    return jnp.broadcast_to(shard[None], (count, *shard.shape))


def prepare(experts_of, strip, *refs):
    sources, (spread, pick, along, select, rival, *kept) = refs[:12], refs[12:-3]
    own_w, ids, sems = refs[-3:]
    *weights, ids_in = sources[:6]
    width = 0
    copies = []
    for source in weights:
        place = own_w.at[:, pl.ds(width, source.shape[1])]
        copies.append(pltpu.make_async_copy(source, place, sems.at[len(copies)]))
        width += source.shape[1]
    fetched = len(copies)
    copies.append(pltpu.make_async_copy(ids_in, ids, sems.at[len(copies)]))
    for source, target in zip(sources[6:], kept, strict=True):
        copies.append(pltpu.make_async_copy(source, target, sems.at[len(copies)]))
    for copy in copies:
        copy.start()
    first, core, place, slab = experts_of()
    count = ids.shape[1]
    row = lax.broadcasted_iota(jnp.int32, (count, count), 0)
    col = lax.broadcasted_iota(jnp.int32, (count, count), 1)
    upper = jnp.where(row <= col, 1.0, 0.0).astype(BF16)
    feature = lax.broadcasted_iota(jnp.int32, (pick.shape[0] // spread.shape[0], 128), 0)
    lane = lax.broadcasted_iota(jnp.int32, feature.shape, 1)
    within = feature - place * strip == lane % strip
    for depth in range(spread.shape[0]):
        taken = within & (lane // strip == depth)
        at = feature.shape[0] * depth
        pick[at : at + feature.shape[0]] = jnp.where(taken, 1.0, 0.0).astype(BF16)
    for copy in copies[:fetched]:
        copy.wait()
    spreads = []
    for depth in range(spread.shape[0]):
        sem = sems.at[len(copies) + depth]
        spreads.append(pltpu.make_async_copy(own_w, spread.at[depth], sem))
        spreads[-1].start()
    copies[fetched].wait()
    one, two = ids[0:1, :], ids[1:2, :]
    spans = along.shape[0] // CAP
    cores = select.shape[0] // CAP
    index = lax.broadcasted_iota(jnp.int32, (spans + 8, count), 0)
    experts = index // cores * slab + place - core + index % cores
    experts = jnp.where(index < spans, experts, index - spans + first)
    named = (one == experts) | (two == experts)
    marks = jnp.where(named, 1.0, 0.0)
    ends = jnp.dot(marks.astype(BF16), upper, preferred_element_type=F32)
    slots = lax.broadcasted_iota(jnp.int32, (CAP, count), 0).astype(F32) + 1.0
    both = (one + two).astype(F32)
    own = first + core
    others = jnp.zeros((CAP, 1), F32)


    def slots_of(at):
        return jnp.where(ends[at : at + 1] == slots, marks[at : at + 1], 0.0)

    for span in range(spans):
        along[CAP * span : CAP * (span + 1)] = slots_of(span).astype(BF16)
    for c in range(cores):
        mine = slots_of(spans + c)
        select[CAP * c : CAP * (c + 1)] = mine.astype(BF16)
        total = jnp.sum(mine * both, axis=1, keepdims=True)
        others = jnp.where(core == c, total, others)
    lanes = lax.broadcasted_iota(jnp.int32, rival.shape, 1)
    rival[...] = jnp.where(lanes == others.astype(jnp.int32) - own, 1.0, 0.0)
    for copy in copies[fetched + 1 :] + spreads:
        copy.wait()


def strips_of(rows_ref, gain_ref, pick_ref, lhs_ref, res_ref):
    rows = rows_ref[...]
    pick = pick_ref[...]
    scaled = (rows.astype(F32) * gain_ref[...]).astype(BF16)
    res_ref[...] = jnp.dot(rows, pick, preferred_element_type=F32).astype(BF16)
    lhs_ref[...] = jnp.dot(scaled, pick, preferred_element_type=F32).astype(BF16)


def advance(came_ref, res_ref, bias_ref, gain_ref, old_ref, out_ref, held_ref):
    seqs, key_width, value_width = old_ref.shape
    count = came_ref.shape[0]
    seq_of = lax.broadcasted_iota(jnp.int32, (8, count), 1) % seqs
    pick = jnp.where(seq_of == lax.broadcasted_iota(jnp.int32, (8, count), 0), 1.0, 0.0)
    total = jnp.dot(pick.astype(BF16), came_ref[...], preferred_element_type=F32)[:seqs]
    res = res_ref[...].astype(F32)
    total = total * lax.rsqrt(jnp.mean(res * res, axis=1, keepdims=True) + EPSILON)
    query = total[:, :key_width].astype(BF16).astype(F32) * key_width ** (-0.5)
    key = total[:, key_width : 2 * key_width].astype(BF16).astype(F32)
    value = total[:, 2 * key_width : 2 * key_width + value_width].astype(BF16).astype(F32)
    pre = total[:, 2 * key_width + value_width :] + bias_ref[...]
    log_decay = (jnp.minimum(pre, 0.0) - jnp.log1p(jnp.exp(-jnp.abs(pre)))) / GATE_SCALE
    down = jnp.concatenate([query, key, jnp.exp(log_decay), jnp.zeros_like(query)], axis=0).T
    gated = []
    for seq in range(seqs):
        for at in range(0, key_width, 64):
            rows = slice(at, at + 64)
            key_col = down[rows, seqs + seq : seqs + seq + 1]
            alpha_col = down[rows, 2 * seqs + seq : 2 * seqs + seq + 1]
            new = alpha_col * old_ref[seq, rows] + key_col * value[seq : seq + 1]
            held_ref[seq, rows] = new
    for seq in range(seqs):
        read = jnp.zeros((8, value_width), F32)
        for at in range(0, key_width, 64):
            rows = slice(at, at + 64)
            part = down[rows, seq : seq + 1] * held_ref[seq, rows]
            read = read + jnp.sum(part.reshape(8, 8, value_width), axis=0)
        read = jnp.sum(read, axis=0, keepdims=True)
        mean = jnp.mean(read * read, axis=1, keepdims=True)
        gated.append(read * lax.rsqrt(mean + EPSILON) * gain_ref[...])
    gated = jnp.concatenate(gated, axis=0).astype(BF16)
    for at in range(out_ref.shape[0]):
        out_ref[at] = gated


def mix(
    which,
    router_ref,
    came_ref,
    gain_ref,
    group_ref,
    rival_ref,
    gate_ref,
    up_ref,
    down_ref,
    state_ref,
    out_ref,
    new_ref,
    rows_ref,
    sem,
):
    copy = pltpu.make_async_copy(state_ref, new_ref, sem)
    copy.start()
    expert = which()
    size = came_ref.shape[2]
    for at in range(came_ref.shape[0]):
        rows_ref[:, size * at : size * (at + 1)] = came_ref[at].astype(F32)
    rows = rows_ref[...]
    mean = jnp.mean(rows * rows, axis=1, keepdims=True)
    rows = (rows * lax.rsqrt(mean + EPSILON) * gain_ref[...]).astype(BF16)
    gate = jnp.dot(rows, gate_ref[...], preferred_element_type=F32)
    up = jnp.dot(rows, up_ref[...], preferred_element_type=F32)
    over = (((1,), (1,)), ((), ()))
    groups = lax.dot_general(rows, group_ref[...], over, preferred_element_type=F32)
    units = (gate * jax.nn.sigmoid(gate) * up).astype(BF16)
    output = jnp.dot(units, down_ref[...], preferred_element_type=F32)
    logits = lax.dot_general(rows, router_ref[...], over, preferred_element_type=F32)
    of_group = lax.broadcasted_iota(jnp.int32, groups.shape, 1)
    own = of_group == expert // (logits.shape[1] // groups.shape[1])
    group_logit = jnp.sum(jnp.where(own, groups, 0.0), axis=1, keepdims=True)
    share = 1.0 / jnp.sum(jnp.exp(groups - group_logit), axis=1, keepdims=True)
    lanes = lax.broadcasted_iota(jnp.int32, logits.shape, 1)
    chosen = jnp.sum(jnp.where(lanes == expert, logits, 0.0), axis=1, keepdims=True)
    rival = jnp.sum(logits * rival_ref[...], axis=1, keepdims=True)
    output = (output * (share * jax.nn.sigmoid(chosen - rival))).astype(BF16)
    piece = out_ref.shape[2]
    for at in range(out_ref.shape[0]):
        out_ref[at] = output[:, piece * at : piece * (at + 1)]
    copy.wait()


def pack(heads_ref, held_ref, res_ref, _, out_ref, __):
    value_width = heads_ref.shape[1]
    part = lax.dot_general(
        heads_ref[...],
        held_ref[:, held_ref.shape[1] - value_width :],
        (((1,), (1,)), ((), ())),
        preferred_element_type=F32,
    )
    with_res = (lax.axis_index("tp") == 0).astype(F32)
    part = part + res_ref[...].astype(F32) * with_res
    lines, lanes = out_ref.shape[1:]
    eighths = part.shape[0] // lines
    size = lanes // eighths
    group = lax.broadcasted_iota(jnp.int32, (2 * lines, lanes), 1) // size
    lower = lax.broadcasted_iota(jnp.int32, (2 * lines, lanes), 0) // lines
    for eighth in range(eighths):
        block = jnp.zeros((2 * lines, lanes), F32)
        for k in range(0, eighths, 2):
            rows = part[lines * k : lines * (k + 2)]
            for low in range(2):
                moved = pltpu.roll(rows, (size * (k + low - eighth)) % lanes, 1)
                block = jnp.where((group == k + low) & (lower == low), moved, block)
        block = (block[:lines] + block[lines:]).astype(BF16)
        quarter, core = eighth // 2, eighth % 2
        for row in range(out_ref.shape[0] // eighths):
            out_ref[eighths * row + eighths // 2 * core + quarter] = block


def dispatch(at_place, came_ref, along_ref, _, out_ref, hidden_ref, __, rows_ref, all_ref):
    depth, row = at_place()
    count, lines, lanes = came_ref.shape
    eighths = rows_ref.shape[0] // lines
    size = lanes // eighths
    heads = eighths // 2
    all_ref[...] = jnp.zeros_like(all_ref)
    hidden = []
    for at in range(count // heads):
        total = came_ref[heads * at].astype(F32)
        for head in range(1, heads):
            total = total + came_ref[heads * at + head].astype(F32)
        total = total.astype(BF16).astype(F32)
        both = jnp.concatenate([total, total], axis=0)
        back = pltpu.roll(both, lanes - size, 1)
        lower = lax.broadcasted_iota(jnp.int32, both.shape, 0) // lines
        hidden.append(jnp.where(lower == 0, both, back))
    group = lax.broadcasted_iota(jnp.int32, (2 * lines, lanes), 1) // size
    for k in range(0, eighths, 2):
        for half in range(2):
            block = jnp.zeros((2 * lines, lanes), F32)
            for m in range(eighths):
                moved = pltpu.roll(hidden[eighths * half + m], (size * (m - k)) % lanes, 1)
                block = jnp.where(group == m, moved, block)
            rows_ref[lines * k : lines * (k + 2), lanes * half : lanes * (half + 1)] = block
    rows = rows_ref[...].astype(BF16)
    own = hidden_ref.shape[0]
    slab = rows.shape[0]
    all_ref[pl.ds(pl.multiple_of(depth * slab, slab), slab)] = rows
    slots = jnp.dot(along_ref[...], all_ref[...], preferred_element_type=F32).astype(BF16)
    span = out_ref.shape[1]
    for at in range(out_ref.shape[0]):
        out_ref[at] = slots[span * at : span * (at + 1)]
    here = lax.broadcasted_iota(jnp.int32, (8, slab), 0)
    there = lax.broadcasted_iota(jnp.int32, (8, slab), 1)
    pick = jnp.where(there == here + own * row, 1.0, 0.0).astype(BF16)
    hidden_ref[...] = jnp.dot(pick, rows, preferred_element_type=F32)[:own].astype(BF16)


def on_device(
    residual_in,
    gla_state,
    norm_gain,
    w_query,
    w_key,
    w_value,
    w_decay,
    decay_bias,
    head_gain,
    w_output,
    ffn_gain,
    router_group,
    router_expert,
    expert_ids,
    w_gate,
    w_up,
    w_down,
):
    depths, rows, cores = (lax.axis_size(a) for a in EP)
    heads = lax.axis_size("tp")
    slab = rows * cores
    parts = cores * heads
    far = depths * rows
    tokens = expert_ids.shape[0]
    seqs, width = residual_in.shape
    strip = w_query.shape[0]
    key_width, value_width = w_query.shape[1], w_value.shape[1]
    in_width = 3 * key_width + value_width
    held = depths * strip
    piece = width // parts

    n_experts = router_expert.shape[0]

    def experts_of():
        core = lax.axis_index("ep_2")
        return lax.axis_index(FAR) * cores, core, lax.axis_index(SLAB), slab

    vmem = pl.BlockSpec(memory_space=pltpu.VMEM)
    later = (residual_in, norm_gain, head_gain, ffn_gain, decay_bias, router_group.T)
    shapes = [
        jax.ShapeDtypeStruct((depths, strip, in_width + value_width), BF16),
        pltpu.VMEM((width, held), BF16),
        pltpu.VMEM((depths * cores * CAP, tokens), BF16),
        pltpu.VMEM((cores * CAP, tokens), BF16),
        pltpu.VMEM((CAP, n_experts), F32),
        *(pltpu.VMEM(a.shape, a.dtype) for a in later),
    ]
    spread, pick, along, select, rival_lane, *later = pl.pallas_call(
        functools.partial(prepare, experts_of, strip),
        out_shape=shapes,
        in_specs=[pl.BlockSpec(memory_space=pl.ANY)] * 12,
        out_specs=[pl.BlockSpec(memory_space=pl.ANY)] + [vmem] * (len(shapes) - 1),
        scratch_shapes=[
            pltpu.VMEM((strip, in_width + value_width), BF16),
            pltpu.VMEM((expert_ids.shape[1], tokens), jnp.int32),
            pltpu.SemaphoreType.DMA((12 + depths,)),
        ],
    )(w_query, w_key, w_value, w_decay, w_output.T, expert_ids.T, *later)
    residual_in, norm_gain, head_gain, ffn_gain, decay_bias, group_rows = later
    head_gain = head_gain.astype(F32)[None]
    ffn_gain = ffn_gain.astype(F32)[None]
    decay_bias = decay_bias[None]
    norm_gain = norm_gain.astype(F32)[None]

    tied = lax.optimization_barrier(
        (spread, residual_in, pick, along, select, rival_lane, norm_gain)
        + (head_gain, ffn_gain, decay_bias)
    )
    spread, residual_in, pick, along, select, rival_lane, norm_gain, *tied = tied
    head_gain, ffn_gain, decay_bias = tied
    gathered = exchange(spread, "ep_0")
    rows_in = lax.all_gather(residual_in, SLAB, axis=0, tiled=True)
    lhs, slab_res = kernel_call(
        strips_of,
        out_shape=[pltpu.VMEM((slab * seqs, held), BF16)] * 2,
        in_specs=[vmem] * 3,
        out_specs=[vmem] * 2,
    )(on_chip(rows_in), on_chip(norm_gain), on_chip(pick))
    gathered, lhs, slab_res = lax.optimization_barrier((gathered, lhs, slab_res))
    gathered = gathered.reshape(held, in_width + value_width)
    sums = jnp.dot(lhs, gathered[:, :in_width], preferred_element_type=F32).astype(BF16)
    arrived = exchange(sums.reshape(slab, seqs, in_width), SLAB)
    gated, new_state = kernel_call(
        advance,
        out_shape=[
            pltpu.VMEM((slab, seqs, value_width), BF16),
            pltpu.VMEM((seqs, key_width, value_width), F32),
        ],
        in_specs=[vmem] * 5,
        out_specs=[vmem] * 2,
    )(*map(on_chip, (arrived.reshape(slab * seqs, in_width), residual_in, decay_bias, head_gain, gla_state[:, 0])))

    slab_heads, slab_res = exchange(gated, SLAB, slab_res)
    slab_heads = slab_heads.reshape(slab * seqs, value_width)
    lines = slab * seqs // parts
    state = pltpu.VMEM(new_state.shape, F32)
    came, new_state = kernel_call(
        pack,
        out_shape=[pltpu.VMEM((slab * heads, lines, held), BF16), state],
        in_specs=[vmem] * 4,
        out_specs=[vmem] * 2,
        input_output_aliases={3: 1},
    )(*map(on_chip, (slab_heads, gathered, slab_res, new_state)))
    came = exchange(came, SLAB_TP)

    def at_place():
        return lax.axis_index("ep_0"), lax.axis_index("ep_1")

    outward, hidden, new_state = kernel_call(
        functools.partial(dispatch, at_place),
        out_shape=[
            pltpu.VMEM((depths, cores * CAP, piece), BF16),
            pltpu.VMEM((cores * seqs, piece), BF16),
            state,
        ],
        in_specs=[vmem] * 3,
        out_specs=[vmem] * 3,
        scratch_shapes=[
            pltpu.VMEM((slab * seqs, piece), F32),
            pltpu.VMEM((tokens, piece), BF16),
        ],
        input_output_aliases={2: 2},
    )(on_chip(came), on_chip(along), on_chip(new_state))
    slot_part = exchange(outward, "ep_0").astype(F32).sum(axis=0).astype(BF16)
    slot_part = to_all(slot_part.reshape(cores, CAP, piece), heads)
    came = exchange(slot_part.reshape(parts, CAP, piece), CHIPS)
    operands = (router_expert, came, ffn_gain, group_rows, rival_lane)
    operands += (w_gate[0], w_up[0], w_down[0], new_state)
    back, new_state = kernel_call(
        functools.partial(mix, lambda: lax.axis_index(EP)),
        out_shape=[
            pltpu.VMEM((parts, CAP, piece), BF16),
            jax.ShapeDtypeStruct(new_state.shape, F32),
        ],
        in_specs=[vmem] * len(operands),
        out_specs=[vmem, pl.BlockSpec(memory_space=pl.ANY)],
        scratch_shapes=[
            pltpu.VMEM((CAP, width), F32),
            pltpu.SemaphoreType.DMA,
        ],
    )(*map(on_chip, operands))
    summed = exchange(back, CHIPS).reshape(heads, cores, CAP, piece).astype(F32).sum(axis=0)
    dense = lax.dot_general(
        select,
        summed.astype(BF16).reshape(cores * CAP, piece),
        (((0,), (0,)), ((), ())),
        preferred_element_type=F32,
    ).astype(BF16)
    moe, hidden = exchange(dense.reshape(far, cores * seqs, piece), FAR, hidden)
    moe = moe.astype(F32).sum(axis=0)
    layer = (hidden.astype(F32) + moe).astype(BF16)
    last = to_all(layer.reshape(cores, seqs, piece), heads).reshape(parts, seqs, piece)
    layer_out = exchange(last, CHIPS).transpose(1, 0, 2).reshape(seqs, width)
    return (layer_out, new_state[:, None])


def solution(mesh):
    torus = Mesh(mesh.devices.reshape(8, 8, 2, mesh.shape["tp"]), (*EP, "tp"))
    in_specs = (
        P(EP, None),
        P(EP, "tp", None, None),
        P(),
        P(EP, "tp"),
        P(EP, "tp"),
        P(EP, "tp"),
        P(EP, "tp"),
        P("tp"),
        P(),
        P("tp", EP),
        P(),
        P(),
        P(),
        P(),
        P(EP, None, "tp"),
        P(EP, None, "tp"),
        P(EP, "tp", None),
    )
    out_specs = (P(EP, None), P(EP, "tp", None, None))
    return jax.shard_map(
        on_device, mesh=torus, in_specs=in_specs, out_specs=out_specs, check_vma=False
    )
```

```python
import functools

import jax
import jax.numpy as jnp
from jax import lax
from jax.experimental import pallas as pl
from jax.experimental.pallas import tpu as pltpu
from jax.sharding import Mesh
from jax.sharding import PartitionSpec as P


CAP = 16
EP = ("ep_0", "ep_1", "ep_2")
FAR = ("ep_0", "ep_1")
SLAB = ("ep_1", "ep_2")
SLAB_TP = ("ep_1", "ep_2", "tp")
CHIPS = ("tp", "ep_2")

EPSILON = 1e-06
GATE_SCALE = 16.0
F32 = jnp.float32
BF16 = jnp.bfloat16


def exchange(blocks, axes, *later):
    came = lax.all_to_all(blocks, axes, split_axis=0, concat_axis=0, tiled=True)
    return lax.optimization_barrier((came, *later)) if later else came


def on_chip(array):
    return pltpu.with_memory_space_constraint(array, pltpu.VMEM)


def kernel_call(body, **settings):
    params = pltpu.CompilerParams(vmem_limit_bytes=6 * 2**20)
    return pl.pallas_call(body, compiler_params=params, **settings)


def to_all(shard, count):
    return jnp.broadcast_to(shard[None], (count, *shard.shape))


def prepare(experts_of, strip, *refs):
    sources, (spread, pick, along, select, rival, *kept) = refs[:12], refs[12:-3]
    own_w, ids, sems = refs[-3:]
    *weights, ids_in = sources[:6]
    width = 0
    copies = []
    for source in weights:
        place = own_w.at[:, pl.ds(width, source.shape[1])]
        copies.append(pltpu.make_async_copy(source, place, sems.at[len(copies)]))
        width += source.shape[1]
    fetched = len(copies)
    copies.append(pltpu.make_async_copy(ids_in, ids, sems.at[len(copies)]))
    for source, target in zip(sources[6:], kept, strict=True):
        copies.append(pltpu.make_async_copy(source, target, sems.at[len(copies)]))
    for copy in copies:
        copy.start()
    first, core, place, slab = experts_of()
    count = ids.shape[1]
    row = lax.broadcasted_iota(jnp.int32, (count, count), 0)
    col = lax.broadcasted_iota(jnp.int32, (count, count), 1)
    upper = jnp.where(row <= col, 1.0, 0.0).astype(BF16)
    feature = lax.broadcasted_iota(jnp.int32, (pick.shape[0] // spread.shape[0], 128), 0)
    lane = lax.broadcasted_iota(jnp.int32, feature.shape, 1)
    within = feature - place * strip == lane % strip
    for depth in range(spread.shape[0]):
        taken = within & (lane // strip == depth)
        at = feature.shape[0] * depth
        pick[at : at + feature.shape[0]] = jnp.where(taken, 1.0, 0.0).astype(BF16)
    for copy in copies[:fetched]:
        copy.wait()
    spreads = []
    for depth in range(spread.shape[0]):
        sem = sems.at[len(copies) + depth]
        spreads.append(pltpu.make_async_copy(own_w, spread.at[depth], sem))
        spreads[-1].start()
    copies[fetched].wait()
    one, two = ids[0:1, :], ids[1:2, :]
    spans = along.shape[0] // CAP
    cores = select.shape[0] // CAP
    index = lax.broadcasted_iota(jnp.int32, (spans + 8, count), 0)
    experts = index // cores * slab + place - core + index % cores
    experts = jnp.where(index < spans, experts, index - spans + first)
    named = (one == experts) | (two == experts)
    marks = jnp.where(named, 1.0, 0.0)
    ends = jnp.dot(marks.astype(BF16), upper, preferred_element_type=F32)
    slots = lax.broadcasted_iota(jnp.int32, (CAP, count), 0).astype(F32) + 1.0
    both = (one + two).astype(F32)
    own = first + core
    others = jnp.zeros((CAP, 1), F32)


    def slots_of(at):
        return jnp.where(ends[at : at + 1] == slots, marks[at : at + 1], 0.0)

    for span in range(spans):
        along[CAP * span : CAP * (span + 1)] = slots_of(span).astype(BF16)
    for c in range(cores):
        mine = slots_of(spans + c)
        select[CAP * c : CAP * (c + 1)] = mine.astype(BF16)
        total = jnp.sum(mine * both, axis=1, keepdims=True)
        others = jnp.where(core == c, total, others)
    lanes = lax.broadcasted_iota(jnp.int32, rival.shape, 1)
    rival[...] = jnp.where(lanes == others.astype(jnp.int32) - own, 1.0, 0.0)
    for copy in copies[fetched + 1 :] + spreads:
        copy.wait()


def strips_of(rows_ref, gain_ref, pick_ref, lhs_ref, res_ref):
    rows = rows_ref[...]
    pick = pick_ref[...]
    scaled = (rows.astype(F32) * gain_ref[...]).astype(BF16)
    res_ref[...] = jnp.dot(rows, pick, preferred_element_type=F32).astype(BF16)
    lhs_ref[...] = jnp.dot(scaled, pick, preferred_element_type=F32).astype(BF16)


def advance(came_ref, res_ref, bias_ref, gain_ref, old_ref, out_ref, held_ref):
    seqs, key_width, value_width = old_ref.shape
    count = came_ref.shape[0]
    seq_of = lax.broadcasted_iota(jnp.int32, (8, count), 1) % seqs
    pick = jnp.where(seq_of == lax.broadcasted_iota(jnp.int32, (8, count), 0), 1.0, 0.0)
    total = jnp.dot(pick.astype(BF16), came_ref[...], preferred_element_type=F32)[:seqs]
    res = res_ref[...].astype(F32)
    total = total * lax.rsqrt(jnp.mean(res * res, axis=1, keepdims=True) + EPSILON)
    query = total[:, :key_width].astype(BF16).astype(F32) * key_width ** (-0.5)
    key = total[:, key_width : 2 * key_width].astype(BF16).astype(F32)
    value = total[:, 2 * key_width : 2 * key_width + value_width].astype(BF16).astype(F32)
    pre = total[:, 2 * key_width + value_width :] + bias_ref[...]
    log_decay = (jnp.minimum(pre, 0.0) - jnp.log1p(jnp.exp(-jnp.abs(pre)))) / GATE_SCALE
    down = jnp.concatenate([query, key, jnp.exp(log_decay), jnp.zeros_like(query)], axis=0).T
    gated = []
    for seq in range(seqs):
        for at in range(0, key_width, 64):
            rows = slice(at, at + 64)
            key_col = down[rows, seqs + seq : seqs + seq + 1]
            alpha_col = down[rows, 2 * seqs + seq : 2 * seqs + seq + 1]
            new = alpha_col * old_ref[seq, rows] + key_col * value[seq : seq + 1]
            held_ref[seq, rows] = new
    for seq in range(seqs):
        read = jnp.zeros((8, value_width), F32)
        for at in range(0, key_width, 64):
            rows = slice(at, at + 64)
            part = down[rows, seq : seq + 1] * held_ref[seq, rows]
            read = read + jnp.sum(part.reshape(8, 8, value_width), axis=0)
        read = jnp.sum(read, axis=0, keepdims=True)
        mean = jnp.mean(read * read, axis=1, keepdims=True)
        gated.append(read * lax.rsqrt(mean + EPSILON) * gain_ref[...])
    gated = jnp.concatenate(gated, axis=0).astype(BF16)
    for at in range(out_ref.shape[0]):
        out_ref[at] = gated


def mix(
    which,
    expert_ref,
    came_ref,
    gain_ref,
    group_ref,
    rival_ref,
    gate_ref,
    up_ref,
    down_ref,
    state_ref,
    out_ref,
    new_ref,
    rows_ref,
    router_ref,
    sems,
):
    fetch = pltpu.make_async_copy(expert_ref, router_ref, sems.at[0])
    fetch.start()
    copies = []
    for seq in range(state_ref.shape[0]):
        source, target = state_ref.at[seq], new_ref.at[seq]
        copies.append(pltpu.make_async_copy(source, target, sems.at[1 + seq]))
        copies[-1].start()
    expert = which()
    size = came_ref.shape[2]
    for at in range(came_ref.shape[0]):
        rows_ref[:, size * at : size * (at + 1)] = came_ref[at].astype(F32)
    rows = rows_ref[...]
    mean = jnp.mean(rows * rows, axis=1, keepdims=True)
    rows = (rows * lax.rsqrt(mean + EPSILON) * gain_ref[...]).astype(BF16)
    gate = jnp.dot(rows, gate_ref[...], preferred_element_type=F32)
    up = jnp.dot(rows, up_ref[...], preferred_element_type=F32)
    over = (((1,), (1,)), ((), ()))
    groups = lax.dot_general(rows, group_ref[...], over, preferred_element_type=F32)
    units = (gate * jax.nn.sigmoid(gate) * up).astype(BF16)
    output = jnp.dot(units, down_ref[...], preferred_element_type=F32)
    fetch.wait()
    logits = lax.dot_general(rows, router_ref[...], over, preferred_element_type=F32)
    of_group = lax.broadcasted_iota(jnp.int32, groups.shape, 1)
    own = of_group == expert // (logits.shape[1] // groups.shape[1])
    group_logit = jnp.sum(jnp.where(own, groups, 0.0), axis=1, keepdims=True)
    share = 1.0 / jnp.sum(jnp.exp(groups - group_logit), axis=1, keepdims=True)
    lanes = lax.broadcasted_iota(jnp.int32, logits.shape, 1)
    chosen = jnp.sum(jnp.where(lanes == expert, logits, 0.0), axis=1, keepdims=True)
    rival = jnp.sum(logits * rival_ref[...], axis=1, keepdims=True)
    output = (output * (share * jax.nn.sigmoid(chosen - rival))).astype(BF16)
    piece = out_ref.shape[2]
    for at in range(out_ref.shape[0]):
        out_ref[at] = output[:, piece * at : piece * (at + 1)]
    for copy in copies:
        copy.wait()


def pack(heads_ref, held_ref, res_ref, _, out_ref, __):
    value_width = heads_ref.shape[1]
    part = lax.dot_general(
        heads_ref[...],
        held_ref[:, held_ref.shape[1] - value_width :],
        (((1,), (1,)), ((), ())),
        preferred_element_type=F32,
    )
    with_res = (lax.axis_index("tp") == 0).astype(F32)
    part = part + res_ref[...].astype(F32) * with_res
    lines, lanes = out_ref.shape[1:]
    eighths = part.shape[0] // lines
    size = lanes // eighths
    group = lax.broadcasted_iota(jnp.int32, (2 * lines, lanes), 1) // size
    lower = lax.broadcasted_iota(jnp.int32, (2 * lines, lanes), 0) // lines
    for eighth in range(eighths):
        block = jnp.zeros((2 * lines, lanes), F32)
        for k in range(0, eighths, 2):
            rows = part[lines * k : lines * (k + 2)]
            for low in range(2):
                moved = pltpu.roll(rows, (size * (k + low - eighth)) % lanes, 1)
                block = jnp.where((group == k + low) & (lower == low), moved, block)
        block = (block[:lines] + block[lines:]).astype(BF16)
        quarter, core = eighth // 2, eighth % 2
        for row in range(out_ref.shape[0] // eighths):
            out_ref[eighths * row + eighths // 2 * core + quarter] = block


def dispatch(at_place, came_ref, along_ref, _, out_ref, hidden_ref, __, rows_ref, all_ref):
    depth, row = at_place()
    count, lines, lanes = came_ref.shape
    eighths = rows_ref.shape[0] // lines
    size = lanes // eighths
    heads = eighths // 2
    all_ref[...] = jnp.zeros_like(all_ref)
    hidden = []
    for at in range(count // heads):
        total = came_ref[heads * at].astype(F32)
        for head in range(1, heads):
            total = total + came_ref[heads * at + head].astype(F32)
        total = total.astype(BF16).astype(F32)
        both = jnp.concatenate([total, total], axis=0)
        back = pltpu.roll(both, lanes - size, 1)
        lower = lax.broadcasted_iota(jnp.int32, both.shape, 0) // lines
        hidden.append(jnp.where(lower == 0, both, back))
    group = lax.broadcasted_iota(jnp.int32, (2 * lines, lanes), 1) // size
    for k in range(0, eighths, 2):
        for half in range(2):
            block = jnp.zeros((2 * lines, lanes), F32)
            for m in range(eighths):
                moved = pltpu.roll(hidden[eighths * half + m], (size * (m - k)) % lanes, 1)
                block = jnp.where(group == m, moved, block)
            rows_ref[lines * k : lines * (k + 2), lanes * half : lanes * (half + 1)] = block
    rows = rows_ref[...].astype(BF16)
    own = hidden_ref.shape[0]
    slab = rows.shape[0]
    all_ref[pl.ds(pl.multiple_of(depth * slab, slab), slab)] = rows
    slots = jnp.dot(along_ref[...], all_ref[...], preferred_element_type=F32).astype(BF16)
    span = out_ref.shape[1]
    for at in range(out_ref.shape[0]):
        out_ref[at] = slots[span * at : span * (at + 1)]
    here = lax.broadcasted_iota(jnp.int32, (8, slab), 0)
    there = lax.broadcasted_iota(jnp.int32, (8, slab), 1)
    pick = jnp.where(there == here + own * row, 1.0, 0.0).astype(BF16)
    hidden_ref[...] = jnp.dot(pick, rows, preferred_element_type=F32)[:own].astype(BF16)


def on_device(
    residual_in,
    gla_state,
    norm_gain,
    w_query,
    w_key,
    w_value,
    w_decay,
    decay_bias,
    head_gain,
    w_output,
    ffn_gain,
    router_group,
    router_expert,
    expert_ids,
    w_gate,
    w_up,
    w_down,
):
    depths, rows, cores = (lax.axis_size(a) for a in EP)
    heads = lax.axis_size("tp")
    slab = rows * cores
    parts = cores * heads
    far = depths * rows
    tokens = expert_ids.shape[0]
    seqs, width = residual_in.shape
    strip = w_query.shape[0]
    key_width, value_width = w_query.shape[1], w_value.shape[1]
    in_width = 3 * key_width + value_width
    held = depths * strip
    piece = width // parts

    n_experts = router_expert.shape[0]

    def experts_of():
        core = lax.axis_index("ep_2")
        return lax.axis_index(FAR) * cores, core, lax.axis_index(SLAB), slab

    vmem = pl.BlockSpec(memory_space=pltpu.VMEM)
    later = (residual_in, norm_gain, head_gain, ffn_gain, decay_bias, router_group.T)
    shapes = [
        jax.ShapeDtypeStruct((depths, strip, in_width + value_width), BF16),
        pltpu.VMEM((width, held), BF16),
        pltpu.VMEM((depths * cores * CAP, tokens), BF16),
        pltpu.VMEM((cores * CAP, tokens), BF16),
        pltpu.VMEM((CAP, n_experts), F32),
        *(pltpu.VMEM(a.shape, a.dtype) for a in later),
    ]
    spread, pick, along, select, rival_lane, *later = pl.pallas_call(
        functools.partial(prepare, experts_of, strip),
        out_shape=shapes,
        in_specs=[pl.BlockSpec(memory_space=pl.ANY)] * 12,
        out_specs=[pl.BlockSpec(memory_space=pl.ANY)] + [vmem] * (len(shapes) - 1),
        scratch_shapes=[
            pltpu.VMEM((strip, in_width + value_width), BF16),
            pltpu.VMEM((expert_ids.shape[1], tokens), jnp.int32),
            pltpu.SemaphoreType.DMA((12 + depths,)),
        ],
    )(w_query, w_key, w_value, w_decay, w_output.T, expert_ids.T, *later)
    residual_in, norm_gain, head_gain, ffn_gain, decay_bias, group_rows = later
    head_gain = head_gain.astype(F32)[None]
    ffn_gain = ffn_gain.astype(F32)[None]
    decay_bias = decay_bias[None]
    norm_gain = norm_gain.astype(F32)[None]

    tied = lax.optimization_barrier(
        (spread, residual_in, pick, along, select, rival_lane, norm_gain)
        + (head_gain, ffn_gain, decay_bias)
    )
    spread, residual_in, pick, along, select, rival_lane, norm_gain, *tied = tied
    head_gain, ffn_gain, decay_bias = tied
    gathered = exchange(spread, "ep_0")
    rows_in = lax.all_gather(residual_in, SLAB, axis=0, tiled=True)
    lhs, slab_res = kernel_call(
        strips_of,
        out_shape=[pltpu.VMEM((slab * seqs, held), BF16)] * 2,
        in_specs=[vmem] * 3,
        out_specs=[vmem] * 2,
    )(on_chip(rows_in), on_chip(norm_gain), on_chip(pick))
    gathered, lhs, slab_res = lax.optimization_barrier((gathered, lhs, slab_res))
    gathered = gathered.reshape(held, in_width + value_width)
    sums = jnp.dot(lhs, gathered[:, :in_width], preferred_element_type=F32).astype(BF16)
    arrived = exchange(sums.reshape(slab, seqs, in_width), SLAB)
    gated, new_state = kernel_call(
        advance,
        out_shape=[
            pltpu.VMEM((slab, seqs, value_width), BF16),
            pltpu.VMEM((seqs, key_width, value_width), F32),
        ],
        in_specs=[vmem] * 5,
        out_specs=[vmem] * 2,
    )(*map(on_chip, (arrived.reshape(slab * seqs, in_width), residual_in, decay_bias, head_gain, gla_state[:, 0])))

    slab_heads, slab_res = exchange(gated, SLAB, slab_res)
    slab_heads = slab_heads.reshape(slab * seqs, value_width)
    lines = slab * seqs // parts
    state = pltpu.VMEM(new_state.shape, F32)
    came, new_state = kernel_call(
        pack,
        out_shape=[pltpu.VMEM((slab * heads, lines, held), BF16), state],
        in_specs=[vmem] * 4,
        out_specs=[vmem] * 2,
        input_output_aliases={3: 1},
    )(*map(on_chip, (slab_heads, gathered, slab_res, new_state)))
    came = exchange(came, SLAB_TP)

    def at_place():
        return lax.axis_index("ep_0"), lax.axis_index("ep_1")

    outward, hidden, new_state = kernel_call(
        functools.partial(dispatch, at_place),
        out_shape=[
            pltpu.VMEM((depths, cores * CAP, piece), BF16),
            pltpu.VMEM((cores * seqs, piece), BF16),
            state,
        ],
        in_specs=[vmem] * 3,
        out_specs=[vmem] * 3,
        scratch_shapes=[
            pltpu.VMEM((slab * seqs, piece), F32),
            pltpu.VMEM((tokens, piece), BF16),
        ],
        input_output_aliases={2: 2},
    )(on_chip(came), on_chip(along), on_chip(new_state))
    slot_part = exchange(outward, "ep_0").astype(F32).sum(axis=0).astype(BF16)
    slot_part = to_all(slot_part.reshape(cores, CAP, piece), heads)
    came = exchange(slot_part.reshape(parts, CAP, piece), CHIPS)
    operands = (came, ffn_gain, group_rows, rival_lane)
    operands += (w_gate[0], w_up[0], w_down[0], new_state)
    back, new_state = kernel_call(
        functools.partial(mix, lambda: lax.axis_index(EP)),
        out_shape=[
            pltpu.VMEM((parts, CAP, piece), BF16),
            jax.ShapeDtypeStruct(new_state.shape, F32),
        ],
        in_specs=[pl.BlockSpec(memory_space=pl.ANY)] + [vmem] * len(operands),
        out_specs=[vmem, pl.BlockSpec(memory_space=pl.ANY)],
        scratch_shapes=[
            pltpu.VMEM((CAP, width), F32),
            pltpu.VMEM(router_expert.shape, BF16),
            pltpu.SemaphoreType.DMA((1 + seqs,)),
        ],
    )(router_expert, *map(on_chip, operands))
    summed = exchange(back, CHIPS).reshape(heads, cores, CAP, piece).astype(F32).sum(axis=0)
    dense = lax.dot_general(
        select,
        summed.astype(BF16).reshape(cores * CAP, piece),
        (((0,), (0,)), ((), ())),
        preferred_element_type=F32,
    ).astype(BF16)
    moe, hidden = exchange(dense.reshape(far, cores * seqs, piece), FAR, hidden)
    moe = moe.astype(F32).sum(axis=0)
    layer = (hidden.astype(F32) + moe).astype(BF16)
    last = to_all(layer.reshape(cores, seqs, piece), heads).reshape(parts, seqs, piece)
    layer_out = exchange(last, CHIPS).transpose(1, 0, 2).reshape(seqs, width)
    return (layer_out, new_state[:, None])


def solution(mesh):
    torus = Mesh(mesh.devices.reshape(8, 8, 2, mesh.shape["tp"]), (*EP, "tp"))
    in_specs = (
        P(EP, None),
        P(EP, "tp", None, None),
        P(),
        P(EP, "tp"),
        P(EP, "tp"),
        P(EP, "tp"),
        P(EP, "tp"),
        P("tp"),
        P(),
        P("tp", EP),
        P(),
        P(),
        P(),
        P(),
        P(EP, None, "tp"),
        P(EP, None, "tp"),
        P(EP, "tp", None),
    )
    out_specs = (P(EP, None), P(EP, "tp", None, None))
    return jax.shard_map(
        on_device, mesh=torus, in_specs=in_specs, out_specs=out_specs, check_vma=False
    )
```
